256 devices in a mesh: sp: 64 (over z, x, core), tp: 4 (over y).
Axes of the slice: x: 4, y: 4, z: 8, core: 2. Of those that a mesh axis runs over, the one named last changes fastest.
Arguments:
- hidden_rows: bfloat16 [8192, 2048], P('sp', 'tp'), may hold values from -6 to 6
- out_cot: bfloat16 [8192, 2048], P('sp', 'tp'), may hold values from -16 to 16
- routes: int32 [8192, 2], P('sp'), may hold values from 0 to 63, all different within a row; in each aligned block of 128 rows (0 to 127, 128 to 255, ...) at most 5 rows name the same one
- route_weight: float32 [8192, 2], P('sp'), may hold values from 0.2 to 2
- gate_w: bfloat16 [64, 2048, 1024], P('sp', None, 'tp'), may hold values from -0.125 to 0.125
- up_w: bfloat16 [64, 2048, 1024], P('sp', None, 'tp'), may hold values from -0.125 to 0.125
- down_w: bfloat16 [64, 1024, 2048], P('sp', 'tp'), may hold values from -0.1875 to 0.1875
- out_weight: bfloat16 [2048, 4096], P('sp', 'tp'), may hold values from -0.09375 to 0.09375
- step_inputs: bfloat16 [8192, 4096], P('sp', 'tp'), may hold values from -6 to 6
- input_map: bfloat16 [8192, 1024], P('sp', 'tp'), may hold values from -2 to 2
- output_map: bfloat16 [8192, 1024], P('sp', 'tp'), may hold values from -2 to 2
- log_decay: float32 [8192, 64], P('sp', 'tp'), may hold values from -1 to 0, as said below
- gate_z: bfloat16 [8192, 4096], P('sp', 'tp'), may hold values from -6 to 6
Outputs:
- grad_gate_w: float32 [64, 2048, 1024], P('sp', None, 'tp')
- grad_up_w: float32 [64, 2048, 1024], P('sp', None, 'tp')
- grad_down_w: float32 [64, 1024, 2048], P('sp', 'tp')
- grad_out_weight: float32 [2048, 4096], P('sp', 'tp')
- grad_step: bfloat16 [8192, 4096], P('sp', 'tp')
- grad_gate_z: bfloat16 [8192, 4096], P('sp', 'tp')
- grad_input_map: float32 [8192, 1024], P('sp', 'tp')
- grad_output_map: float32 [8192, 1024], P('sp', 'tp')
- grad_log_decay: float32 [8192, 64], P('sp', 'tp')
The draws below stay inside these ranges and needn't reach their ends.
Inputs may be any that keep to these rules, and one draw needn't show every extreme that they name: `routes`: each row names 2 different experts. Among the positions of one index of sp no expert is named more than 5 times, a bound that some block reaches. `log_decay`: every entry is negative.
All inputs are finite; a program needn't handle non-finite values.
Results may differ from the reference program's by a relative error of at most 0.015.
Values may be sent and summed in bfloat16 or wider, within the bound.
No kernel may reach another device: no remote copies, remote signals or barrier semaphores. Data moves between devices by JAX's collectives and lax.ppermute only.
A program may use at most 128 MiB of HBM per device.

```python
import math
import jax
import jax.numpy as jnp
import numpy as np
from jax import lax

D = 2048
MIXER_HEADS = 64
HEAD_DIM = 64
GROUPS = 8
NS = 128
FF = 1024
TOP = 2
BLOCK = 128
TOK_DEV = 128
SEQUENCE_TOKENS = 8192
EXPERTS = 64
INNER = 4096
CAP = 5
N_SP = 64
N_TP = 4


def draw_log_decay(key, part):
    random_child_keys = jax.random.split(key, 7)
    slow_share = 0.5
    rough_low = 0.5
    rough_high = 1.5
    slow_heads = jax.random.bernoulli(random_child_keys[0], slow_share, (MIXER_HEADS,))
    fast_rate = jnp.exp(jax.random.uniform(random_child_keys[1], (MIXER_HEADS,), jnp.float32, jnp.log(1.0 / 100.0), jnp.log(1.0 / 30.0)))
    slow_rate = jnp.exp(jax.random.uniform(random_child_keys[2], (MIXER_HEADS,), jnp.float32, jnp.log(0.6), jnp.log(1.4))) / SEQUENCE_TOKENS
    head_rate = jnp.where(slow_heads, slow_rate, fast_rate)
    block_factor = jnp.exp(jax.random.uniform(random_child_keys[3], (SEQUENCE_TOKENS // TOK_DEV,), jnp.float32, jnp.log(0.5), jnp.log(2.0)))
    position_factor = jnp.repeat(block_factor, TOK_DEV)
    roughness = jax.random.uniform(random_child_keys[4], (SEQUENCE_TOKENS, MIXER_HEADS), jnp.float32, rough_low, rough_high)
    head_decay_speeds = head_rate[None, :] * position_factor[:, None] * roughness
    spike_position = jax.random.randint(random_child_keys[5], (3,), 0, SEQUENCE_TOKENS)
    spike_retained = jax.random.uniform(random_child_keys[6], (3, MIXER_HEADS), jnp.float32, 0.55, 0.8)
    token_places = jnp.arange(SEQUENCE_TOKENS)
    spike_log_value = jnp.sum(jnp.where(token_places[:, None, None] == spike_position[None, :, None], jnp.log(spike_retained)[None, :, :], 0.0), axis=1)
    return (spike_log_value - head_decay_speeds).astype(jnp.float32)


def strengthened(array, rng, source, target, shards_of, factor):
    owner, partner = [(jnp.arange(array.shape[dim]) // (array.shape[dim] // shards_of)).reshape([-1 if axis == dim else 1 for axis in range(array.ndim)]) for dim in (source, target)]
    chosen = jax.random.permutation(rng, shards_of)[partner]
    strong = (owner == chosen) | (owner == (partner + shards_of // 2) % shards_of)
    return jnp.where(strong, factor * array, array)


def levels(rng, shape, cuts, least, top_value):
    gain, own = 1.0, jax.random.fold_in(rng, 6)
    for axis_at, parts in cuts:
        draws = jnp.exp(jax.random.uniform(jax.random.fold_in(own, axis_at), (parts,), jnp.float32, least / len(cuts), top_value / len(cuts)))
        gain = gain * jnp.repeat(draws, shape[axis_at] // parts).reshape([-1 if axis == axis_at else 1 for axis in range(len(shape))])
    return gain


def deal_out(stream_key, own, number, rows, number_of, top, limit, slope):
    order = jax.random.permutation(stream_key, number_of)
    heavy_load, usual = load_shares(number_of, rows * top, limit, slope, True), load_shares(number_of, rows * top, limit, slope, False)
    places = jnp.arange(number_of)

    def named(lengths, turn):
        used = int((lengths > 0).sum())
        fixed = max(1, used // 4)
        passed = fixed + (places - fixed + turn * (used - fixed)) % max(1, number_of - fixed)
        return jnp.zeros((number_of,), jnp.int32).at[order[jnp.where(places < fixed, places, passed)]].set(jnp.asarray(lengths, jnp.int32))

    lengths = jnp.where(number % 4 == 0, named(heavy_load, number // 4), named(usual, number - number // 4 - 1))
    mixed = jax.random.permutation(jax.random.fold_in(own, 3), number_of)
    source_of, sink = mixed[0:number_of // 2 * 2:2], mixed[1:number_of // 2 * 2:2]
    slack = jnp.minimum(lengths[source_of] - 1, limit - lengths[sink]) // 2
    slack = jnp.where((source_of == order[0]) | (sink == order[0]) | (lengths[sink] == 0), 0, jnp.maximum(slack, 0))
    passed = jax.random.randint(jax.random.fold_in(own, 4), (number_of // 2,), 0, 1 << 20) % (slack + 1)
    lengths = lengths.at[source_of].add(-passed).at[sink].add(passed)
    labels = jnp.searchsorted(jnp.cumsum(lengths), jnp.arange(rows * top), side="right").astype(jnp.int32)
    listing = labels.reshape(top, rows).T
    listing = listing[jax.random.permutation(jax.random.fold_in(own, 1), rows)]
    turn = jax.random.randint(jax.random.fold_in(own, 2), (rows, 1), 0, top)
    return jnp.take_along_axis(listing, (jnp.arange(top)[None, :] + turn) % top, axis=1)


def load_shares(number_of, total, bound, slope, full):
    portions = [(1 << 20) // math.isqrt(grade ** slope) + 1 for grade in range(1, number_of + 1)]
    largest = bound if full else min(bound, max(-(-total // number_of), total * portions[0] // sum(portions)))
    least = 1 if total - largest >= number_of - 1 else 0
    holding, surplus = [largest] + [least] * (number_of - 1), total - largest - least * (number_of - 1)
    while surplus > 0:
        free = [i for i in range(1, number_of) if holding[i] < largest] or [i for i in range(1, number_of) if holding[i] < bound]
        pool, budget = sum([portions[i] for i in free]), surplus
        for i in free:
            extra = min(bound - holding[i], max(1, budget * portions[i] // pool), surplus)
            holding[i] = holding[i] + extra
            surplus = surplus - extra
    return np.array(holding)


def noise(stream_key, shape, deviation, most, shards=(), kind=jnp.bfloat16):
    loudness = levels(stream_key, shape, shards, -0.22, 0.18) if shards else 1.0
    drawn = jax.random.normal(stream_key, shape, jnp.float32) * deviation * loudness
    return jnp.minimum(jnp.maximum(drawn, -most), most).astype(kind)


def heavy_noise(stream_key, dims, width, bound, pieces, heavy, held_as=jnp.bfloat16):
    result = width * jax.random.normal(stream_key, dims, jnp.float32)
    if pieces:
        result = result * levels(stream_key, dims, pieces, -0.22, 0.18)
    return jnp.clip(strengthened(result, jax.random.fold_in(stream_key, 3), *heavy), -bound, bound).astype(held_as)


def setup_inputs(seed: int = 0) -> dict:
    keys = jax.random.split(jax.random.key(seed), 14)
    hidden_rows = noise(keys[0], (SEQUENCE_TOKENS, D), 1.0, 6.0, ((0, 64), (1, 4)))
    out_cot = heavy_noise(keys[1], (SEQUENCE_TOKENS, D), 1.0, 16.0, ((0, 64), (1, 4)), (0, 1, 64, 4.0))
    routes_keys = jax.random.split(jax.random.fold_in(keys[2], 1), SEQUENCE_TOKENS // TOK_DEV)
    routes_turns = jax.random.permutation(jax.random.fold_in(keys[2], 3), SEQUENCE_TOKENS // TOK_DEV)
    routes = jax.vmap(lambda own, number: deal_out(jax.random.fold_in(keys[2], 2), own, number, TOK_DEV, EXPERTS, TOP, CAP, 2))(routes_keys, routes_turns).reshape((SEQUENCE_TOKENS, TOP))
    route_weight = jnp.clip(jnp.exp(math.log(2.0) - 2.3025851 * jax.random.uniform(keys[3], (SEQUENCE_TOKENS, TOP), jnp.float32) ** levels(keys[3], (SEQUENCE_TOKENS, TOP), ((0, 64),), -0.2, 0.2)), 0.2, 2.0)
    gate_w = noise(keys[4], (EXPERTS, D, FF), D ** -0.5, 0.125, ((0, 64), (2, 4)))
    up_w = noise(keys[5], (EXPERTS, D, FF), D ** -0.5, 0.125, ((0, 64), (2, 4)))
    down_w = noise(keys[6], (EXPERTS, FF, D), FF ** -0.5, 0.1875, ((0, 64), (1, 4)))
    out_weight = noise(keys[7], (D, INNER), INNER ** -0.5, 0.09375, ((0, 64), (1, 4)))
    step_inputs = noise(keys[8], (SEQUENCE_TOKENS, INNER), 1.0, 6.0, ((0, 64), (1, 4)))
    input_map = noise(keys[9], (SEQUENCE_TOKENS, GROUPS * NS), 0.3, 2.0, ((0, 64), (1, 4)))
    output_map = noise(keys[10], (SEQUENCE_TOKENS, GROUPS * NS), 0.3, 2.0, ((0, 64), (1, 4)))
    log_decay = draw_log_decay(jax.random.fold_in(keys[13], 71), 0)
    gate_z = noise(keys[12], (SEQUENCE_TOKENS, INNER), 1.0, 6.0, ((0, 64), (1, 4)))
    return dict(hidden_rows=hidden_rows, out_cot=out_cot, routes=routes, route_weight=route_weight, gate_w=gate_w, up_w=up_w, down_w=down_w, out_weight=out_weight, step_inputs=step_inputs, input_map=input_map, output_map=output_map, log_decay=log_decay, gate_z=gate_z)


epsilon = 1e-06
exact_mode = lax.Precision.HIGHEST
by_rows = (((0,), (0,)), ((), ()))
by_cols = (((1,), (1,)), ((), ()))

def block_step(carry_state, inputs):
    x_block, b_block, c_block, log_block = inputs
    per_group = x_block.shape[1] // b_block.shape[1]
    cum_log = jnp.cumsum(log_block, axis=0)
    token_places = jnp.arange(log_block.shape[0])
    lower_mask = (token_places[:, None] >= token_places[None, :])[:, :, None]
    log_spans = jnp.where(lower_mask, cum_log[:, None, :] - cum_log[None, :, :], 0.0)
    decay_mask = jnp.where(lower_mask, jnp.exp(log_spans), 0.0)
    scores = jnp.einsum('tgn,sgn->tsg', c_block, b_block, precision=exact_mode)
    scores = jnp.repeat(scores, per_group, axis=2)
    within = jnp.einsum('tsh,shp->thp', scores * decay_mask, x_block, precision=exact_mode)
    c_heads = jnp.repeat(c_block, per_group, axis=1)
    b_heads = jnp.repeat(b_block, per_group, axis=1)
    carried = jnp.einsum('thn,hpn->thp', c_heads, carry_state, precision=exact_mode) * jnp.exp(cum_log)[:, :, None]
    last_log = cum_log[-1]
    to_end = jnp.exp(last_log[None, :] - cum_log)
    new_state = carry_state * jnp.exp(last_log)[:, None, None] + jnp.einsum('shn,shp->hpn', b_heads * to_end[:, :, None], x_block, precision=exact_mode)
    return (new_state, within + carried)

def mixer_forward(step_in, map_in, map_out, log_in, gate_in, entry_state):
    length, head_count = log_in.shape
    groups = map_in.shape[1] // NS
    blocks = length // BLOCK
    x_blocks = step_in.reshape(blocks, BLOCK, head_count, HEAD_DIM)
    b_blocks = map_in.reshape(blocks, BLOCK, groups, NS)
    c_blocks = map_out.reshape(blocks, BLOCK, groups, NS)
    log_blocks = log_in.reshape(blocks, BLOCK, head_count)
    _, outputs = lax.scan(block_step, entry_state, (x_blocks, b_blocks, c_blocks, log_blocks))
    mixed = outputs.reshape(length, head_count * HEAD_DIM)
    gated = (mixed * jax.nn.silu(gate_in)).reshape(length, groups, -1)
    normed = gated * lax.rsqrt(lax.optimization_barrier(jnp.mean(gated * gated, axis=-1, keepdims=True)) + epsilon)
    return normed.reshape(length, head_count * HEAD_DIM)

def expert_backward(row_block, cot_block, gate_mat, up_mat, down_mat):
    gate_pre = jnp.dot(row_block, gate_mat, preferred_element_type=jnp.float32)
    up_pre = jnp.dot(row_block, up_mat, preferred_element_type=jnp.float32)
    gate_sigmoid = jax.nn.sigmoid(gate_pre)
    hidden = (gate_pre * gate_sigmoid * up_pre).astype(jnp.bfloat16)
    d_act = lax.dot_general(cot_block, down_mat, by_cols, preferred_element_type=jnp.float32)
    d_gate = (d_act * up_pre * gate_sigmoid * (1.0 + gate_pre * (1.0 - gate_sigmoid))).astype(jnp.bfloat16)
    d_up = (d_act * gate_pre * gate_sigmoid).astype(jnp.bfloat16)
    grad_down = lax.dot_general(hidden, cot_block, by_rows, preferred_element_type=jnp.float32)
    grad_gate = lax.dot_general(row_block, d_gate, by_rows, preferred_element_type=jnp.float32)
    grad_up = lax.dot_general(row_block, d_up, by_rows, preferred_element_type=jnp.float32)
    return (grad_gate, grad_up, grad_down, d_gate, d_up)

def reference(hidden_rows, out_cot, routes, route_weight, gate_w, up_w, down_w, out_weight, step_inputs, input_map, output_map, log_decay, gate_z):
    per_source = TOK_DEV * TOP
    buffer_rows = N_SP * CAP
    flat_routes = routes.reshape(N_SP, per_source)
    expert_hits = (flat_routes[:, :, None] == jnp.arange(EXPERTS, dtype=jnp.int32)[None, None, :]).astype(jnp.int32)
    slot_rank = lax.optimization_barrier(jnp.sum((jnp.cumsum(expert_hits, axis=1) - expert_hits) * expert_hits, axis=2))
    source = jnp.arange(N_SP, dtype=jnp.int32)[:, None]
    slot_index = (flat_routes * buffer_rows + source * CAP + slot_rank).reshape(-1).astype(jnp.int32)
    owner_token = jnp.repeat(jnp.arange(SEQUENCE_TOKENS, dtype=jnp.int32), TOP)
    slot_token = jnp.full((EXPERTS * buffer_rows,), SEQUENCE_TOKENS, jnp.int32).at[slot_index].set(owner_token)
    slot_weight = jnp.zeros((EXPERTS * buffer_rows,), jnp.float32).at[slot_index].set(route_weight.reshape(-1))
    padded_rows = jnp.concatenate([hidden_rows, jnp.zeros((1, D), jnp.bfloat16)], axis=0)
    padded_cot = jnp.concatenate([out_cot.astype(jnp.float32), jnp.zeros((1, D), jnp.float32)], axis=0)
    range_width = FF // N_TP

    def per_expert(expert):
        first_slot = (expert * buffer_rows).astype(jnp.int32)
        tokens_here = lax.dynamic_slice_in_dim(slot_token, first_slot, buffer_rows)
        weights_here = lax.dynamic_slice_in_dim(slot_weight, first_slot, buffer_rows)
        row_block = padded_rows[tokens_here]
        cot_block = (padded_cot[tokens_here] * weights_here[:, None]).astype(jnp.bfloat16)
        gate_mat = gate_w[expert]
        up_mat = up_w[expert]
        grad_gate, grad_up, grad_down, d_gate, d_up = expert_backward(row_block, cot_block, gate_mat, up_mat, down_w[expert])
        running = jnp.zeros((buffer_rows, D), jnp.float32)
        for quarter in range(N_TP):
            low_col = quarter * range_width
            high_col = low_col + range_width
            range_term = lax.dot_general(d_gate[:, low_col:high_col], gate_mat[:, low_col:high_col], by_cols, preferred_element_type=jnp.float32)
            range_term = range_term + lax.dot_general(d_up[:, low_col:high_col], up_mat[:, low_col:high_col], by_cols, preferred_element_type=jnp.float32)
            running = running + lax.optimization_barrier(range_term.astype(jnp.bfloat16)).astype(jnp.float32)
        return (grad_gate, grad_up, grad_down, running.astype(jnp.bfloat16))
    grad_gate_w, grad_up_w, grad_down_w, slot_grads = lax.map(per_expert, jnp.arange(EXPERTS, dtype=jnp.int32))
    routed = jax.ops.segment_sum(slot_grads.reshape(-1, D).astype(jnp.float32), slot_token, num_segments=SEQUENCE_TOKENS + 1)[:SEQUENCE_TOKENS]
    mid_grad = (out_cot.astype(jnp.float32) + routed).astype(jnp.bfloat16)
    d_normed = jnp.dot(mid_grad, out_weight, preferred_element_type=jnp.float32)
    start_state = jnp.zeros((MIXER_HEADS, HEAD_DIM, NS), jnp.float32)

    def forward(step_in, map_in, map_out, log_in, gate_in):
        return mixer_forward(step_in, map_in, map_out, log_in, gate_in, start_state)
    normed, pullback = jax.vjp(forward, step_inputs.astype(jnp.float32), input_map.astype(jnp.float32), output_map.astype(jnp.float32), log_decay, gate_z.astype(jnp.float32))
    grad_out_weight = lax.dot_general(mid_grad, normed.astype(jnp.bfloat16), by_rows, preferred_element_type=jnp.float32)
    grad_step, grad_in_map, grad_out_map, grad_log, grad_gate = pullback(d_normed)
    return (grad_gate_w, grad_up_w, grad_down_w, grad_out_weight, grad_step.astype(jnp.bfloat16), grad_gate.astype(jnp.bfloat16), grad_in_map, grad_out_map, grad_log)
```

```python
import jax
import jax.numpy as jnp
from jax import lax
from jax.experimental import pallas as pl
from jax.experimental.pallas import tpu as pltpu
from jax.sharding import Mesh
from jax.sharding import PartitionSpec as P

SP = ("sp_0", "sp_1", "sp_2")
FAR, NEAR, CORE = SP
CAP = 5
SUB = 8
LANES = 128
HEAD_DIM = 64
NS = 128
epsilon = 1e-06
exact = lax.Precision.HIGHEST
by_rows = (((0,), (0,)), ((), ()))
by_cols = (((1,), (1,)), ((), ()))


def mul(a, b, dims=None, precision=None):
    dims = (((1,), (0,)), ((), ())) if dims is None else dims
    return lax.dot_general(a, b, dims, precision=precision, preferred_element_type=jnp.float32)


def places(shape, dim):
    return lax.broadcasted_iota(jnp.int32, shape, dim)


def head_spread(heads, width):
    shape = (heads, width)
    return (places(shape, 1) // HEAD_DIM == places(shape, 0)).astype(jnp.float32)


def running(log):
    length = log.shape[0]
    shape = (length, length)
    lower = (places(shape, 0) >= places(shape, 1)).astype(jnp.float32)
    cum = mul(lower, log, precision=exact)
    cum_row = mul(log, lower, (((0,), (1,)), ((), ())), precision=exact)
    return cum, cum_row


def to_end_wide(log, cum, width):
    last = cum[-1:, :]
    return mul(jnp.exp(last - cum), head_spread(log.shape[1], width), precision=exact)


def place_kernel(routes_ref, weight_ref, rows_ref, cot_ref, out_ref, placing_ref, wide_ref):
    top, length = routes_ref.shape
    experts = placing_ref.shape[0] // CAP
    shape = (experts, length)
    expert = places(shape, 0)
    hits = [routes_ref[k : k + 1, :] == expert for k in range(top)]
    named = hits[0]
    for k in range(1, top):
        named = jnp.logical_or(named, hits[k])
    square = (length, length)
    sooner = (places(square, 0) < places(square, 1)).astype(jnp.bfloat16)
    taken = mul(named.astype(jnp.bfloat16), sooner)
    ranks = [jnp.sum(jnp.where(h, taken, 0.0), axis=0, keepdims=True) for h in hits]
    rows, cot = rows_ref[...], cot_ref[...]
    width = rows.shape[1]
    pieces = 2 * width // LANES
    for slot in range(CAP):
        here = [jnp.logical_and(hits[k], ranks[k] == float(slot)) for k in range(top)]
        weight = jnp.zeros((experts, 1), jnp.float32)
        for k in range(top):
            weight = weight + jnp.sum(
                jnp.where(here[k], weight_ref[k : k + 1, :], 0.0), axis=1, keepdims=True
            )
        chosen = here[0]
        for k in range(1, top):
            chosen = jnp.logical_or(chosen, here[k])
        chosen = chosen.astype(jnp.float32).astype(jnp.bfloat16)
        placing_ref[slot * experts : (slot + 1) * experts, :] = chosen
        both = (mul(chosen, rows), mul(chosen, cot) * weight)
        for j in range(pieces):
            source = both[j * LANES // width]
            start = j * LANES % width
            wide_ref[slot, pl.ds(j, experts, stride=pieces), :] = source[
                :, start : start + LANES
            ]
    for slot in range(CAP):
        out_ref[:, slot * LANES : (slot + 1) * LANES] = wide_ref[slot].astype(out_ref.dtype)


def arrange_kernel(got_ref, rows_ref, cot_ref, wide_ref):
    for slot in range(CAP):
        wide_ref[slot] = got_ref[:, slot * LANES : (slot + 1) * LANES].astype(jnp.float32)
    slots, width = rows_ref.shape
    count = slots // CAP
    pieces = 2 * width // LANES
    for slot in range(CAP):
        for j in range(pieces):
            block = wide_ref[slot, pl.ds(j, count, stride=pieces), :]
            out_ref = rows_ref if j * LANES < width else cot_ref
            start = j * LANES % width
            out_ref[slot * count : (slot + 1) * count, start : start + LANES] = block.astype(
                out_ref.dtype
            )


def block_of(rank, step, parts, width):
    return pl.multiple_of(lax.rem(rank + step, parts) * width, width)


def expert_kernel(rank_ref, *refs):
    parts = (len(refs) - 6) // 3
    rows_refs, cot_refs, part_refs = refs[:parts], refs[parts : 2 * parts], refs[-parts:]
    gate_ref, up_ref, down_ref, hidden_ref, dgate_ref, dup_ref = refs[2 * parts : -parts]
    slots, width = rows_refs[0].shape
    gate_pre = up_pre = d_act = None
    for step in range(parts):
        block = pl.ds(block_of(rank_ref[0], step, parts, width), width)
        rows, cot = rows_refs[step][...], cot_refs[step][...]
        one, two = mul(rows, gate_ref[block, :]), mul(rows, up_ref[block, :])
        three = mul(cot, down_ref[:, block], by_cols)
        gate_pre = one if step == 0 else gate_pre + one
        up_pre = two if step == 0 else up_pre + two
        d_act = three if step == 0 else d_act + three
    sig = jax.nn.sigmoid(gate_pre)
    hidden_ref[...] = (gate_pre * sig * up_pre).astype(jnp.bfloat16)
    d_gate = (d_act * up_pre * sig * (1.0 + gate_pre * (1.0 - sig))).astype(jnp.bfloat16)
    d_up = (d_act * gate_pre * sig).astype(jnp.bfloat16)
    dgate_ref[...] = d_gate
    dup_ref[...] = d_up
    for step in range(parts):
        block = pl.ds(block_of(rank_ref[0], step, parts, width), width)
        part = mul(d_gate, gate_ref[block, :], by_cols) + mul(d_up, up_ref[block, :], by_cols)
        part_refs[step][...] = part.astype(part_refs[step].dtype)


def weight_grad_kernel(rank_ref, *refs):
    parts = (len(refs) - 6) // 2
    rows_refs, cot_refs = refs[:parts], refs[parts : 2 * parts]
    hidden_ref, dgate_ref, dup_ref, gate_ref, up_ref, down_ref = refs[2 * parts :]
    width = rows_refs[0].shape[1]
    for step in range(parts):
        block = pl.ds(block_of(rank_ref[0], step, parts, width), width)
        rows, cot = rows_refs[step][...], cot_refs[step][...]
        gate_ref[block, :] = mul(rows, dgate_ref[...], by_rows)
        up_ref[block, :] = mul(rows, dup_ref[...], by_rows)
        down_ref[:, block] = mul(hidden_ref[...], cot, by_rows)


def add_kernel(one_ref, two_ref, three_ref, four_ref, out_ref, wide_ref):
    slots, width = one_ref.shape
    total = one_ref[...].astype(jnp.float32)
    for got_ref in (two_ref, three_ref, four_ref):
        total = total + got_ref[...].astype(jnp.float32)
    count = slots // CAP
    pieces = width // LANES
    for slot in range(CAP):
        for j in range(pieces):
            wide_ref[slot, pl.ds(j, count, stride=pieces), :] = total[
                slot * count : (slot + 1) * count, j * LANES : (j + 1) * LANES
            ]
    for slot in range(CAP):
        out_ref[:, slot * LANES : (slot + 1) * LANES] = wide_ref[slot].astype(out_ref.dtype)


def mid_kernel(place_ref, back_ref, placing_ref, cot_ref, out_ref, wide_ref, slots_ref):
    for slot in range(CAP):
        wide_ref[slot] = back_ref[:, slot * LANES : (slot + 1) * LANES].astype(jnp.float32)
    slots, width = slots_ref.shape
    count = slots // CAP
    pieces = width // LANES
    for slot in range(CAP):
        for j in range(pieces):
            block = wide_ref[slot, pl.ds(j, count, stride=pieces), :]
            slots_ref[slot * count : (slot + 1) * count, j * LANES : (j + 1) * LANES] = block.astype(
                slots_ref.dtype
            )
    routed = mul(placing_ref[...], slots_ref[...], by_rows)
    mid = (cot_ref[...].astype(jnp.float32) + routed).astype(jnp.bfloat16)
    shape = (width, width)
    source, target = places(shape, 0), places(shape, 1)
    near, core, piece = place_ref[1], place_ref[2], place_ref[3]
    near_count = place_ref[4]
    row = source // piece
    source_core, source_near, source_far = row % 2, row // 2 % near_count, row // (2 * near_count)
    step_near = (source_near - near + near_count) % near_count
    step_core = (source_core - core + 2) % 2
    per_block = width // (2 * near_count)
    moved = (step_near * 2 + step_core) * per_block + source_far * piece + source % piece
    out_ref[...] = mul(mid, (moved == target).astype(jnp.float32).astype(jnp.bfloat16)).astype(
        out_ref.dtype
    )


def weight_kernel(mine_ref, other_ref, out_ref):
    piece, steps, tp_count = 32, 4, 4
    per_tp = mine_ref.shape[0] // (tp_count * steps * piece)
    for q in range(tp_count):
        for step in range(steps):
            for core, ref in enumerate((mine_ref, other_ref)):
                for far in range(per_tp):
                    source = ((q * per_tp + far) * steps + step) * piece
                    target = (((q * steps + step) * 2 + core) * per_tp + far) * piece
                    out_ref[target : target + piece, :] = ref[source : source + piece, :]


def spread_kernel(*refs):
    mid_refs, out_refs = refs[:4], refs[4:]
    width = mid_refs[0].shape[1] // len(out_refs)
    for j, out_ref in enumerate(out_refs):
        for k, mid_ref in enumerate(mid_refs):
            out_ref[:, k * width : (k + 1) * width] = mid_ref[:, j * width : (j + 1) * width]


def put_state(out_ref, group, part):
    rows = part.shape[0] // 2
    tiles = part.reshape(rows // SUB, 2, SUB, NS)
    for k in range(2):
        out_ref[group * rows : (group + 1) * rows, k * NS : (k + 1) * NS] = (
            tiles[:, k].reshape(rows, NS).astype(out_ref.dtype)
        )


def get_state(ref, group, groups):
    rows = ref.shape[0] // groups
    halves = [
        ref[group * rows : (group + 1) * rows, k * NS : (k + 1) * NS]
        .astype(jnp.float32)
        .reshape(rows // SUB, SUB, NS)
        for k in range(2)
    ]
    return jnp.stack(halves, axis=1).reshape(2 * rows, NS)


def mix_kernel(got_ref, out_ref, back_ref, rest_ref):
    count = got_ref.shape[0]
    state = got_ref[:, : 2 * NS]
    logs = sum(
        got_ref[:, 2 * NS + k : 2 * NS + k + 1].astype(jnp.float32) for k in range(3)
    )
    log = jnp.broadcast_to(logs, (count, NS))
    through = log
    step = SUB
    while step < count:
        through = through + jnp.concatenate(
            [jnp.zeros((step, NS), jnp.float32), through[:-step]], axis=0
        )
        step *= 2
    before = through - log
    through_row, before_row = jnp.transpose(through)[:1], jnp.transpose(before)[:1]
    shape = (count, count)
    one, two = places(shape, 0), places(shape, 1)
    same = one % SUB == two % SUB
    spans = before[:, :1] - through_row
    weights = jnp.exp(jnp.where(jnp.logical_and(same, two < one), spans, -jnp.inf))
    high = weights.astype(jnp.bfloat16)
    low = (weights - high.astype(jnp.float32)).astype(jnp.bfloat16)
    out_ref[...] = (mul(high, state) + mul(low, state)).astype(out_ref.dtype)
    spans = before_row - through[:, :1]
    weights = jnp.exp(jnp.where(jnp.logical_and(same, one < two), spans, -jnp.inf))
    high = weights.astype(jnp.bfloat16)
    back_ref[...] = high
    rest_ref[...] = (weights - high.astype(jnp.float32)).astype(jnp.bfloat16)


def mix_back_kernel(got_ref, back_ref, rest_ref, out_ref):
    state = got_ref[...]
    out_ref[...] = (mul(back_ref[...], state) + mul(rest_ref[...], state)).astype(out_ref.dtype)


def state_kernel(x_ref, b_ref, log_ref, out_ref):
    log = log_ref[...]
    width = x_ref.shape[1]
    cum, _ = running(log)
    scaled = (x_ref[...].astype(jnp.float32) * to_end_wide(log, cum, width)).astype(jnp.bfloat16)
    groups = b_ref.shape[1] // NS
    each = width // groups
    for g in range(groups):
        part = mul(scaled[:, g * each : (g + 1) * each], b_ref[:, g * NS : (g + 1) * NS], by_rows)
        put_state(out_ref, g, part)
    rows, heads = out_ref.shape[0], log.shape[1]
    shape = (rows, heads)
    owner = places(shape, 0) // (rows // heads) == places(shape, 1)
    total = jnp.sum(jnp.where(owner, cum[-1:, :], 0.0), axis=1, keepdims=True)
    high = total.astype(jnp.bfloat16).astype(jnp.float32)
    middle = (total - high).astype(jnp.bfloat16).astype(jnp.float32)
    low = total - high - middle
    lane = places((rows, NS), 1)
    out_ref[:, 2 * NS :] = jnp.where(
        lane == 0, high, jnp.where(lane == 1, middle, jnp.where(lane == 2, low, 0.0))
    ).astype(out_ref.dtype)


def decays(cum, cum_row, head):
    length = cum.shape[0]
    shape = (length, length)
    spans = cum[:, head : head + 1] - cum_row[head : head + 1, :]
    return jnp.exp(jnp.where(places(shape, 0) >= places(shape, 1), spans, -jnp.inf))


def half_masks(length):
    lane = places((length, 2 * HEAD_DIM), 1)
    return (lane < HEAD_DIM, lane >= HEAD_DIM)


def forward_kernel(x_ref, b_ref, c_ref, log_ref, z_ref, entry_ref, y_ref, half_ref):
    log = log_ref[...]
    length, heads = log.shape
    width = x_ref.shape[1]
    groups = b_ref.shape[1] // NS
    each = width // groups
    per_group = heads // groups
    cum, cum_row = running(log)
    from_start = mul(jnp.exp(cum), head_spread(heads, width), precision=exact)
    masks = half_masks(length)
    zero = jnp.zeros((length, 2 * HEAD_DIM), jnp.bfloat16)
    for g in range(groups):
        c_group = c_ref[:, g * NS : (g + 1) * NS]
        scores = mul(c_group, b_ref[:, g * NS : (g + 1) * NS], by_cols)
        carried = mul(c_group, get_state(entry_ref, g, groups).astype(jnp.bfloat16), by_cols)
        pieces = []
        for pair in range(per_group // 2):
            head = g * per_group + 2 * pair
            x_pair = x_ref[:, head * HEAD_DIM : (head + 2) * HEAD_DIM]
            total = None
            for k in range(2):
                weights = (scores * decays(cum, cum_row, head + k)).astype(jnp.bfloat16)
                part = mul(weights, jnp.where(masks[k], x_pair, zero))
                total = part if total is None else total + part
            pieces.append(total)
        cols = slice(g * each, (g + 1) * each)
        y = jnp.concatenate(pieces, axis=1) + carried * from_start[:, cols]
        z = z_ref[:, cols].astype(jnp.float32)
        gated = y * (z * jax.nn.sigmoid(z))
        mean = jnp.mean(gated * gated, axis=1, keepdims=True)
        y_ref[:, cols] = y
        half_ref[:, cols] = (gated * lax.rsqrt(mean + epsilon)).astype(half_ref.dtype)


def gate_kernel(rank_ref, m0, m1, m2, m3, w_ref, y_ref, z_ref, c_ref, log_ref, dy_ref, dz_ref, out_ref):
    log = log_ref[...]
    heads = log.shape[1]
    width = y_ref.shape[1]
    groups = c_ref.shape[1] // NS
    each = width // groups
    cum, _ = running(log)
    from_start = mul(jnp.exp(cum), head_spread(heads, width), precision=exact)
    mid_refs = (m0, m1, m2, m3)
    parts, rows = len(mid_refs), m0.shape[1]
    for g in range(groups):
        cols = slice(g * each, (g + 1) * each)
        d_normed = None
        for step in range(parts):
            block = pl.ds(block_of(rank_ref[0], step, parts, rows), rows)
            part = mul(mid_refs[step][...], w_ref[block, cols])
            d_normed = part if d_normed is None else d_normed + part
        y = y_ref[:, cols]
        z = z_ref[:, cols].astype(jnp.float32)
        sig = jax.nn.sigmoid(z)
        silu = z * sig
        gated = y * silu
        inverse = lax.rsqrt(jnp.mean(gated * gated, axis=1, keepdims=True) + epsilon)
        normed = gated * inverse
        along = jnp.mean(d_normed * normed, axis=1, keepdims=True)
        d_gated = inverse * (d_normed - normed * along)
        d_y = d_gated * silu
        dy_ref[:, cols] = d_y.astype(dy_ref.dtype)
        dz_ref[:, cols] = (d_gated * y * (sig * (1.0 + z * (1.0 - sig)))).astype(dz_ref.dtype)
        scaled = (d_y * from_start[:, cols]).astype(jnp.bfloat16)
        part = mul(scaled, c_ref[:, g * NS : (g + 1) * NS], by_rows)
        put_state(out_ref, g, part)


def within_kernel(
    dy_ref, x_ref, b_ref, c_ref, log_ref, entry_ref, dx_ref, db_ref, dc_ref, dlog_ref
):
    log = log_ref[...]
    length, heads = log.shape
    width = x_ref.shape[1]
    groups = b_ref.shape[1] // NS
    per_group = heads // groups
    cum, cum_row = running(log)
    start = jnp.exp(cum)
    masks = half_masks(length)
    zero = jnp.zeros((length, 2 * HEAD_DIM), jnp.bfloat16)
    d_cum = jnp.zeros((length, heads), jnp.float32)
    d_row = jnp.zeros((heads, length), jnp.float32)
    head_col = places((length, heads), 1)
    head_row = places((heads, length), 0)
    for g in range(groups):
        c_group = c_ref[:, g * NS : (g + 1) * NS]
        b_group = b_ref[:, g * NS : (g + 1) * NS]
        c_wide = c_group.astype(jnp.float32)
        scores = mul(c_group, b_group, by_cols)
        d_scores = jnp.zeros((length, length), jnp.float32)
        d_c = jnp.zeros((length, NS), jnp.float32)
        entry = get_state(entry_ref, g, groups).astype(jnp.bfloat16)
        for pair in range(per_group // 2):
            head = g * per_group + 2 * pair
            cols = slice(head * HEAD_DIM, (head + 2) * HEAD_DIM)
            x_pair = x_ref[:, cols]
            dy_pair = dy_ref[:, cols]
            entry_pair = entry[2 * pair * HEAD_DIM : (2 * pair + 2) * HEAD_DIM, :]
            d_x = None
            for k in range(2):
                decay = decays(cum, cum_row, head + k)
                dy_one = jnp.where(masks[k], dy_pair, zero)
                weights = scores * decay
                d_weights = mul(dy_one, x_pair, by_cols)
                part = mul(weights.astype(jnp.bfloat16), dy_one, by_rows)
                d_x = part if d_x is None else d_x + part
                d_scores = d_scores + d_weights * decay
                spread = d_weights * weights
                from_entry = mul(dy_one, entry_pair) * start[:, head + k : head + k + 1]
                d_c = d_c + from_entry
                rows = jnp.sum(spread + c_wide * from_entry, axis=1, keepdims=True)
                d_cum = jnp.where(head_col == head + k, rows, d_cum)
                d_row = jnp.where(
                    head_row == head + k, jnp.sum(spread, axis=0, keepdims=True), d_row
                )
            dx_ref[:, cols] = d_x
        half = d_scores.astype(jnp.bfloat16)
        dc_ref[:, g * NS : (g + 1) * NS] = d_c + mul(half, b_group)
        db_ref[:, g * NS : (g + 1) * NS] = mul(half, c_group, by_rows)
    shape = (length, length)
    upper = (places(shape, 0) <= places(shape, 1)).astype(jnp.float32)
    dlog_ref[...] = mul(upper, d_cum, precision=exact) - mul(upper, d_row, by_cols, precision=exact)


def final_kernel(
    x_ref, b_ref, log_ref, grad_ref, entry_ref, dx_ref, db_ref, dlog_ref, gx_ref, gb_ref, glog_ref
):
    log = log_ref[...]
    length, heads = log.shape
    width = x_ref.shape[1]
    groups = b_ref.shape[1] // NS
    each = width // groups
    cum, _ = running(log)
    spread = head_spread(heads, width)
    to_end = to_end_wide(log, cum, width)
    x = x_ref[...].astype(jnp.float32)
    scaled = (x * to_end).astype(jnp.bfloat16)
    moved = jnp.zeros((length, heads), jnp.float32)
    ones = jnp.ones((8, NS), jnp.float32)
    kept = jnp.zeros((8, heads), jnp.float32)
    for g in range(groups):
        cols = slice(g * each, (g + 1) * each)
        grad_wide = get_state(grad_ref, g, groups)
        grad = grad_wide.astype(jnp.bfloat16)
        d_x = mul(b_ref[:, g * NS : (g + 1) * NS], grad, by_cols) * to_end[:, cols]
        gx_ref[:, cols] = (dx_ref[:, cols] + d_x).astype(gx_ref.dtype)
        moved = moved + mul(x[:, cols] * d_x, spread[:, cols], by_cols, precision=exact)
        gb_ref[:, g * NS : (g + 1) * NS] = db_ref[:, g * NS : (g + 1) * NS] + mul(
            scaled[:, cols], grad
        )
        both = get_state(entry_ref, g, groups) * grad_wide
        kept = kept + mul(
            mul(ones, both, by_cols, precision=exact), spread[:, cols], by_cols, precision=exact
        )
    shape = (length, length)
    earlier = (places(shape, 0) > places(shape, 1)).astype(jnp.float32)
    glog_ref[...] = (
        dlog_ref[...] + mul(earlier, moved, precision=exact) + kept[:1, :] * jnp.exp(cum[-1:, :])
    )


def out_grad_kernel(rank_ref, *refs):
    count = (len(refs) - 1) // 2
    mid_refs, half_refs, out_ref = refs[:count], refs[count : 2 * count], refs[-1]
    total = None
    for mid_ref, half_ref in zip(mid_refs, half_refs):
        part = mul(mid_ref[...], half_ref[...], by_rows)
        total = part if total is None else total + part
    parts = 4
    rows = total.shape[0] // parts
    for step in range(parts):
        block = pl.ds(block_of(rank_ref[0], step, parts, rows), rows)
        out_ref[block, :] = total[step * rows : (step + 1) * rows].astype(out_ref.dtype)


def call(kernel, shapes, *args, scratch=(), scalars=0):
    whole = pl.BlockSpec(memory_space=pltpu.VMEM)
    scalar = pl.BlockSpec(memory_space=pltpu.SMEM)
    return pl.pallas_call(
        kernel,
        out_shape=tuple(jax.ShapeDtypeStruct(s, d) for s, d in shapes),
        in_specs=[scalar if i < scalars else whole for i in range(len(args))],
        out_specs=tuple(whole for _ in shapes),
        scratch_shapes=[pltpu.VMEM(s, d) for s, d in scratch],
        compiler_params=pltpu.CompilerParams(vmem_limit_bytes=50 * 1024 * 1024),
        name=kernel.__name__,
    )(*args)


def swap(array, axis):
    return lax.all_to_all(array, axis, split_axis=0, concat_axis=0, tiled=True)


def moved(array, axis, step):
    count = lax.axis_size(axis)
    return lax.ppermute(array, axis, [((i + step) % count, i) for i in range(count)])


def from_others(array, axis):
    return [array] + [moved(array, axis, step) for step in (1, 2, 3)]


def local(
    hidden_rows,
    out_cot,
    routes,
    route_weight,
    gate_w,
    up_w,
    down_w,
    out_weight,
    step_inputs,
    input_map,
    output_map,
    log_decay,
    gate_z,
):
    f32, bf16 = jnp.float32, jnp.bfloat16
    length, heads = log_decay.shape
    inner = step_inputs.shape[1]
    maps = input_map.shape[1]
    sp_count, tp_count = lax.axis_size(SP), lax.axis_size("tp")
    width = hidden_rows.shape[1]
    slots = sp_count * CAP
    pieces = width // LANES
    hidden_units = gate_w.shape[2]
    full = width * tp_count

    rank = lax.axis_index("tp").astype(jnp.int32)[None]
    position = jnp.stack(
        [
            jnp.asarray(v, jnp.int32)
            for v in (
                lax.axis_index(FAR),
                lax.axis_index(NEAR),
                lax.axis_index(CORE),
                out_weight.shape[0],
                lax.axis_size(NEAR),
            )
        ]
    )
    sent, placing = call(
        place_kernel,
        [((sp_count * 2 * pieces, CAP * LANES), bf16), ((slots, length), bf16)],
        routes.T,
        route_weight.T,
        hidden_rows,
        out_cot,
        scratch=[((CAP, sp_count * 2 * pieces, LANES), f32)],
    )
    state_rows = inner // 2
    (own,) = call(
        state_kernel, [((state_rows, 3 * NS), bf16)], step_inputs, input_map, log_decay
    )
    near_pieces, _ = lax.optimization_barrier((from_others(out_weight, NEAR), placing))
    near_weight = jnp.concatenate(near_pieces, axis=0)
    sent, own = lax.optimization_barrier((sent, own))
    got = swap(sent.reshape(sp_count, 2 * pieces, CAP * LANES), SP)
    rows, cot = call(
        arrange_kernel,
        [((slots, width), bf16)] * 2,
        got.reshape(sent.shape),
        scratch=[((CAP, sent.shape[0], LANES), f32)],
    )
    rows_next, rows_last = moved(rows, "tp", 1), moved(rows, "tp", -1)
    cot_next, cot_last = moved(cot, "tp", 1), moved(cot, "tp", -1)
    filled = (
        rows,
        rows_next,
        moved(rows_last, "tp", -1),
        rows_last,
        cot,
        cot_next,
        moved(cot_next, "tp", 1),
        cot_last,
    )
    half_weight = lax.all_gather(near_weight, FAR, axis=0, tiled=True)
    got_own = swap(own.reshape(sp_count, SUB, 3 * NS), SP).reshape(own.shape)
    mixed, back, rest = call(
        mix_kernel,
        [((state_rows, 2 * NS), bf16)] + [((state_rows, state_rows), bf16)] * 2,
        got_own,
    )
    entry = swap(mixed.reshape(sp_count, SUB, 2 * NS), SP).reshape(mixed.shape)
    filled, mixed = lax.optimization_barrier((filled, mixed))
    hidden, d_gate, d_up, *partials = call(
        expert_kernel,
        [((slots, hidden_units), bf16)] * 3 + [((slots, width), bf16)] * tp_count,
        rank,
        *filled,
        gate_w[0],
        up_w[0],
        down_w[0],
        scalars=1,
    )
    half_weight, _ = lax.optimization_barrier((half_weight, d_up))
    (full_weight,) = call(
        weight_kernel,
        [((full, inner), bf16)],
        half_weight,
        moved(half_weight, CORE, 1),
    )
    (summed,) = call(
        add_kernel,
        [((sp_count * pieces, CAP * LANES), bf16)],
        partials[0],
        *(moved(partials[step], "tp", -step) for step in (1, 2, 3)),
        scratch=[((CAP, sp_count * pieces, LANES), f32)],
    )
    returned = swap(summed.reshape(sp_count, pieces, CAP * LANES), SP).reshape(summed.shape)
    placing, full_weight = lax.optimization_barrier((placing, full_weight))
    (mid_part,) = call(
        mid_kernel,
        [((length, width), bf16)],
        position,
        returned,
        placing,
        out_cot,
        scratch=[((CAP, summed.shape[0], LANES), f32), ((slots, width), bf16)],
        scalars=1,
    )
    mids = from_others(mid_part, "tp")
    grad_gate, grad_up, grad_down = call(
        weight_grad_kernel,
        [((full, hidden_units), f32)] * 2 + [((hidden_units, full), f32)],
        rank,
        *filled,
        hidden,
        d_gate,
        d_up,
        scalars=1,
    )
    y, half = call(
        forward_kernel,
        [((length, inner), f32), ((length, inner), bf16)],
        step_inputs,
        input_map,
        output_map,
        log_decay,
        gate_z,
        entry,
    )
    halves = from_others(half, NEAR)
    halves_other = [moved(h, CORE, 1) for h in halves]
    d_y, grad_z, entry_grad = call(
        gate_kernel,
        [((length, inner), bf16)] * 2 + [((state_rows, 2 * NS), bf16)],
        rank,
        *mids,
        full_weight,
        y,
        gate_z,
        output_map,
        log_decay,
        scalars=1,
    )
    got_grad = swap(entry_grad.reshape(sp_count, SUB, 2 * NS), SP).reshape(entry_grad.shape)
    (mixed_grad,) = call(
        mix_back_kernel, [((state_rows, 2 * NS), bf16)], got_grad, back, rest
    )
    carried = swap(mixed_grad.reshape(sp_count, SUB, 2 * NS), SP).reshape(mixed_grad.shape)
    near_count = lax.axis_size(NEAR)
    blocks = call(
        spread_kernel,
        [((length, full // (2 * near_count)), bf16)] * (2 * near_count),
        *mids,
    )
    mids_here, halves_here = [], []
    for step in range(near_count):
        for core in range(2):
            pairs = [
                (
                    n * 2 + c,
                    (n + step) % near_count * 2 + (c + core) % 2,
                )
                for n in range(near_count)
                for c in range(2)
            ]
            block = blocks[step * 2 + core]
            if step or core:
                block = lax.ppermute(block, (NEAR, CORE), pairs)
            mids_here.append(block)
            halves_here.append((halves_other if core else halves)[-step % near_count])
    mids_here, _ = lax.optimization_barrier((mids_here, entry_grad))
    (out_grad,) = call(
        out_grad_kernel,
        [((full // (2 * near_count), inner), bf16)],
        rank,
        *mids_here,
        *halves_here,
        scalars=1,
    )
    grad_out_weight = lax.psum_scatter(
        out_grad, FAR, scatter_dimension=0, tiled=True
    ).astype(f32)
    d_x, d_b, grad_out_map, d_log = call(
        within_kernel,
        [((length, inner), f32), ((length, maps), f32), ((length, maps), f32), ((length, heads), f32)],
        d_y,
        step_inputs,
        input_map,
        output_map,
        log_decay,
        entry,
    )
    grad_step, grad_in_map, grad_log = call(
        final_kernel,
        [((length, inner), bf16), ((length, maps), f32), ((length, heads), f32)],
        step_inputs,
        input_map,
        log_decay,
        carried,
        entry,
        d_x,
        d_b,
        d_log,
    )
    return (
        grad_gate[None],
        grad_up[None],
        grad_down[None],
        grad_out_weight,
        grad_step,
        grad_z,
        grad_in_map,
        grad_out_map,
        grad_log,
    )


def solution(mesh):
    torus = Mesh(mesh.devices.reshape(8, 4, 2, mesh.shape["tp"]), ("sp_0", "sp_1", "sp_2", "tp"))
    placed = (
        P(SP, "tp"),
        P(SP, "tp"),
        P(SP, None),
        P(SP, None),
        P(SP, None, "tp"),
        P(SP, None, "tp"),
        P(SP, "tp", None),
        P(SP, "tp"),
        P(SP, "tp"),
        P(SP, "tp"),
        P(SP, "tp"),
        P(SP, "tp"),
        P(SP, "tp"),
    )
    return jax.shard_map(
        local,
        mesh=torus,
        in_specs=placed,
        out_specs=(
            P(SP, None, "tp"),
            P(SP, None, "tp"),
            P(SP, "tp", None),
            P(SP, "tp"),
            P(SP, "tp"),
            P(SP, "tp"),
            P(SP, "tp"),
            P(SP, "tp"),
            P(SP, "tp"),
        ),
        check_vma=False,
    )
```

```python
import jax
import jax.numpy as jnp
from jax import lax
from jax.experimental import pallas as pl
from jax.experimental.pallas import tpu as pltpu
from jax.sharding import Mesh
from jax.sharding import PartitionSpec as P


SP = ("sp_0", "sp_1", "sp_2")
FAR, NEAR, CORE = SP
CAP = 5
SUB = 8
GRANT = 16 * 1024 * 1024
PIECE = 32
LANES = 128
HEAD_DIM = 64
NS = 128
epsilon = 1e-06
exact = lax.Precision.HIGHEST
by_rows = (((0,), (0,)), ((), ()))
by_cols = (((1,), (1,)), ((), ()))


def mul(a, b, dims=None, precision=None):
    dims = (((1,), (0,)), ((), ())) if dims is None else dims
    return lax.dot_general(a, b, dims, precision=precision, preferred_element_type=jnp.float32)


def places(shape, dim):
    return lax.broadcasted_iota(jnp.int32, shape, dim)


def head_spread(heads, width):
    shape = (heads, width)
    return (places(shape, 1) // HEAD_DIM == places(shape, 0)).astype(jnp.float32)


def running(log):
    length = log.shape[1]
    shape = (length, length)
    lower = (places(shape, 0) >= places(shape, 1)).astype(jnp.float32)
    return mul(lower, log, by_cols, precision=exact), mul(log, lower, by_cols, precision=exact)


def to_end_wide(cum, width):
    last = cum[-1:, :]
    return mul(jnp.exp(last - cum), head_spread(cum.shape[1], width), precision=exact)


def place_kernel(routes_ref, weight_ref, rows_ref, cot_ref, out_ref, placing_ref, wide_ref):
    top, length = routes_ref.shape
    experts = placing_ref.shape[0] // CAP
    shape = (experts, length)
    expert = places(shape, 0)
    hits = [routes_ref[k : k + 1, :] == expert for k in range(top)]
    named = hits[0]
    for k in range(1, top):
        named = jnp.logical_or(named, hits[k])
    square = (length, length)
    sooner = (places(square, 0) < places(square, 1)).astype(jnp.bfloat16)
    taken = mul(named.astype(jnp.bfloat16), sooner)
    ranks = [jnp.sum(jnp.where(h, taken, 0.0), axis=0, keepdims=True) for h in hits]
    rows, cot = rows_ref[...], cot_ref[...]
    width = rows.shape[1]
    pieces = 2 * width // LANES
    for slot in range(CAP):
        here = [jnp.logical_and(hits[k], ranks[k] == float(slot)) for k in range(top)]
        weight = jnp.zeros((experts, 1), jnp.float32)
        for k in range(top):
            weight = weight + jnp.sum(
                jnp.where(here[k], weight_ref[k : k + 1, :], 0.0), axis=1, keepdims=True
            )
        chosen = here[0]
        for k in range(1, top):
            chosen = jnp.logical_or(chosen, here[k])
        chosen = chosen.astype(jnp.float32).astype(jnp.bfloat16)
        placing_ref[slot * experts : (slot + 1) * experts, :] = chosen
        both = (mul(chosen, rows), mul(chosen, cot) * weight)
        for j in range(pieces):
            source = both[j * LANES // width]
            start = j * LANES % width
            wide_ref[slot, pl.ds(j, experts, stride=pieces), :] = source[
                :, start : start + LANES
            ]
    for slot in range(CAP):
        out_ref[:, slot * LANES : (slot + 1) * LANES] = wide_ref[slot].astype(out_ref.dtype)


def arrange_kernel(got_ref, rows_ref, cot_ref, wide_ref):
    for slot in range(CAP):
        wide_ref[slot] = got_ref[:, slot * LANES : (slot + 1) * LANES].astype(jnp.float32)
    slots, width = rows_ref.shape
    count = slots // CAP
    pieces = 2 * width // LANES
    for slot in range(CAP):
        for j in range(pieces):
            block = wide_ref[slot, pl.ds(j, count, stride=pieces), :]
            out_ref = rows_ref if j * LANES < width else cot_ref
            start = j * LANES % width
            out_ref[slot * count : (slot + 1) * count, start : start + LANES] = block.astype(
                out_ref.dtype
            )


def block_of(rank, step, parts, width):
    return pl.multiple_of(lax.rem(rank + step, parts) * width, width)


def expert_kernel(rank_ref, *refs):
    parts = (len(refs) - 6) // 3
    rows_refs, cot_refs, part_refs = refs[:parts], refs[parts : 2 * parts], refs[-parts:]
    gate_ref, up_ref, down_ref, hidden_ref, dgate_ref, dup_ref = refs[2 * parts : -parts]
    _, width = rows_refs[0].shape
    gate_pre = up_pre = d_act = None
    for step in range(parts):
        block = pl.ds(block_of(rank_ref[0], step, parts, width), width)
        rows, cot = rows_refs[step][...], cot_refs[step][...]
        one, two = mul(rows, gate_ref[block, :]), mul(rows, up_ref[block, :])
        three = mul(cot, down_ref[:, block], by_cols)
        gate_pre = one if step == 0 else gate_pre + one
        up_pre = two if step == 0 else up_pre + two
        d_act = three if step == 0 else d_act + three
    sig = jax.nn.sigmoid(gate_pre)
    hidden_ref[...] = (gate_pre * sig * up_pre).astype(jnp.bfloat16)
    d_gate = (d_act * up_pre * sig * (1.0 + gate_pre * (1.0 - sig))).astype(jnp.bfloat16)
    d_up = (d_act * gate_pre * sig).astype(jnp.bfloat16)
    dgate_ref[...] = d_gate
    dup_ref[...] = d_up
    for step in range(parts):
        block = pl.ds(block_of(rank_ref[0], step, parts, width), width)
        part = mul(d_gate, gate_ref[block, :], by_cols) + mul(d_up, up_ref[block, :], by_cols)
        part_refs[step][...] = part.astype(part_refs[step].dtype)


def weight_grad_kernel(rank_ref, *refs):
    parts = (len(refs) - 6) // 2
    rows_refs, cot_refs = refs[:parts], refs[parts : 2 * parts]
    hidden_ref, dgate_ref, dup_ref, gate_ref, up_ref, down_ref = refs[2 * parts :]
    width = rows_refs[0].shape[1]
    for step in range(parts):
        block = pl.ds(block_of(rank_ref[0], step, parts, width), width)
        rows, cot = rows_refs[step][...], cot_refs[step][...]
        gate_ref[block, :] = mul(rows, dgate_ref[...], by_rows)
        up_ref[block, :] = mul(rows, dup_ref[...], by_rows)
        down_ref[:, block] = mul(hidden_ref[...], cot, by_rows)


def add_kernel(one_ref, two_ref, three_ref, four_ref, out_ref, wide_ref):
    slots, width = one_ref.shape
    total = one_ref[...].astype(jnp.float32)
    for got_ref in (two_ref, three_ref, four_ref):
        total = total + got_ref[...].astype(jnp.float32)
    count = slots // CAP
    pieces = width // LANES
    wide_ref[...] = jnp.zeros_like(wide_ref)
    for slot in range(CAP):
        for j in range(pieces):
            tile, row = divmod(slot * pieces + j, SUB)
            wide_ref[tile, pl.ds(row, count, stride=SUB), :] = total[
                slot * count : (slot + 1) * count, j * LANES : (j + 1) * LANES
            ]
    for tile in range(wide_ref.shape[0]):
        out_ref[:, tile * LANES : (tile + 1) * LANES] = wide_ref[tile].astype(out_ref.dtype)


def mid_kernel(near_ref, core_ref, back_ref, placing_ref, cot_ref, out_ref, wide_ref, slots_ref):
    for tile in range(wide_ref.shape[0]):
        wide_ref[tile] = back_ref[:, tile * LANES : (tile + 1) * LANES].astype(jnp.float32)
    slots, width = slots_ref.shape
    count = slots // CAP
    pieces = width // LANES
    for slot in range(CAP):
        for j in range(pieces):
            tile, row = divmod(slot * pieces + j, SUB)
            block = wide_ref[tile, pl.ds(row, count, stride=SUB), :]
            slots_ref[slot * count : (slot + 1) * count, j * LANES : (j + 1) * LANES] = block.astype(
                slots_ref.dtype
            )
    routed = mul(placing_ref[...], slots_ref[...], by_rows)
    mid = (cot_ref[...].astype(jnp.float32) + routed).astype(jnp.bfloat16)
    near, core = near_ref[0], core_ref[0]
    lane = places((1, width), 1)
    per_block = 2 * PIECE
    block, inside = lane // per_block, lane % per_block
    step_near, step_core = block // 2, block % 2
    far, row = inside // PIECE, inside % PIECE
    source = (
        far * (width // 2) + (near + step_near) % 4 * per_block + (core + step_core) % 2 * PIECE + row
    )
    moved = (places((width, width), 0) == source).astype(jnp.float32).astype(jnp.bfloat16)
    out_ref[...] = mul(mid, moved).astype(out_ref.dtype)


def weight_kernel(mine_ref, other_ref, out_ref, sems):
    steps, tp_count = 4, 4
    per_tp = mine_ref.shape[0] // (tp_count * steps * PIECE)
    copies = []
    for q in range(tp_count):
        for step in range(steps):
            for core, ref in enumerate((mine_ref, other_ref)):
                for far in range(per_tp):
                    source = ((q * per_tp + far) * steps + step) * PIECE
                    target = (((q * steps + step) * 2 + core) * per_tp + far) * PIECE
                    copies.append(
                        pltpu.make_async_copy(
                            ref.at[pl.ds(source, PIECE), :],
                            out_ref.at[pl.ds(target, PIECE), :],
                            sems.at[len(copies)],
                        )
                    )
    for copy in copies:
        copy.start()
    for copy in copies:
        copy.wait()


def ordered_weight(mine, other):
    far_spec = pl.BlockSpec(memory_space=pltpu.HBM)
    rows, width = mine.shape
    return pl.pallas_call(
        weight_kernel,
        out_shape=jax.ShapeDtypeStruct((2 * rows, width), mine.dtype),
        in_specs=[far_spec, far_spec],
        out_specs=pl.BlockSpec(memory_space=pltpu.VMEM),
        scratch_shapes=[pltpu.SemaphoreType.DMA((2 * rows // PIECE,))],
        compiler_params=pltpu.CompilerParams(vmem_limit_bytes=GRANT),
        name="weight_kernel",
    )(in_hbm(mine), in_hbm(other))


def spread_kernel(*refs):
    mid_refs, out_refs = refs[:4], refs[4:]
    width = mid_refs[0].shape[1] // len(out_refs)
    for j, out_ref in enumerate(out_refs):
        for k, mid_ref in enumerate(mid_refs):
            out_ref[:, k * width : (k + 1) * width] = mid_ref[:, j * width : (j + 1) * width]


def put_state(out_ref, group, part):
    rows = part.shape[0] // 2
    tiles = part.reshape(rows // SUB, 2, SUB, NS)
    for k in range(2):
        out_ref[group * rows : (group + 1) * rows, k * NS : (k + 1) * NS] = (
            tiles[:, k].reshape(rows, NS).astype(out_ref.dtype)
        )


def get_state(ref, group, groups):
    rows = ref.shape[0] // groups
    halves = [
        ref[group * rows : (group + 1) * rows, k * NS : (k + 1) * NS]
        .astype(jnp.float32)
        .reshape(rows // SUB, SUB, NS)
        for k in range(2)
    ]
    return jnp.stack(halves, axis=1).reshape(2 * rows, NS)


def mix_kernel(got_ref, out_ref, back_ref, rest_ref):
    count = got_ref.shape[0]
    devices = count // SUB
    state = got_ref[:, : 2 * NS]
    shape = (devices, count)
    chosen = (places(shape, 1) == SUB * places(shape, 0)).astype(jnp.float32).astype(jnp.bfloat16)
    parts = mul(chosen, got_ref[:, 2 * NS :])
    logs = jnp.sum(jnp.where(places(parts.shape, 1) < 3, parts, 0.0), axis=1, keepdims=True)
    log = jnp.broadcast_to(logs, parts.shape)
    small = (devices, devices)
    one, two = places(small, 0), places(small, 1)
    through = mul((one >= two).astype(jnp.float32), log, precision=exact)
    before = through - log
    through_row = mul(log, (one <= two).astype(jnp.float32), by_rows, precision=exact)[:1]
    before_row = mul(log, (one < two).astype(jnp.float32), by_rows, precision=exact)[:1]
    tall = (count, devices)
    copies = (places(tall, 0) // SUB == places(tall, 1)).astype(jnp.float32).astype(jnp.bfloat16)
    square = (count, count)
    same = places(square, 0) % SUB == places(square, 1) % SUB

    def spread(weights):
        wide = mul(mul(copies, weights).astype(jnp.bfloat16), copies, by_cols)
        return jnp.where(same, wide, 0.0).astype(jnp.bfloat16)

    def split(spans, mask):
        weights = jnp.exp(jnp.where(mask, spans, -jnp.inf))
        high = weights.astype(jnp.bfloat16)
        return spread(high), spread((weights - high.astype(jnp.float32)).astype(jnp.bfloat16))

    high, low = split(before[:, :1] - through_row, two < one)
    out_ref[...] = (mul(high, state) + mul(low, state)).astype(out_ref.dtype)
    back_ref[...], rest_ref[...] = split(before_row - through[:, :1], one < two)


def mix_back_kernel(got_ref, back_ref, rest_ref, out_ref):
    state = got_ref[...]
    out_ref[...] = (mul(back_ref[...], state) + mul(rest_ref[...], state)).astype(out_ref.dtype)


def state_kernel(x_ref, b_ref, log_ref, out_ref):
    log = log_ref[...]
    width = x_ref.shape[1]
    cum, _ = running(log)
    scaled = (x_ref[...].astype(jnp.float32) * to_end_wide(cum, width)).astype(jnp.bfloat16)
    groups = b_ref.shape[1] // NS
    each = width // groups
    for g in range(groups):
        part = mul(scaled[:, g * each : (g + 1) * each], b_ref[:, g * NS : (g + 1) * NS], by_rows)
        put_state(out_ref, g, part)
    rows, heads = out_ref.shape[0], log.shape[0]
    shape = (rows, heads)
    owner = places(shape, 0) // (rows // heads) == places(shape, 1)
    total = jnp.sum(jnp.where(owner, cum[-1:, :], 0.0), axis=1, keepdims=True)
    high = total.astype(jnp.bfloat16).astype(jnp.float32)
    middle = (total - high).astype(jnp.bfloat16).astype(jnp.float32)
    low = total - high - middle
    lane = places((rows, NS), 1)
    out_ref[:, 2 * NS :] = jnp.where(
        lane == 0, high, jnp.where(lane == 1, middle, jnp.where(lane == 2, low, 0.0))
    ).astype(out_ref.dtype)


def decays(cum, cum_row, head):
    length = cum.shape[0]
    shape = (length, length)
    spans = cum[:, head : head + 1] - cum_row[head : head + 1, :]
    return jnp.exp(jnp.where(places(shape, 0) >= places(shape, 1), spans, -jnp.inf))


def half_masks(length):
    lane = places((length, 2 * HEAD_DIM), 1)
    return (lane < HEAD_DIM, lane >= HEAD_DIM)


def forward_kernel(x_ref, b_ref, c_ref, log_ref, z_ref, entry_ref, y_ref, half_ref):
    log = log_ref[...]
    heads, length = log.shape
    width = x_ref.shape[1]
    groups = b_ref.shape[1] // NS
    each = width // groups
    per_group = heads // groups
    cum, cum_row = running(log)
    from_start = mul(jnp.exp(cum), head_spread(heads, width), precision=exact)
    masks = half_masks(length)
    zero = jnp.zeros((length, 2 * HEAD_DIM), jnp.bfloat16)
    for g in range(groups):
        c_group = c_ref[:, g * NS : (g + 1) * NS]
        scores = mul(c_group, b_ref[:, g * NS : (g + 1) * NS], by_cols)
        carried = mul(c_group, get_state(entry_ref, g, groups).astype(jnp.bfloat16), by_cols)
        pieces = []
        for pair in range(per_group // 2):
            head = g * per_group + 2 * pair
            x_pair = x_ref[:, head * HEAD_DIM : (head + 2) * HEAD_DIM]
            total = None
            for k in range(2):
                weights = (scores * decays(cum, cum_row, head + k)).astype(jnp.bfloat16)
                part = mul(weights, jnp.where(masks[k], x_pair, zero))
                total = part if total is None else total + part
            pieces.append(total)
        cols = slice(g * each, (g + 1) * each)
        y = jnp.concatenate(pieces, axis=1) + carried * from_start[:, cols]
        z = z_ref[:, cols].astype(jnp.float32)
        gated = y * (z * jax.nn.sigmoid(z))
        mean = jnp.mean(gated * gated, axis=1, keepdims=True)
        y_ref[:, cols] = y
        half_ref[:, cols] = (gated * lax.rsqrt(mean + epsilon)).astype(half_ref.dtype)


def gate_kernel(rank_ref, m0, m1, m2, m3, w_ref, y_ref, z_ref, c_ref, log_ref, dy_ref, dz_ref, out_ref):
    log = log_ref[...]
    heads = log.shape[0]
    width = y_ref.shape[1]
    groups = c_ref.shape[1] // NS
    each = width // groups
    cum, _ = running(log)
    from_start = mul(jnp.exp(cum), head_spread(heads, width), precision=exact)
    mid_refs = (m0, m1, m2, m3)
    parts, rows = len(mid_refs), m0.shape[1]
    for g in range(groups):
        cols = slice(g * each, (g + 1) * each)
        d_normed = None
        for step in range(parts):
            block = pl.ds(block_of(rank_ref[0], step, parts, rows), rows)
            part = mul(mid_refs[step][...], w_ref[block, cols])
            d_normed = part if d_normed is None else d_normed + part
        y = y_ref[:, cols]
        z = z_ref[:, cols].astype(jnp.float32)
        sig = jax.nn.sigmoid(z)
        silu = z * sig
        gated = y * silu
        inverse = lax.rsqrt(jnp.mean(gated * gated, axis=1, keepdims=True) + epsilon)
        normed = gated * inverse
        along = jnp.mean(d_normed * normed, axis=1, keepdims=True)
        d_gated = inverse * (d_normed - normed * along)
        d_y = d_gated * silu
        dy_ref[:, cols] = d_y.astype(dy_ref.dtype)
        dz_ref[:, cols] = (d_gated * y * (sig * (1.0 + z * (1.0 - sig)))).astype(dz_ref.dtype)
        scaled = (d_y * from_start[:, cols]).astype(jnp.bfloat16)
        part = mul(scaled, c_ref[:, g * NS : (g + 1) * NS], by_rows)
        put_state(out_ref, g, part)


def within_kernel(
    dy_ref, x_ref, b_ref, c_ref, log_ref, entry_ref, dx_ref, db_ref, dc_ref, dlog_ref
):
    log = log_ref[...]
    heads, length = log.shape
    groups = b_ref.shape[1] // NS
    per_group = heads // groups
    cum, cum_row = running(log)
    start = jnp.exp(cum)
    masks = half_masks(length)
    zero = jnp.zeros((length, 2 * HEAD_DIM), jnp.bfloat16)
    d_cum = jnp.zeros((length, heads), jnp.float32)
    d_row = jnp.zeros((heads, length), jnp.float32)
    head_col = places((length, heads), 1)
    head_row = places((heads, length), 0)
    for g in range(groups):
        c_group = c_ref[:, g * NS : (g + 1) * NS]
        b_group = b_ref[:, g * NS : (g + 1) * NS]
        c_wide = c_group.astype(jnp.float32)
        scores = mul(c_group, b_group, by_cols)
        d_scores = jnp.zeros((length, length), jnp.float32)
        d_c = jnp.zeros((length, NS), jnp.float32)
        entry = get_state(entry_ref, g, groups).astype(jnp.bfloat16)
        for pair in range(per_group // 2):
            head = g * per_group + 2 * pair
            cols = slice(head * HEAD_DIM, (head + 2) * HEAD_DIM)
            x_pair = x_ref[:, cols]
            dy_pair = dy_ref[:, cols]
            entry_pair = entry[2 * pair * HEAD_DIM : (2 * pair + 2) * HEAD_DIM, :]
            d_x = None
            for k in range(2):
                decay = decays(cum, cum_row, head + k)
                dy_one = jnp.where(masks[k], dy_pair, zero)
                weights = scores * decay
                d_weights = mul(dy_one, x_pair, by_cols)
                part = mul(weights.astype(jnp.bfloat16), dy_one, by_rows)
                d_x = part if d_x is None else d_x + part
                d_scores = d_scores + d_weights * decay
                spread = d_weights * weights
                from_entry = mul(dy_one, entry_pair) * start[:, head + k : head + k + 1]
                d_c = d_c + from_entry
                rows = jnp.sum(spread + c_wide * from_entry, axis=1, keepdims=True)
                d_cum = jnp.where(head_col == head + k, rows, d_cum)
                d_row = jnp.where(
                    head_row == head + k, jnp.sum(spread, axis=0, keepdims=True), d_row
                )
            dx_ref[:, cols] = d_x
        half = d_scores.astype(jnp.bfloat16)
        dc_ref[:, g * NS : (g + 1) * NS] = d_c + mul(half, b_group)
        db_ref[:, g * NS : (g + 1) * NS] = mul(half, c_group, by_rows)
    shape = (length, length)
    upper = (places(shape, 0) <= places(shape, 1)).astype(jnp.float32)
    dlog_ref[...] = mul(upper, d_cum, precision=exact) - mul(upper, d_row, by_cols, precision=exact)


def final_kernel(
    x_ref,
    b_ref,
    log_ref,
    grad_ref,
    entry_ref,
    dx_ref,
    db_ref,
    dlog_ref,
    out_ref,
    gx_ref,
    gb_ref,
    glog_ref,
    gout_ref,
):
    gout_ref[...] = out_ref[...].astype(jnp.float32)
    log = log_ref[...]
    heads, length = log.shape
    width = x_ref.shape[1]
    groups = b_ref.shape[1] // NS
    each = width // groups
    cum, _ = running(log)
    spread = head_spread(heads, width)
    to_end = to_end_wide(cum, width)
    x = x_ref[...].astype(jnp.float32)
    scaled = (x * to_end).astype(jnp.bfloat16)
    moved = jnp.zeros((length, heads), jnp.float32)
    ones = jnp.ones((8, NS), jnp.float32)
    kept = jnp.zeros((8, heads), jnp.float32)
    for g in range(groups):
        cols = slice(g * each, (g + 1) * each)
        grad_wide = get_state(grad_ref, g, groups)
        grad = grad_wide.astype(jnp.bfloat16)
        d_x = mul(b_ref[:, g * NS : (g + 1) * NS], grad, by_cols) * to_end[:, cols]
        gx_ref[:, cols] = (dx_ref[:, cols] + d_x).astype(gx_ref.dtype)
        moved = moved + mul(x[:, cols] * d_x, spread[:, cols], by_cols, precision=exact)
        gb_ref[:, g * NS : (g + 1) * NS] = db_ref[:, g * NS : (g + 1) * NS] + mul(
            scaled[:, cols], grad
        )
        both = get_state(entry_ref, g, groups) * grad_wide
        kept = kept + mul(
            mul(ones, both, by_cols, precision=exact), spread[:, cols], by_cols, precision=exact
        )
    shape = (length, length)
    earlier = (places(shape, 0) > places(shape, 1)).astype(jnp.float32)
    total = dlog_ref[...] + mul(earlier, moved, precision=exact) + kept[:1, :] * jnp.exp(cum[-1:, :])
    same = (places(shape, 0) == places(shape, 1)).astype(jnp.float32)
    glog_ref[...] = mul(total, same, by_rows, precision=exact)


def out_grad_kernel(rank_ref, near_ref, core_ref, *refs):
    mid_refs, half_ref, out_ref = refs[:-2], refs[-2], refs[-1]
    near_count = len(mid_refs) // 2
    total = None
    for j, mid_ref in enumerate(mid_refs):
        near = lax.rem(near_ref[0] + near_count - j // 2, near_count)
        core = lax.rem(core_ref[0] + j % 2, 2)
        part = mul(mid_ref[...], half_ref[near * 2 + core], by_rows)
        total = part if total is None else total + part
    parts = 4
    rows = total.shape[0] // parts
    for step in range(parts):
        block = pl.ds(block_of(rank_ref[0], step, parts, rows), rows)
        out_ref[block, :] = total[step * rows : (step + 1) * rows].astype(out_ref.dtype)


def in_hbm(array):
    return pltpu.with_memory_space_constraint(array, pltpu.HBM)


def call(kernel, shapes, *args, scratch=(), scalars=0, far=(), kept=()):
    near_spec = pl.BlockSpec(memory_space=pltpu.VMEM)
    far_spec = pl.BlockSpec(memory_space=pltpu.HBM)
    scalar = pl.BlockSpec(memory_space=pltpu.SMEM)
    n_in, n_out = len(args), len(shapes)
    staged = [(args[i].shape, args[i].dtype) for i in far] + [shapes[i] for i in kept]

    def body(*refs):
        ins, outs = list(refs[:n_in]), list(refs[n_in : n_in + n_out])
        own = refs[n_in + n_out :]
        stage, sems = own[len(scratch) : len(scratch) + len(staged)], own[-1]
        fetches = []
        for k, i in enumerate(far):
            fetches.append(pltpu.make_async_copy(ins[i], stage[k], sems.at[k]))
            fetches[-1].start()
            ins[i] = stage[k]
        for fetch in fetches:
            fetch.wait()
        writes = []
        for k, i in enumerate(kept, len(far)):
            writes.append(pltpu.make_async_copy(stage[k], outs[i], sems.at[k]))
            outs[i] = stage[k]
        kernel(*ins, *outs, *own[: len(scratch)])
        for write in writes:
            write.start()
        for write in writes:
            write.wait()

    spaces = [far_spec if i in far else near_spec for i in range(n_in)]
    return pl.pallas_call(
        body,
        out_shape=tuple(
            pltpu.HBM(s, d) if i in kept else jax.ShapeDtypeStruct(s, d)
            for i, (s, d) in enumerate(shapes)
        ),
        in_specs=[scalar if i < scalars else spaces[i] for i in range(n_in)],
        out_specs=tuple(far_spec if i in kept else near_spec for i in range(n_out)),
        scratch_shapes=[pltpu.VMEM(s, d) for s, d in (*scratch, *staged)]
        + [pltpu.SemaphoreType.DMA((max(len(staged), 1),))],
        compiler_params=pltpu.CompilerParams(vmem_limit_bytes=GRANT),
    )(*(in_hbm(arg) if i in far else arg for i, arg in enumerate(args)))


def swap(array, axis):
    return lax.all_to_all(array, axis, split_axis=0, concat_axis=0, tiled=True)


def moved(array, axis, step):
    count = lax.axis_size(axis)
    return lax.ppermute(array, axis, [((i + step) % count, i) for i in range(count)])


def from_others(array, axis):
    return [array] + [moved(array, axis, step) for step in (1, 2, 3)]


def local(
    hidden_rows,
    out_cot,
    routes,
    route_weight,
    gate_w,
    up_w,
    down_w,
    out_weight,
    step_inputs,
    input_map,
    output_map,
    log_decay,
    gate_z,
):
    f32, bf16 = jnp.float32, jnp.bfloat16
    inner = step_inputs.shape[1]
    maps = input_map.shape[1]
    sp_count, tp_count = lax.axis_size(SP), lax.axis_size("tp")
    width = hidden_rows.shape[1]
    slots = sp_count * CAP
    back_tiles = -(-CAP * width // (LANES * SUB))
    pieces = width // LANES
    hidden_units = gate_w.shape[2]
    full = width * tp_count

    length, heads = log_decay.shape
    log_decay = log_decay.T
    rank = lax.axis_index("tp").astype(jnp.int32)[None]
    near = lax.axis_index(NEAR).astype(jnp.int32)[None]
    core = lax.axis_index(CORE).astype(jnp.int32)[None]
    sent, placing = call(
        place_kernel,
        [((sp_count * 2 * pieces, CAP * LANES), bf16), ((slots, length), bf16)],
        routes.T,
        route_weight.T,
        hidden_rows,
        out_cot,
        scratch=[((CAP, sp_count * 2 * pieces, LANES), f32)],
        far=(0, 1, 2, 3), kept=(1,),
    )
    state_rows = inner // 2
    (own,) = call(
        state_kernel,
        [((state_rows, 3 * NS), bf16)],
        step_inputs,
        input_map,
        log_decay,
        far=(0, 1, 2),
    )
    near_pieces = from_others(out_weight, NEAR)
    got = swap(sent.reshape(sp_count, 2 * pieces, CAP * LANES), SP)
    rows, cot = call(
        arrange_kernel,
        [((slots, width), bf16)] * 2,
        got.reshape(sent.shape),
        scratch=[((CAP, sent.shape[0], LANES), f32)],
    )
    rows_next, rows_last = moved(rows, "tp", 1), moved(rows, "tp", -1)
    cot_next, cot_last = moved(cot, "tp", 1), moved(cot, "tp", -1)
    rows_far, cot_far = moved(rows_last, "tp", -1), moved(cot_next, "tp", 1)
    near_pieces, _ = lax.optimization_barrier((near_pieces, rows_last))
    near_weight = jnp.concatenate(near_pieces, axis=0)
    filled = (
        rows,
        rows_next,
        rows_far,
        rows_last,
        cot,
        cot_next,
        cot_far,
        cot_last,
    )
    half_weight = lax.all_gather(near_weight, FAR, axis=0, tiled=True)
    got_own = swap(own.reshape(sp_count, SUB, 3 * NS), SP).reshape(own.shape)
    mixed, back, rest = call(
        mix_kernel,
        [((state_rows, 2 * NS), bf16)] + [((state_rows, state_rows), bf16)] * 2,
        got_own,
        kept=(1, 2),
    )
    filled, mixed = lax.optimization_barrier((filled, mixed))
    hidden, d_gate, d_up, *partials = call(
        expert_kernel,
        [((slots, hidden_units), bf16)] * 3 + [((slots, width), bf16)] * tp_count,
        rank,
        *filled,
        gate_w[0],
        up_w[0],
        down_w[0],
        scalars=1,
        far=(9, 10, 11), kept=(0, 1, 2),
    )
    received = [partials[0]] + [moved(partials[step], "tp", -step) for step in (1, 2, 3)]
    entry = swap(mixed.reshape(sp_count, SUB, 2 * NS), SP).reshape(mixed.shape)
    (summed,) = call(
        add_kernel,
        [((sp_count * SUB, back_tiles * LANES), bf16)],
        *received,
        scratch=[((back_tiles, sp_count * SUB, LANES), f32)],
    )
    half_weight, _ = lax.optimization_barrier((half_weight, summed))
    other_weight = moved(half_weight, CORE, 1)
    full_weight = ordered_weight(half_weight, other_weight)
    grad_gate, grad_up, grad_down = call(
        weight_grad_kernel,
        [((full, hidden_units), f32)] * 2 + [((hidden_units, full), f32)],
        rank,
        *filled,
        hidden,
        d_gate,
        d_up,
        scalars=1,
        far=(9, 10, 11), kept=(0, 1, 2),
    )
    returned = swap(summed.reshape(sp_count, SUB, back_tiles * LANES), SP).reshape(summed.shape)
    (mid_part,) = call(
        mid_kernel,
        [((length, width), bf16)],
        near,
        core,
        returned,
        placing,
        out_cot,
        scratch=[((back_tiles, summed.shape[0], LANES), f32), ((slots, width), bf16)],
        scalars=2,
        far=(3, 4),
    )
    mids = from_others(mid_part, "tp")
    y, half = call(
        forward_kernel,
        [((length, inner), f32), ((length, inner), bf16)],
        step_inputs,
        input_map,
        output_map,
        log_decay,
        gate_z,
        entry,
        far=(0, 1, 2, 3, 4, 5), kept=(0, 1),
    )
    halves = lax.all_gather(half, (NEAR, CORE), axis=0)
    d_y, grad_z, entry_grad = call(
        gate_kernel,
        [((length, inner), bf16)] * 2 + [((state_rows, 2 * NS), bf16)],
        rank,
        *mids,
        full_weight,
        y,
        gate_z,
        output_map,
        log_decay,
        scalars=1,
        far=(6, 7, 8, 9), kept=(0, 1),
    )
    got_grad = swap(entry_grad.reshape(sp_count, SUB, 2 * NS), SP).reshape(entry_grad.shape)
    (mixed_grad,) = call(
        mix_back_kernel, [((state_rows, 2 * NS), bf16)], got_grad, back, rest, far=(1, 2)
    )
    carried = swap(mixed_grad.reshape(sp_count, SUB, 2 * NS), SP).reshape(mixed_grad.shape)
    near_count = lax.axis_size(NEAR)
    blocks = call(
        spread_kernel,
        [((length, full // (2 * near_count)), bf16)] * (2 * near_count),
        *mids,
    )
    mids_here = []
    for step in range(near_count):
        for side in range(2):
            pairs = [
                (
                    n * 2 + c,
                    (n + step) % near_count * 2 + (c + side) % 2,
                )
                for n in range(near_count)
                for c in range(2)
            ]
            block = blocks[step * 2 + side]
            if step or side:
                block = lax.ppermute(block, (NEAR, CORE), pairs)
            mids_here.append(block)
    mids_here, _ = lax.optimization_barrier((mids_here, entry_grad))
    (out_grad,) = call(
        out_grad_kernel,
        [((full // (2 * near_count), inner), bf16)],
        rank,
        near,
        core,
        *mids_here,
        halves,
        scalars=3,
        far=(11,), kept=(0,),
    )
    out_part = lax.psum_scatter(out_grad, FAR, scatter_dimension=0, tiled=True)
    d_x, d_b, grad_out_map, d_log = call(
        within_kernel,
        [((length, inner), f32), ((length, maps), f32), ((length, maps), f32), ((length, heads), f32)],
        d_y,
        step_inputs,
        input_map,
        output_map,
        log_decay,
        entry,
        far=(0, 1, 2, 3, 4, 5), kept=(2,),
    )
    grad_step, grad_in_map, grad_log, grad_out_weight = call(
        final_kernel,
        [((length, inner), bf16), ((length, maps), f32), ((heads, length), f32), (out_part.shape, f32)],
        step_inputs,
        input_map,
        log_decay,
        carried,
        entry,
        d_x,
        d_b,
        d_log,
        out_part,
        far=(0, 1, 2, 4, 8), kept=(0, 1, 2, 3),
    )
    return (
        grad_gate[None],
        grad_up[None],
        grad_down[None],
        grad_out_weight,
        grad_step,
        grad_z,
        grad_in_map,
        grad_out_map,
        grad_log.T,
    )


def solution(mesh):
    torus = Mesh(mesh.devices.reshape(8, 4, 2, mesh.shape["tp"]), ("sp_0", "sp_1", "sp_2", "tp"))
    placed = (
        P(SP, "tp"),
        P(SP, "tp"),
        P(SP, None),
        P(SP, None),
        P(SP, None, "tp"),
        P(SP, None, "tp"),
        P(SP, "tp", None),
        P(SP, "tp"),
        P(SP, "tp"),
        P(SP, "tp"),
        P(SP, "tp"),
        P(SP, "tp"),
        P(SP, "tp"),
    )
    return jax.shard_map(
        local,
        mesh=torus,
        in_specs=placed,
        out_specs=(
            P(SP, None, "tp"),
            P(SP, None, "tp"),
            P(SP, "tp", None),
            P(SP, "tp"),
            P(SP, "tp"),
            P(SP, "tp"),
            P(SP, "tp"),
            P(SP, "tp"),
            P(SP, "tp"),
        ),
        check_vma=False,
    )
```

```python
import jax
import jax.numpy as jnp
from jax import lax
from jax.experimental import pallas as pl
from jax.experimental.pallas import tpu as pltpu
from jax.sharding import Mesh
from jax.sharding import PartitionSpec as P


SP = ("sp_0", "sp_1", "sp_2")
FAR, NEAR, CORE = SP
CAP = 5
SUB = 8
GRANT = 16 * 1024 * 1024
PIECE = 32
LANES = 128
HEAD_DIM = 64
NS = 128
epsilon = 1e-06
exact = lax.Precision.HIGHEST
by_rows = (((0,), (0,)), ((), ()))
by_cols = (((1,), (1,)), ((), ()))


def mul(a, b, dims=None, precision=None):
    dims = (((1,), (0,)), ((), ())) if dims is None else dims
    return lax.dot_general(a, b, dims, precision=precision, preferred_element_type=jnp.float32)


def places(shape, dim):
    return lax.broadcasted_iota(jnp.int32, shape, dim)


def head_spread(heads, width):
    shape = (heads, width)
    return (places(shape, 1) // HEAD_DIM == places(shape, 0)).astype(jnp.float32)


def running(log):
    length = log.shape[1]
    shape = (length, length)
    lower = (places(shape, 0) >= places(shape, 1)).astype(jnp.float32)
    return mul(lower, log, by_cols, precision=exact), mul(log, lower, by_cols, precision=exact)


def to_end_wide(cum, width):
    last = cum[-1:, :]
    return mul(jnp.exp(last - cum), head_spread(cum.shape[1], width), precision=exact)


def gather_cells(wide_ref, out_ref, count):
    for tile in range(out_ref.shape[1] // LANES):
        for first in range(0, count, 2):
            rows = jnp.concatenate(
                [
                    wide_ref[pl.ds(tile * SUB * count + first + k, SUB, stride=count), :]
                    for k in range(2)
                ],
                axis=0,
            )
            out_ref[first * SUB : (first + 2) * SUB, tile * LANES : (tile + 1) * LANES] = rows.astype(
                out_ref.dtype
            )


def place_kernel(routes_ref, weight_ref, rows_ref, cot_ref, out_ref, placing_ref, wide_ref):
    top, length = routes_ref.shape
    experts = placing_ref.shape[0] // CAP
    shape = (experts, length)
    expert = places(shape, 0)
    hits = [routes_ref[k : k + 1, :] == expert for k in range(top)]
    named = hits[0]
    for k in range(1, top):
        named = jnp.logical_or(named, hits[k])
    square = (length, length)
    sooner = (places(square, 0) < places(square, 1)).astype(jnp.bfloat16)
    taken = mul(named.astype(jnp.bfloat16), sooner)
    ranks = [jnp.sum(jnp.where(h, taken, 0.0), axis=0, keepdims=True) for h in hits]
    rows, cot = rows_ref[...], cot_ref[...]
    width = rows.shape[1]
    pieces = 2 * width // LANES
    for slot in range(CAP):
        here = [jnp.logical_and(hits[k], ranks[k] == float(slot)) for k in range(top)]
        weight = jnp.zeros((experts, 1), jnp.float32)
        for k in range(top):
            weight = weight + jnp.sum(
                jnp.where(here[k], weight_ref[k : k + 1, :], 0.0), axis=1, keepdims=True
            )
        chosen = here[0]
        for k in range(1, top):
            chosen = jnp.logical_or(chosen, here[k])
        chosen = chosen.astype(jnp.float32).astype(jnp.bfloat16)
        placing_ref[slot * experts : (slot + 1) * experts, :] = chosen
        both = (mul(chosen, rows), mul(chosen, cot) * weight)
        for j in range(pieces):
            source = both[j * LANES // width]
            start = j * LANES % width
            cell = (slot * pieces + j) * experts
            wide_ref[cell : cell + experts, :] = source[:, start : start + LANES]
    gather_cells(wide_ref, out_ref, experts)


def arrange_kernel(got_ref, rows_ref, cot_ref, wide_ref):
    for slot in range(CAP):
        wide_ref[slot] = got_ref[:, slot * LANES : (slot + 1) * LANES].astype(jnp.float32)
    slots, width = rows_ref.shape
    count = slots // CAP
    pieces = 2 * width // LANES
    for slot in range(CAP):
        for j in range(pieces):
            block = wide_ref[slot, pl.ds(j, count, stride=pieces), :]
            out_ref = rows_ref if j * LANES < width else cot_ref
            start = j * LANES % width
            out_ref[slot * count : (slot + 1) * count, start : start + LANES] = block.astype(
                out_ref.dtype
            )


def block_of(rank, step, parts, width):
    return pl.multiple_of(lax.rem(rank + step, parts) * width, width)


def expert_kernel(rank_ref, *refs):
    parts = (len(refs) - 6) // 3
    rows_refs, cot_refs, part_refs = refs[:parts], refs[parts : 2 * parts], refs[-parts:]
    gate_ref, up_ref, down_ref, hidden_ref, dgate_ref, dup_ref = refs[2 * parts : -parts]
    _, width = rows_refs[0].shape
    gate_pre = up_pre = d_act = None
    for step in range(parts):
        block = pl.ds(block_of(rank_ref[0], step, parts, width), width)
        rows, cot = rows_refs[step][...], cot_refs[step][...]
        one, two = mul(rows, gate_ref[block, :]), mul(rows, up_ref[block, :])
        three = mul(cot, down_ref[:, block], by_cols)
        gate_pre = one if step == 0 else gate_pre + one
        up_pre = two if step == 0 else up_pre + two
        d_act = three if step == 0 else d_act + three
    sig = jax.nn.sigmoid(gate_pre)
    hidden_ref[...] = (gate_pre * sig * up_pre).astype(jnp.bfloat16)
    d_gate = (d_act * up_pre * sig * (1.0 + gate_pre * (1.0 - sig))).astype(jnp.bfloat16)
    d_up = (d_act * gate_pre * sig).astype(jnp.bfloat16)
    dgate_ref[...] = d_gate
    dup_ref[...] = d_up
    for step in range(parts):
        block = pl.ds(block_of(rank_ref[0], step, parts, width), width)
        part = mul(d_gate, gate_ref[block, :], by_cols) + mul(d_up, up_ref[block, :], by_cols)
        part_refs[step][...] = part.astype(part_refs[step].dtype)


def weight_grad_kernel(rank_ref, *refs):
    parts = (len(refs) - 6) // 2
    rows_refs, cot_refs = refs[:parts], refs[parts : 2 * parts]
    hidden_ref, dgate_ref, dup_ref, gate_ref, up_ref, down_ref = refs[2 * parts :]
    width = rows_refs[0].shape[1]
    for step in range(parts):
        block = pl.ds(block_of(rank_ref[0], step, parts, width), width)
        rows, cot = rows_refs[step][...], cot_refs[step][...]
        gate_ref[block, :] = mul(rows, dgate_ref[...], by_rows)
        up_ref[block, :] = mul(rows, dup_ref[...], by_rows)
        down_ref[:, block] = mul(hidden_ref[...], cot, by_rows)


def add_kernel(one_ref, two_ref, three_ref, four_ref, out_ref, wide_ref):
    slots, width = one_ref.shape
    total = one_ref[...].astype(jnp.float32)
    for got_ref in (two_ref, three_ref, four_ref):
        total = total + got_ref[...].astype(jnp.float32)
    count = slots // CAP
    pieces = width // LANES
    used = CAP * pieces * count
    wide_ref[used:, :] = jnp.zeros((wide_ref.shape[0] - used, LANES), jnp.float32)
    for slot in range(CAP):
        for j in range(pieces):
            cell = (slot * pieces + j) * count
            wide_ref[cell : cell + count, :] = total[
                slot * count : (slot + 1) * count, j * LANES : (j + 1) * LANES
            ]
    gather_cells(wide_ref, out_ref, count)


def mid_kernel(near_ref, core_ref, back_ref, placing_ref, cot_ref, out_ref, wide_ref, slots_ref):
    for tile in range(wide_ref.shape[0]):
        wide_ref[tile] = back_ref[:, tile * LANES : (tile + 1) * LANES].astype(jnp.float32)
    slots, width = slots_ref.shape
    count = slots // CAP
    pieces = width // LANES
    for slot in range(CAP):
        for j in range(pieces):
            tile, row = divmod(slot * pieces + j, SUB)
            block = wide_ref[tile, pl.ds(row, count, stride=SUB), :]
            slots_ref[slot * count : (slot + 1) * count, j * LANES : (j + 1) * LANES] = block.astype(
                slots_ref.dtype
            )
    routed = mul(placing_ref[...], slots_ref[...], by_rows)
    mid = (cot_ref[...].astype(jnp.float32) + routed).astype(jnp.bfloat16)
    near, core = near_ref[0], core_ref[0]
    lane = places((1, width), 1)
    per_block = 2 * PIECE
    block, inside = lane // per_block, lane % per_block
    step_near, step_core = block // 2, block % 2
    far, row = inside // PIECE, inside % PIECE
    source = (
        far * (width // 2) + (near + step_near) % 4 * per_block + (core + step_core) % 2 * PIECE + row
    )
    moved = (places((width, width), 0) == source).astype(jnp.float32).astype(jnp.bfloat16)
    out_ref[...] = mul(mid, moved).astype(out_ref.dtype)


def weight_kernel(
    mine_ref, other_ref, y_ref, z_ref, c_ref, log_ref, out_ref, y_out, z_out, c_out, wide_ref, log, sems
):
    steps, tp_count = 4, 4
    per_tp = mine_ref.shape[0] // (tp_count * steps * PIECE)
    copies = []
    for q in range(tp_count):
        for step in range(steps):
            for core, ref in enumerate((mine_ref, other_ref)):
                for far in range(per_tp):
                    source = ((q * per_tp + far) * steps + step) * PIECE
                    target = (((q * steps + step) * 2 + core) * per_tp + far) * PIECE
                    copies.append(
                        pltpu.make_async_copy(
                            ref.at[pl.ds(source, PIECE), :],
                            out_ref.at[pl.ds(target, PIECE), :],
                            sems.at[len(copies)],
                        )
                    )
    extra = ((log_ref, log), (y_ref, y_out), (z_ref, z_out), (c_ref, c_out))
    moves = [
        pltpu.make_async_copy(source, target, sems.at[len(copies) + k])
        for k, (source, target) in enumerate(extra)
    ]
    for copy in moves + copies:
        copy.start()
    moves[0].wait()
    cum, _ = running(log[...])
    heads, width = log.shape[0], wide_ref.shape[1]
    wide_ref[...] = mul(jnp.exp(cum), head_spread(heads, width), precision=exact)
    for copy in moves[1:] + copies:
        copy.wait()


def ordered_weight(mine, other, y, z, c, log):
    far_spec = pl.BlockSpec(memory_space=pltpu.HBM)
    rows, width = mine.shape
    near_spec = pl.BlockSpec(memory_space=pltpu.VMEM)
    shapes = [((2 * rows, width), mine.dtype)]
    shapes += [(a.shape, a.dtype) for a in (y, z, c)] + [(y.shape, jnp.float32)]
    return pl.pallas_call(
        weight_kernel,
        out_shape=tuple(jax.ShapeDtypeStruct(s, d) for s, d in shapes),
        in_specs=[far_spec] * 6,
        out_specs=(near_spec,) * len(shapes),
        scratch_shapes=[
            pltpu.VMEM(log.shape, log.dtype),
            pltpu.SemaphoreType.DMA((2 * rows // PIECE + 4,)),
        ],
        compiler_params=pltpu.CompilerParams(vmem_limit_bytes=GRANT),
        name="weight_kernel",
    )(*(in_hbm(a) for a in (mine, other, y, z, c, log)))


def spread_kernel(*refs):
    mid_refs, out_refs = refs[:4], refs[4:]
    width = mid_refs[0].shape[1] // len(out_refs)
    for j, out_ref in enumerate(out_refs):
        for k, mid_ref in enumerate(mid_refs):
            out_ref[:, k * width : (k + 1) * width] = mid_ref[:, j * width : (j + 1) * width]


def put_state(out_ref, group, part):
    rows = part.shape[0] // 2
    tiles = part.reshape(rows // SUB, 2, SUB, NS)
    for k in range(2):
        out_ref[group * rows : (group + 1) * rows, k * NS : (k + 1) * NS] = (
            tiles[:, k].reshape(rows, NS).astype(out_ref.dtype)
        )


def get_state(ref, group, groups):
    rows = ref.shape[0] // groups
    halves = [
        ref[group * rows : (group + 1) * rows, k * NS : (k + 1) * NS]
        .astype(jnp.float32)
        .reshape(rows // SUB, SUB, NS)
        for k in range(2)
    ]
    return jnp.stack(halves, axis=1).reshape(2 * rows, NS)


def mix_kernel(got_ref, out_ref, back_ref):
    count = got_ref.shape[0]
    devices = count // SUB
    state = got_ref[:, : 2 * NS]
    shape = (devices, count)
    chosen = (places(shape, 1) == SUB * places(shape, 0)).astype(jnp.float32).astype(jnp.bfloat16)
    parts = mul(chosen, got_ref[:, 2 * NS :])
    logs = jnp.sum(jnp.where(places(parts.shape, 1) < 3, parts, 0.0), axis=1, keepdims=True)
    log = jnp.broadcast_to(logs, parts.shape)
    small = (devices, devices)
    one, two = places(small, 0), places(small, 1)
    through = mul((one >= two).astype(jnp.float32), log, precision=exact)
    before = through - log
    through_row = mul(log, (one <= two).astype(jnp.float32), by_rows, precision=exact)[:1]
    before_row = mul(log, (one < two).astype(jnp.float32), by_rows, precision=exact)[:1]
    tall = (count, devices)
    copies = (places(tall, 0) // SUB == places(tall, 1)).astype(jnp.float32).astype(jnp.bfloat16)
    square = (count, count)
    same = places(square, 0) % SUB == places(square, 1) % SUB

    def spread(weights):
        wide = mul(mul(copies, weights).astype(jnp.bfloat16), copies, by_cols)
        return jnp.where(same, wide, 0.0).astype(jnp.bfloat16)

    def wide_weights(spans, mask):
        return spread(jnp.exp(jnp.where(mask, spans, -jnp.inf)).astype(jnp.bfloat16))

    weights = wide_weights(before[:, :1] - through_row, two < one)
    out_ref[...] = mul(weights, state).astype(out_ref.dtype)
    back_ref[...] = wide_weights(before_row - through[:, :1], one < two)


def mix_back_kernel(got_ref, back_ref, out_ref):
    out_ref[...] = mul(back_ref[...], got_ref[...]).astype(out_ref.dtype)


def state_kernel(x_ref, b_ref, log_ref, out_ref):
    log = log_ref[...]
    width = x_ref.shape[1]
    cum, _ = running(log)
    scaled = (x_ref[...].astype(jnp.float32) * to_end_wide(cum, width)).astype(jnp.bfloat16)
    groups = b_ref.shape[1] // NS
    each = width // groups
    for g in range(groups):
        part = mul(scaled[:, g * each : (g + 1) * each], b_ref[:, g * NS : (g + 1) * NS], by_rows)
        put_state(out_ref, g, part)
    rows, heads = out_ref.shape[0], log.shape[0]
    shape = (rows, heads)
    owner = places(shape, 0) // (rows // heads) == places(shape, 1)
    total = jnp.sum(jnp.where(owner, cum[-1:, :], 0.0), axis=1, keepdims=True)
    high = total.astype(jnp.bfloat16).astype(jnp.float32)
    middle = (total - high).astype(jnp.bfloat16).astype(jnp.float32)
    low = total - high - middle
    lane = places((rows, NS), 1)
    out_ref[:, 2 * NS :] = jnp.where(
        lane == 0, high, jnp.where(lane == 1, middle, jnp.where(lane == 2, low, 0.0))
    ).astype(out_ref.dtype)


def head_column(values, head):
    return jnp.sum(jnp.where(places(values.shape, 1) == head, values, 0.0), axis=1, keepdims=True)


def decays(column, row):
    shape = (column.shape[0], row.shape[1])
    return jnp.exp(jnp.where(places(shape, 0) >= places(shape, 1), column - row, -jnp.inf))


def half_masks(length):
    lane = places((length, 2 * HEAD_DIM), 1)
    return (lane < HEAD_DIM, lane >= HEAD_DIM)


def forward_kernel(x_ref, b_ref, c_ref, log_ref, z_ref, entry_ref, y_ref, half_ref, row_ref):
    log = log_ref[...]
    heads, length = log.shape
    width = x_ref.shape[1]
    groups = b_ref.shape[1] // NS
    each = width // groups
    per_group = heads // groups
    cum, cum_row = running(log)
    row_ref[...] = cum_row
    from_start = mul(jnp.exp(cum), head_spread(heads, width), precision=exact)
    masks = half_masks(length)
    zero = jnp.zeros((length, 2 * HEAD_DIM), jnp.bfloat16)
    for g in range(groups):
        c_group = c_ref[:, g * NS : (g + 1) * NS]
        scores = mul(c_group, b_ref[:, g * NS : (g + 1) * NS], by_cols)
        carried = mul(c_group, get_state(entry_ref, g, groups).astype(jnp.bfloat16), by_cols)

        def pair_step(pair, carry):
            head = g * per_group + 2 * pair
            lanes = pl.ds(pl.multiple_of(head * HEAD_DIM, 2 * HEAD_DIM), 2 * HEAD_DIM)
            x_pair = x_ref[:, lanes]
            total = jnp.zeros((length, 2 * HEAD_DIM), jnp.float32)
            for k in range(2):
                decay = decays(head_column(cum, head + k), row_ref[pl.ds(head + k, 1), :])
                weights = (scores * decay).astype(jnp.bfloat16)
                total = total + mul(weights, jnp.where(masks[k], x_pair, zero))
            y_ref[:, lanes] = total
            return carry

        lax.fori_loop(0, per_group // 2, pair_step, 0)
        cols = slice(g * each, (g + 1) * each)
        y = y_ref[:, cols] + carried * from_start[:, cols]
        z = z_ref[:, cols].astype(jnp.float32)
        gated = y * (z * jax.nn.sigmoid(z))
        mean = jnp.mean(gated * gated, axis=1, keepdims=True)
        y_ref[:, cols] = y
        half_ref[:, cols] = (gated * lax.rsqrt(mean + epsilon)).astype(half_ref.dtype)


def gate_kernel(rank_ref, m0, m1, m2, m3, w_ref, y_ref, z_ref, c_ref, wide_ref, dy_ref, dz_ref, out_ref):
    width = y_ref.shape[1]
    groups = c_ref.shape[1] // NS
    each = width // groups
    mid_refs = (m0, m1, m2, m3)
    parts, rows = len(mid_refs), m0.shape[1]
    for g in range(groups):
        cols = slice(g * each, (g + 1) * each)
        d_normed = None
        for step in range(parts):
            block = pl.ds(block_of(rank_ref[0], step, parts, rows), rows)
            part = mul(mid_refs[step][...], w_ref[block, cols])
            d_normed = part if d_normed is None else d_normed + part
        y = y_ref[:, cols]
        z = z_ref[:, cols].astype(jnp.float32)
        sig = jax.nn.sigmoid(z)
        silu = z * sig
        gated = y * silu
        inverse = lax.rsqrt(jnp.mean(gated * gated, axis=1, keepdims=True) + epsilon)
        normed = gated * inverse
        along = jnp.mean(d_normed * normed, axis=1, keepdims=True)
        d_gated = inverse * (d_normed - normed * along)
        d_y = d_gated * silu
        dy_ref[:, cols] = d_y.astype(dy_ref.dtype)
        dz_ref[:, cols] = (d_gated * y * (sig * (1.0 + z * (1.0 - sig)))).astype(dz_ref.dtype)
        scaled = (d_y * wide_ref[:, cols]).astype(jnp.bfloat16)
        part = mul(scaled, c_ref[:, g * NS : (g + 1) * NS], by_rows)
        put_state(out_ref, g, part)


def within_kernel(
    dy_ref,
    x_ref,
    b_ref,
    c_ref,
    log_ref,
    entry_ref,
    dx_ref,
    db_ref,
    dc_ref,
    dlog_ref,
    scaled_ref,
    end_ref,
    b_out,
    entry_out,
    last_ref,
    state_ref,
    row_ref,
):
    log = log_ref[...]
    heads, length = log.shape
    width = x_ref.shape[1]
    groups = b_ref.shape[1] // NS
    per_group = heads // groups
    cum, cum_row = running(log)
    row_ref[...] = cum_row
    to_end = to_end_wide(cum, width)
    end_ref[...] = to_end
    scaled_ref[...] = (x_ref[...].astype(jnp.float32) * to_end).astype(scaled_ref.dtype)
    b_out[...] = b_ref[...]
    entry_out[...] = entry_ref[...]
    last_ref[...] = jnp.broadcast_to(jnp.exp(cum[-1:, :]), last_ref.shape)
    masks = half_masks(length)
    zero = jnp.zeros((length, 2 * HEAD_DIM), jnp.bfloat16)
    d_cum = jnp.zeros((length, heads), jnp.float32)
    d_row = jnp.zeros((heads, length), jnp.float32)
    head_col = places((length, heads), 1)
    head_row = places((heads, length), 0)
    for g in range(groups):
        c_group = c_ref[:, g * NS : (g + 1) * NS]
        b_group = b_ref[:, g * NS : (g + 1) * NS]
        c_wide = c_group.astype(jnp.float32)
        scores = mul(c_group, b_group, by_cols)
        state_ref[...] = get_state(entry_ref, g, groups).astype(jnp.bfloat16)

        def pair_step(pair, carry):
            d_scores, d_c, d_cum, d_row = carry
            head = g * per_group + 2 * pair
            cols = pl.ds(pl.multiple_of(head * HEAD_DIM, 2 * HEAD_DIM), 2 * HEAD_DIM)
            state_rows = pl.ds(pl.multiple_of(pair * 2 * HEAD_DIM, 2 * HEAD_DIM), 2 * HEAD_DIM)
            x_pair, dy_pair, entry_pair = x_ref[:, cols], dy_ref[:, cols], state_ref[state_rows, :]
            d_x = jnp.zeros((length, 2 * HEAD_DIM), jnp.float32)
            for k in range(2):
                column = head_column(cum, head + k)
                decay = decays(column, row_ref[pl.ds(head + k, 1), :])
                dy_one = jnp.where(masks[k], dy_pair, zero)
                weights = scores * decay
                d_weights = mul(dy_one, x_pair, by_cols)
                d_x = d_x + mul(weights.astype(jnp.bfloat16), dy_one, by_rows)
                d_scores = d_scores + d_weights * decay
                spread = d_weights * weights
                from_entry = mul(dy_one, entry_pair) * jnp.exp(column)
                d_c = d_c + from_entry
                rows = jnp.sum(spread + c_wide * from_entry, axis=1, keepdims=True)
                d_cum = jnp.where(head_col == head + k, rows, d_cum)
                d_row = jnp.where(
                    head_row == head + k, jnp.sum(spread, axis=0, keepdims=True), d_row
                )
            dx_ref[:, cols] = d_x
            return d_scores, d_c, d_cum, d_row

        square = jnp.zeros((length, length), jnp.float32)
        d_scores, d_c, d_cum, d_row = lax.fori_loop(
            0, per_group // 2, pair_step, (square, jnp.zeros((length, NS), jnp.float32), d_cum, d_row)
        )
        half = d_scores.astype(jnp.bfloat16)
        dc_ref[:, g * NS : (g + 1) * NS] = d_c + mul(half, b_group)
        db_ref[:, g * NS : (g + 1) * NS] = mul(half, c_group, by_rows)
    shape = (length, length)
    upper = (places(shape, 0) <= places(shape, 1)).astype(jnp.float32)
    dlog_ref[...] = mul(upper, d_cum, precision=exact) - mul(upper, d_row, by_cols, precision=exact)


def final_kernel(
    grad_ref,
    scaled_ref,
    end_ref,
    b_ref,
    entry_ref,
    last_ref,
    dx_ref,
    db_ref,
    dlog_ref,
    out_ref,
    gx_ref,
    gb_ref,
    glog_ref,
    gout_ref,
):
    length, heads = dlog_ref.shape
    width = dx_ref.shape[1]
    groups = b_ref.shape[1] // NS
    each = width // groups
    spread = head_spread(heads, width)
    moved = jnp.zeros((length, heads), jnp.float32)
    ones = jnp.ones((SUB, NS), jnp.float32)
    kept = jnp.zeros((SUB, heads), jnp.float32)
    for g in range(groups):
        cols = slice(g * each, (g + 1) * each)
        grad_wide = get_state(grad_ref, g, groups)
        grad = grad_wide.astype(jnp.bfloat16)
        scaled = scaled_ref[:, cols]
        raw = mul(b_ref[:, g * NS : (g + 1) * NS], grad, by_cols)
        gx_ref[:, cols] = (dx_ref[:, cols] + raw * end_ref[:, cols]).astype(gx_ref.dtype)
        moved = moved + mul(
            scaled.astype(jnp.float32) * raw, spread[:, cols], by_cols, precision=exact
        )
        gb_ref[:, g * NS : (g + 1) * NS] = db_ref[:, g * NS : (g + 1) * NS] + mul(scaled, grad)
        both = get_state(entry_ref, g, groups) * grad_wide
        kept = kept + mul(
            mul(ones, both, by_cols, precision=exact), spread[:, cols], by_cols, precision=exact
        )
    shape = (length, length)
    earlier = (places(shape, 0) > places(shape, 1)).astype(jnp.float32)
    total = dlog_ref[...] + mul(earlier, moved, precision=exact) + (kept * last_ref[...])[:1, :]
    same = (places(shape, 0) == places(shape, 1)).astype(jnp.float32)
    glog_ref[...] = mul(total, same, by_rows, precision=exact)
    gout_ref[...] = out_ref[...].astype(jnp.float32)


def out_grad_kernel(rank_ref, near_ref, core_ref, *refs):
    mid_refs, half_ref, out_ref, all_ref = refs[:-3], refs[-3], refs[-2], refs[-1]
    near_count, length = len(mid_refs) // 2, mid_refs[0].shape[0]
    for j, mid_ref in enumerate(mid_refs):
        near = lax.rem(near_ref[0] + near_count - j // 2, near_count)
        core = lax.rem(core_ref[0] + j % 2, 2)
        all_ref[pl.ds(pl.multiple_of((near * 2 + core) * length, length), length), :] = mid_ref[...]
    total = mul(all_ref[...], half_ref[...], by_rows)
    parts = 4
    rows = total.shape[0] // parts
    for step in range(parts):
        block = pl.ds(block_of(rank_ref[0], step, parts, rows), rows)
        out_ref[block, :] = total[step * rows : (step + 1) * rows].astype(out_ref.dtype)


def in_hbm(array):
    return pltpu.with_memory_space_constraint(array, pltpu.HBM)


def call(kernel, shapes, *args, scratch=(), scalars=0, far=(), kept=()):
    near_spec = pl.BlockSpec(memory_space=pltpu.VMEM)
    far_spec = pl.BlockSpec(memory_space=pltpu.HBM)
    scalar = pl.BlockSpec(memory_space=pltpu.SMEM)
    n_in, n_out = len(args), len(shapes)
    staged = [(args[i].shape, args[i].dtype) for i in far] + [shapes[i] for i in kept]

    def body(*refs):
        ins, outs = list(refs[:n_in]), list(refs[n_in : n_in + n_out])
        own = refs[n_in + n_out :]
        stage, sems = own[len(scratch) : len(scratch) + len(staged)], own[-1]
        fetches = []
        for k, i in enumerate(far):
            fetches.append(pltpu.make_async_copy(ins[i], stage[k], sems.at[k]))
            fetches[-1].start()
            ins[i] = stage[k]
        for fetch in fetches:
            fetch.wait()
        writes = []
        for k, i in enumerate(kept, len(far)):
            writes.append(pltpu.make_async_copy(stage[k], outs[i], sems.at[k]))
            outs[i] = stage[k]
        kernel(*ins, *outs, *own[: len(scratch)])
        for write in writes:
            write.start()
        for write in writes:
            write.wait()

    spaces = [far_spec if i in far else near_spec for i in range(n_in)]
    return pl.pallas_call(
        body,
        out_shape=tuple(
            pltpu.HBM(s, d) if i in kept else jax.ShapeDtypeStruct(s, d)
            for i, (s, d) in enumerate(shapes)
        ),
        in_specs=[scalar if i < scalars else spaces[i] for i in range(n_in)],
        out_specs=tuple(far_spec if i in kept else near_spec for i in range(n_out)),
        scratch_shapes=[pltpu.VMEM(s, d) for s, d in (*scratch, *staged)]
        + [pltpu.SemaphoreType.DMA((max(len(staged), 1),))],
        compiler_params=pltpu.CompilerParams(vmem_limit_bytes=GRANT),
    )(*(in_hbm(arg) if i in far else arg for i, arg in enumerate(args)))


def swap(array, axis):
    return lax.all_to_all(array, axis, split_axis=0, concat_axis=0, tiled=True)


def moved(array, axis, step):
    count = lax.axis_size(axis)
    return lax.ppermute(array, axis, [((i + step) % count, i) for i in range(count)])


def from_others(array, axis):
    return [array] + [moved(array, axis, step) for step in (1, 2, 3)]


def local(
    hidden_rows,
    out_cot,
    routes,
    route_weight,
    gate_w,
    up_w,
    down_w,
    out_weight,
    step_inputs,
    input_map,
    output_map,
    log_decay,
    gate_z,
):
    f32, bf16 = jnp.float32, jnp.bfloat16
    inner = step_inputs.shape[1]
    maps = input_map.shape[1]
    sp_count, tp_count = lax.axis_size(SP), lax.axis_size("tp")
    width = hidden_rows.shape[1]
    slots = sp_count * CAP
    back_tiles = -(-CAP * width // (LANES * SUB))
    pieces = width // LANES
    hidden_units = gate_w.shape[2]
    full = width * tp_count

    length, heads = log_decay.shape
    log_decay = log_decay.T
    rank = lax.axis_index("tp").astype(jnp.int32)[None]
    near = lax.axis_index(NEAR).astype(jnp.int32)[None]
    core = lax.axis_index(CORE).astype(jnp.int32)[None]
    sent, placing = call(
        place_kernel,
        [((sp_count * 2 * pieces, CAP * LANES), bf16), ((slots, length), bf16)],
        routes.T,
        route_weight.T,
        hidden_rows,
        out_cot,
        scratch=[((CAP * 2 * pieces * sp_count, LANES), f32)],
        far=(0, 1, 2, 3), kept=(1,),
    )
    state_rows = inner // 2
    (own,) = call(
        state_kernel,
        [((state_rows, 3 * NS), bf16)],
        step_inputs,
        input_map,
        log_decay,
        far=(0, 1, 2),
    )
    near_pieces = from_others(out_weight, NEAR)
    got = swap(sent.reshape(sp_count, 2 * pieces, CAP * LANES), SP)
    got, near_pieces = lax.optimization_barrier((got, near_pieces))
    rows, cot = call(
        arrange_kernel,
        [((slots, width), bf16)] * 2,
        got.reshape(sent.shape),
        scratch=[((CAP, sent.shape[0], LANES), f32)],
    )
    rows_next, rows_last = moved(rows, "tp", 1), moved(rows, "tp", -1)
    cot_next, cot_last = moved(cot, "tp", 1), moved(cot, "tp", -1)
    rows_far, cot_far = moved(rows_last, "tp", -1), moved(cot_next, "tp", 1)
    near_pieces, _ = lax.optimization_barrier(
        (near_pieces, (rows_next, rows_last, cot_next, cot_last))
    )
    near_weight = jnp.concatenate(near_pieces, axis=0)
    filled = (
        rows,
        rows_next,
        rows_far,
        rows_last,
        cot,
        cot_next,
        cot_far,
        cot_last,
    )
    half_weight = lax.all_gather(near_weight, FAR, axis=0, tiled=True)
    got_own = swap(own.reshape(sp_count, SUB, 3 * NS), SP).reshape(own.shape)
    mixed, back = call(
        mix_kernel,
        [((state_rows, 2 * NS), bf16), ((state_rows, state_rows), bf16)],
        got_own,
        kept=(1,),
    )
    filled, mixed = lax.optimization_barrier((filled, mixed))
    hidden, d_gate, d_up, *partials = call(
        expert_kernel,
        [((slots, hidden_units), bf16)] * 3 + [((slots, width), bf16)] * tp_count,
        rank,
        *filled,
        gate_w[0],
        up_w[0],
        down_w[0],
        scalars=1,
        far=(9, 10, 11), kept=(0, 1, 2),
    )
    received = [partials[0]] + [moved(partials[step], "tp", -step) for step in (1, 2, 3)]
    entry = swap(mixed.reshape(sp_count, SUB, 2 * NS), SP).reshape(mixed.shape)
    (summed,) = call(
        add_kernel,
        [((sp_count * SUB, back_tiles * LANES), bf16)],
        *received,
        scratch=[((back_tiles * SUB * sp_count, LANES), f32)],
    )
    half_weight, _ = lax.optimization_barrier((half_weight, summed))
    other_weight = moved(half_weight, CORE, 1)
    grad_gate, grad_up, grad_down = call(
        weight_grad_kernel,
        [((full, hidden_units), f32)] * 2 + [((hidden_units, full), f32)],
        rank,
        *filled,
        hidden,
        d_gate,
        d_up,
        scalars=1,
        far=(9, 10, 11), kept=(0, 1, 2),
    )
    returned = swap(summed.reshape(sp_count, SUB, back_tiles * LANES), SP).reshape(summed.shape)
    (mid_part,) = call(
        mid_kernel,
        [((length, width), bf16)],
        near,
        core,
        returned,
        placing,
        out_cot,
        scratch=[((back_tiles, summed.shape[0], LANES), f32), ((slots, width), bf16)],
        scalars=2,
        far=(3, 4),
    )
    mids = from_others(mid_part, "tp")
    y, half = call(
        forward_kernel,
        [((length, inner), f32), ((length, inner), bf16)],
        step_inputs,
        input_map,
        output_map,
        log_decay,
        gate_z,
        entry,
        scratch=[(log_decay.shape, f32)], far=(0, 1, 2, 3, 4, 5), kept=(0, 1),
    )
    full_weight, *gate_values = ordered_weight(
        half_weight, other_weight, y, gate_z, output_map, log_decay
    )
    halves = lax.all_gather(half, (NEAR, CORE), axis=0, tiled=True)
    d_y, grad_z, entry_grad = call(
        gate_kernel,
        [((length, inner), bf16)] * 2 + [((state_rows, 2 * NS), bf16)],
        rank,
        *mids,
        full_weight,
        *gate_values,
        scalars=1,
        kept=(0, 1),
    )
    got_grad = swap(entry_grad.reshape(sp_count, SUB, 2 * NS), SP).reshape(entry_grad.shape)
    (mixed_grad,) = call(mix_back_kernel, [((state_rows, 2 * NS), bf16)], got_grad, back, far=(1,))
    carried = swap(mixed_grad.reshape(sp_count, SUB, 2 * NS), SP).reshape(mixed_grad.shape)
    near_count = lax.axis_size(NEAR)
    blocks = call(
        spread_kernel,
        [((length, full // (2 * near_count)), bf16)] * (2 * near_count),
        *mids,
    )
    mids_here = []
    for step in range(near_count):
        for side in range(2):
            pairs = [
                (
                    n * 2 + c,
                    (n + step) % near_count * 2 + (c + side) % 2,
                )
                for n in range(near_count)
                for c in range(2)
            ]
            block = blocks[step * 2 + side]
            if step or side:
                block = lax.ppermute(block, (NEAR, CORE), pairs)
            mids_here.append(block)
    mids_here, _ = lax.optimization_barrier((mids_here, entry_grad))
    (out_grad,) = call(
        out_grad_kernel,
        [((full // (2 * near_count), inner), bf16)],
        rank,
        near,
        core,
        *mids_here,
        halves,
        scratch=[((halves.shape[0], full // (2 * near_count)), bf16)],
        scalars=3,
        far=(11,), kept=(0,),
    )
    out_part = lax.psum_scatter(out_grad, FAR, scatter_dimension=0, tiled=True)
    d_x, d_b, grad_out_map, d_log, *tail = call(
        within_kernel,
        [
            ((length, inner), f32),
            ((length, maps), f32),
            ((length, maps), f32),
            ((length, heads), f32),
            ((length, inner), bf16),
            ((length, inner), f32),
            (input_map.shape, bf16),
            (entry.shape, bf16),
            ((SUB, heads), f32),
        ],
        d_y,
        step_inputs,
        input_map,
        output_map,
        log_decay,
        entry,
        scratch=[((inner * NS // maps, NS), bf16), (log_decay.shape, f32)],
        far=(0, 1, 2, 3, 4, 5),
        kept=(2,),
    )
    grad_step, grad_in_map, grad_log, grad_out_weight = call(
        final_kernel,
        [((length, inner), bf16), ((length, maps), f32), ((heads, length), f32), (out_part.shape, f32)],
        carried,
        *tail,
        d_x,
        d_b,
        d_log,
        out_part,
        far=(9,),
        kept=(0, 1, 2, 3),
    )
    return (
        grad_gate[None],
        grad_up[None],
        grad_down[None],
        grad_out_weight,
        grad_step,
        grad_z,
        grad_in_map,
        grad_out_map,
        grad_log.T,
    )


def solution(mesh):
    torus = Mesh(mesh.devices.reshape(8, 4, 2, mesh.shape["tp"]), ("sp_0", "sp_1", "sp_2", "tp"))
    placed = (
        P(SP, "tp"),
        P(SP, "tp"),
        P(SP, None),
        P(SP, None),
        P(SP, None, "tp"),
        P(SP, None, "tp"),
        P(SP, "tp", None),
        P(SP, "tp"),
        P(SP, "tp"),
        P(SP, "tp"),
        P(SP, "tp"),
        P(SP, "tp"),
        P(SP, "tp"),
    )
    return jax.shard_map(
        local,
        mesh=torus,
        in_specs=placed,
        out_specs=(
            P(SP, None, "tp"),
            P(SP, None, "tp"),
            P(SP, "tp", None),
            P(SP, "tp"),
            P(SP, "tp"),
            P(SP, "tp"),
            P(SP, "tp"),
            P(SP, "tp"),
            P(SP, "tp"),
        ),
        check_vma=False,
    )
```

```python
import jax
import jax.numpy as jnp
from jax import lax
from jax.experimental import pallas as pl
from jax.experimental.pallas import tpu as pltpu
from jax.sharding import Mesh
from jax.sharding import PartitionSpec as P


SP = ("sp_0", "sp_1", "sp_2")
FAR, NEAR, CORE = SP
CAP = 5
SUB = 8
GRANT = 16 * 1024 * 1024
PIECE = 32
LANES = 128
HEAD_DIM = 64
NS = 128
epsilon = 1e-06
exact = lax.Precision.HIGHEST
by_rows = (((0,), (0,)), ((), ()))
by_cols = (((1,), (1,)), ((), ()))


def mul(a, b, dims=None, precision=None):
    dims = (((1,), (0,)), ((), ())) if dims is None else dims
    return lax.dot_general(a, b, dims, precision=precision, preferred_element_type=jnp.float32)


def places(shape, dim):
    return lax.broadcasted_iota(jnp.int32, shape, dim)


def head_spread(heads, width):
    shape = (heads, width)
    return (places(shape, 1) // HEAD_DIM == places(shape, 0)).astype(jnp.float32)


def running(log):
    length = log.shape[1]
    shape = (length, length)
    lower = (places(shape, 0) >= places(shape, 1)).astype(jnp.float32)
    return mul(lower, log, by_cols, precision=exact), mul(log, lower, by_cols, precision=exact)


def to_end_wide(cum, width):
    last = cum[-1:, :]
    return mul(jnp.exp(last - cum), head_spread(cum.shape[1], width), precision=exact)


def gather_cells(wide_ref, out_ref, count):
    for tile in range(out_ref.shape[1] // LANES):
        for first in range(0, count, 2):
            rows = jnp.concatenate(
                [
                    wide_ref[pl.ds(tile * SUB * count + first + k, SUB, stride=count), :]
                    for k in range(2)
                ],
                axis=0,
            )
            out_ref[first * SUB : (first + 2) * SUB, tile * LANES : (tile + 1) * LANES] = rows.astype(
                out_ref.dtype
            )


def place_kernel(routes_ref, weight_ref, rows_ref, cot_ref, out_ref, placing_ref, wide_ref):
    top, length = routes_ref.shape
    experts = placing_ref.shape[0] // CAP
    shape = (experts, length)
    expert = places(shape, 0)
    hits = [routes_ref[k : k + 1, :] == expert for k in range(top)]
    named = hits[0]
    for k in range(1, top):
        named = jnp.logical_or(named, hits[k])
    square = (length, length)
    sooner = (places(square, 0) < places(square, 1)).astype(jnp.bfloat16)
    taken = mul(named.astype(jnp.bfloat16), sooner)
    ranks = [jnp.sum(jnp.where(h, taken, 0.0), axis=0, keepdims=True) for h in hits]
    rows, cot = rows_ref[...], cot_ref[...]
    width = rows.shape[1]
    pieces = 2 * width // LANES
    for slot in range(CAP):
        here = [jnp.logical_and(hits[k], ranks[k] == float(slot)) for k in range(top)]
        weight = jnp.zeros((experts, 1), jnp.float32)
        for k in range(top):
            weight = weight + jnp.sum(
                jnp.where(here[k], weight_ref[k : k + 1, :], 0.0), axis=1, keepdims=True
            )
        chosen = here[0]
        for k in range(1, top):
            chosen = jnp.logical_or(chosen, here[k])
        chosen = chosen.astype(jnp.float32).astype(jnp.bfloat16)
        placing_ref[slot * experts : (slot + 1) * experts, :] = chosen
        both = (mul(chosen, rows), mul(chosen, cot) * weight)
        for j in range(pieces):
            source = both[j * LANES // width]
            start = j * LANES % width
            cell = (slot * pieces + j) * experts
            wide_ref[cell : cell + experts, :] = source[:, start : start + LANES]
    gather_cells(wide_ref, out_ref, experts)


def arrange_kernel(got_ref, rows_ref, cot_ref, wide_ref):
    for slot in range(CAP):
        wide_ref[slot] = got_ref[:, slot * LANES : (slot + 1) * LANES].astype(jnp.float32)
    slots, width = rows_ref.shape
    count = slots // CAP
    pieces = 2 * width // LANES
    for slot in range(CAP):
        for j in range(pieces):
            block = wide_ref[slot, pl.ds(j, count, stride=pieces), :]
            out_ref = rows_ref if j * LANES < width else cot_ref
            start = j * LANES % width
            out_ref[slot * count : (slot + 1) * count, start : start + LANES] = block.astype(
                out_ref.dtype
            )


def block_of(rank, step, parts, width):
    return pl.multiple_of(lax.rem(rank + step, parts) * width, width)


def expert_kernel(rank_ref, *refs):
    refs, flush = refs[:-2], refs[-2]
    parts = (len(refs) - 6) // 3
    rows_refs, cot_refs, part_refs = refs[:parts], refs[parts : 2 * parts], refs[-parts:]
    gate_ref, up_ref, down_ref, hidden_ref, dgate_ref, dup_ref = refs[2 * parts : -parts]
    _, width = rows_refs[0].shape
    gate_pre = up_pre = d_act = None
    for step in range(parts):
        block = pl.ds(block_of(rank_ref[0], step, parts, width), width)
        rows, cot = rows_refs[step][...], cot_refs[step][...]
        one, two = mul(rows, gate_ref[block, :]), mul(rows, up_ref[block, :])
        three = mul(cot, down_ref[:, block], by_cols)
        gate_pre = one if step == 0 else gate_pre + one
        up_pre = two if step == 0 else up_pre + two
        d_act = three if step == 0 else d_act + three
    sig = jax.nn.sigmoid(gate_pre)
    hidden_ref[...] = (gate_pre * sig * up_pre).astype(jnp.bfloat16)
    d_gate = (d_act * up_pre * sig * (1.0 + gate_pre * (1.0 - sig))).astype(jnp.bfloat16)
    d_up = (d_act * gate_pre * sig).astype(jnp.bfloat16)
    dgate_ref[...] = d_gate
    dup_ref[...] = d_up
    for k in range(3):
        flush(k)
    for step in range(parts):
        block = pl.ds(block_of(rank_ref[0], step, parts, width), width)
        part = mul(d_gate, gate_ref[block, :], by_cols) + mul(d_up, up_ref[block, :], by_cols)
        part_refs[step][...] = part.astype(part_refs[step].dtype)


def weight_grad_kernel(rank_ref, *refs):
    parts = (len(refs) - 6) // 2
    rows_refs, cot_refs = refs[:parts], refs[parts : 2 * parts]
    hidden_ref, dgate_ref, dup_ref, gate_ref, up_ref, down_ref = refs[2 * parts :]
    width = rows_refs[0].shape[1]
    for step in range(parts):
        block = pl.ds(block_of(rank_ref[0], step, parts, width), width)
        rows, cot = rows_refs[step][...], cot_refs[step][...]
        gate_ref[block, :] = mul(rows, dgate_ref[...], by_rows)
        up_ref[block, :] = mul(rows, dup_ref[...], by_rows)
        down_ref[:, block] = mul(hidden_ref[...], cot, by_rows)


def add_kernel(one_ref, two_ref, three_ref, four_ref, out_ref, wide_ref):
    slots, width = one_ref.shape
    total = one_ref[...].astype(jnp.float32)
    for got_ref in (two_ref, three_ref, four_ref):
        total = total + got_ref[...].astype(jnp.float32)
    count = slots // CAP
    pieces = width // LANES
    used = CAP * pieces * count
    wide_ref[used:, :] = jnp.zeros((wide_ref.shape[0] - used, LANES), jnp.float32)
    for slot in range(CAP):
        for j in range(pieces):
            cell = (slot * pieces + j) * count
            wide_ref[cell : cell + count, :] = total[
                slot * count : (slot + 1) * count, j * LANES : (j + 1) * LANES
            ]
    gather_cells(wide_ref, out_ref, count)


def mid_kernel(near_ref, core_ref, back_ref, placing_ref, cot_ref, out_ref, wide_ref, slots_ref):
    for tile in range(wide_ref.shape[0]):
        wide_ref[tile] = back_ref[:, tile * LANES : (tile + 1) * LANES].astype(jnp.float32)
    slots, width = slots_ref.shape
    count = slots // CAP
    pieces = width // LANES
    for slot in range(CAP):
        for j in range(pieces):
            tile, row = divmod(slot * pieces + j, SUB)
            block = wide_ref[tile, pl.ds(row, count, stride=SUB), :]
            slots_ref[slot * count : (slot + 1) * count, j * LANES : (j + 1) * LANES] = block.astype(
                slots_ref.dtype
            )
    routed = mul(placing_ref[...], slots_ref[...], by_rows)
    mid = (cot_ref[...].astype(jnp.float32) + routed).astype(jnp.bfloat16)
    near, core = near_ref[0], core_ref[0]
    lane = places((1, width), 1)
    per_block = 2 * PIECE
    block, inside = lane // per_block, lane % per_block
    step_near, step_core = block // 2, block % 2
    far, row = inside // PIECE, inside % PIECE
    source = (
        far * (width // 2) + (near + step_near) % 4 * per_block + (core + step_core) % 2 * PIECE + row
    )
    moved = (places((width, width), 0) == source).astype(jnp.float32).astype(jnp.bfloat16)
    out_ref[...] = mul(mid, moved).astype(out_ref.dtype)


def weight_kernel(
    mine_ref,
    other_ref,
    y_ref,
    z_ref,
    c_ref,
    back_ref,
    log_ref,
    out_ref,
    y_out,
    z_out,
    c_out,
    back_out,
    wide_ref,
    log,
    sems,
):
    steps, tp_count = 4, 4
    per_tp = mine_ref.shape[0] // (tp_count * steps * PIECE)
    copies = []
    for q in range(tp_count):
        for step in range(steps):
            for core, ref in enumerate((mine_ref, other_ref)):
                for far in range(per_tp):
                    source = ((q * per_tp + far) * steps + step) * PIECE
                    target = (((q * steps + step) * 2 + core) * per_tp + far) * PIECE
                    copies.append(
                        pltpu.make_async_copy(
                            ref.at[pl.ds(source, PIECE), :],
                            out_ref.at[pl.ds(target, PIECE), :],
                            sems.at[len(copies)],
                        )
                    )
    extra = ((log_ref, log), (y_ref, y_out), (z_ref, z_out), (c_ref, c_out), (back_ref, back_out))
    moves = [
        pltpu.make_async_copy(source, target, sems.at[len(copies) + k])
        for k, (source, target) in enumerate(extra)
    ]
    for copy in moves + copies:
        copy.start()
    moves[0].wait()
    cum, _ = running(log[...])
    heads, width = log.shape[0], wide_ref.shape[1]
    wide_ref[...] = mul(jnp.exp(cum), head_spread(heads, width), precision=exact)
    for copy in moves[1:] + copies:
        copy.wait()


def ordered_weight(mine, other, y, z, c, back, log):
    far_spec = pl.BlockSpec(memory_space=pltpu.HBM)
    rows, width = mine.shape
    near_spec = pl.BlockSpec(memory_space=pltpu.VMEM)
    shapes = [((2 * rows, width), mine.dtype)]
    shapes += [(a.shape, a.dtype) for a in (y, z, c, back)] + [(y.shape, jnp.float32)]
    return pl.pallas_call(
        weight_kernel,
        out_shape=tuple(jax.ShapeDtypeStruct(s, d) for s, d in shapes),
        in_specs=[far_spec] * 7,
        out_specs=(near_spec,) * len(shapes),
        scratch_shapes=[
            pltpu.VMEM(log.shape, log.dtype),
            pltpu.SemaphoreType.DMA((2 * rows // PIECE + 5,)),
        ],
        compiler_params=pltpu.CompilerParams(vmem_limit_bytes=GRANT),
        name="weight_kernel",
    )(*(in_hbm(a) for a in (mine, other, y, z, c, back, log)))


def spread_kernel(*refs):
    mid_refs, out_refs = refs[:4], refs[4:]
    width = mid_refs[0].shape[1] // len(out_refs)
    for j, out_ref in enumerate(out_refs):
        for k, mid_ref in enumerate(mid_refs):
            out_ref[:, k * width : (k + 1) * width] = mid_ref[:, j * width : (j + 1) * width]


def put_state(out_ref, group, part):
    rows = part.shape[0] // 2
    tiles = part.reshape(rows // SUB, 2, SUB, NS)
    for k in range(2):
        out_ref[group * rows : (group + 1) * rows, k * NS : (k + 1) * NS] = (
            tiles[:, k].reshape(rows, NS).astype(out_ref.dtype)
        )


def get_state(ref, group, groups):
    rows = ref.shape[0] // groups
    halves = [
        ref[group * rows : (group + 1) * rows, k * NS : (k + 1) * NS]
        .astype(jnp.float32)
        .reshape(rows // SUB, SUB, NS)
        for k in range(2)
    ]
    return jnp.stack(halves, axis=1).reshape(2 * rows, NS)


def mix_kernel(
    got_ref, gate_ref, up_ref, down_ref, out_ref, back_ref, gate_out, up_out, down_out, sems
):
    fetches = [
        pltpu.make_async_copy(source, target, sems.at[k])
        for k, (source, target) in enumerate(
            ((gate_ref, gate_out), (up_ref, up_out), (down_ref, down_out))
        )
    ]
    for fetch in fetches:
        fetch.start()
    count = got_ref.shape[0]
    devices = count // SUB
    state = got_ref[:, : 2 * NS]
    shape = (devices, count)
    chosen = (places(shape, 1) == SUB * places(shape, 0)).astype(jnp.float32).astype(jnp.bfloat16)
    parts = mul(chosen, got_ref[:, 2 * NS :])
    logs = jnp.sum(jnp.where(places(parts.shape, 1) < 3, parts, 0.0), axis=1, keepdims=True)
    log = jnp.broadcast_to(logs, parts.shape)
    small = (devices, devices)
    one, two = places(small, 0), places(small, 1)
    through = mul((one >= two).astype(jnp.float32), log, precision=exact)
    before = through - log
    through_row = mul(log, (one <= two).astype(jnp.float32), by_rows, precision=exact)[:1]
    before_row = mul(log, (one < two).astype(jnp.float32), by_rows, precision=exact)[:1]
    tall = (count, devices)
    copies = (places(tall, 0) // SUB == places(tall, 1)).astype(jnp.float32).astype(jnp.bfloat16)
    square = (count, count)
    same = places(square, 0) % SUB == places(square, 1) % SUB

    def spread(weights):
        wide = mul(mul(copies, weights).astype(jnp.bfloat16), copies, by_cols)
        return jnp.where(same, wide, 0.0).astype(jnp.bfloat16)

    def wide_weights(spans, mask):
        return spread(jnp.exp(jnp.where(mask, spans, -jnp.inf)).astype(jnp.bfloat16))

    weights = wide_weights(before[:, :1] - through_row, two < one)
    out_ref[...] = mul(weights, state).astype(out_ref.dtype)
    back_ref[...] = wide_weights(before_row - through[:, :1], one < two)
    for fetch in fetches:
        fetch.wait()


def mix_back_kernel(got_ref, back_ref, out_ref):
    out_ref[...] = mul(back_ref[...], got_ref[...]).astype(out_ref.dtype)


def state_kernel(x_ref, b_ref, log_ref, out_ref):
    log = log_ref[...]
    width = x_ref.shape[1]
    cum, _ = running(log)
    scaled = (x_ref[...].astype(jnp.float32) * to_end_wide(cum, width)).astype(jnp.bfloat16)
    groups = b_ref.shape[1] // NS
    each = width // groups
    for g in range(groups):
        part = mul(scaled[:, g * each : (g + 1) * each], b_ref[:, g * NS : (g + 1) * NS], by_rows)
        put_state(out_ref, g, part)
    rows, heads = out_ref.shape[0], log.shape[0]
    shape = (rows, heads)
    owner = places(shape, 0) // (rows // heads) == places(shape, 1)
    total = jnp.sum(jnp.where(owner, cum[-1:, :], 0.0), axis=1, keepdims=True)
    high = total.astype(jnp.bfloat16).astype(jnp.float32)
    middle = (total - high).astype(jnp.bfloat16).astype(jnp.float32)
    low = total - high - middle
    lane = places((rows, NS), 1)
    out_ref[:, 2 * NS :] = jnp.where(
        lane == 0, high, jnp.where(lane == 1, middle, jnp.where(lane == 2, low, 0.0))
    ).astype(out_ref.dtype)


def head_column(values, head):
    return jnp.sum(jnp.where(places(values.shape, 1) == head, values, 0.0), axis=1, keepdims=True)


def decays(column, row):
    shape = (column.shape[0], row.shape[1])
    return jnp.exp(jnp.where(places(shape, 0) >= places(shape, 1), column - row, -jnp.inf))


def half_masks(length):
    lane = places((length, 2 * HEAD_DIM), 1)
    return (lane < HEAD_DIM, lane >= HEAD_DIM)


def forward_kernel(x_ref, b_ref, c_ref, log_ref, z_ref, entry_ref, y_ref, half_ref, row_ref):
    log = log_ref[...]
    heads, length = log.shape
    width = x_ref.shape[1]
    groups = b_ref.shape[1] // NS
    each = width // groups
    per_group = heads // groups
    cum, cum_row = running(log)
    row_ref[...] = cum_row
    from_start = mul(jnp.exp(cum), head_spread(heads, width), precision=exact)
    masks = half_masks(length)
    zero = jnp.zeros((length, 2 * HEAD_DIM), jnp.bfloat16)
    for g in range(groups):
        c_group = c_ref[:, g * NS : (g + 1) * NS]
        scores = mul(c_group, b_ref[:, g * NS : (g + 1) * NS], by_cols)
        carried = mul(c_group, get_state(entry_ref, g, groups).astype(jnp.bfloat16), by_cols)

        def pair_step(pair, carry):
            head = g * per_group + 2 * pair
            lanes = pl.ds(pl.multiple_of(head * HEAD_DIM, 2 * HEAD_DIM), 2 * HEAD_DIM)
            x_pair = x_ref[:, lanes]
            total = jnp.zeros((length, 2 * HEAD_DIM), jnp.float32)
            for k in range(2):
                decay = decays(head_column(cum, head + k), row_ref[pl.ds(head + k, 1), :])
                weights = (scores * decay).astype(jnp.bfloat16)
                total = total + mul(weights, jnp.where(masks[k], x_pair, zero))
            y_ref[:, lanes] = total
            return carry

        lax.fori_loop(0, per_group // 2, pair_step, 0)
        cols = slice(g * each, (g + 1) * each)
        y = y_ref[:, cols] + carried * from_start[:, cols]
        z = z_ref[:, cols].astype(jnp.float32)
        gated = y * (z * jax.nn.sigmoid(z))
        mean = jnp.mean(gated * gated, axis=1, keepdims=True)
        y_ref[:, cols] = y
        half_ref[:, cols] = (gated * lax.rsqrt(mean + epsilon)).astype(half_ref.dtype)


def gate_kernel(rank_ref, m0, m1, m2, m3, w_ref, y_ref, z_ref, c_ref, wide_ref, dy_ref, dz_ref, out_ref):
    width = y_ref.shape[1]
    groups = c_ref.shape[1] // NS
    each = width // groups
    mid_refs = (m0, m1, m2, m3)
    parts, rows = len(mid_refs), m0.shape[1]
    for g in range(groups):
        cols = slice(g * each, (g + 1) * each)
        d_normed = None
        for step in range(parts):
            block = pl.ds(block_of(rank_ref[0], step, parts, rows), rows)
            part = mul(mid_refs[step][...], w_ref[block, cols])
            d_normed = part if d_normed is None else d_normed + part
        y = y_ref[:, cols]
        z = z_ref[:, cols].astype(jnp.float32)
        sig = jax.nn.sigmoid(z)
        silu = z * sig
        gated = y * silu
        inverse = lax.rsqrt(jnp.mean(gated * gated, axis=1, keepdims=True) + epsilon)
        normed = gated * inverse
        along = jnp.mean(d_normed * normed, axis=1, keepdims=True)
        d_gated = inverse * (d_normed - normed * along)
        d_y = d_gated * silu
        dy_ref[:, cols] = d_y.astype(dy_ref.dtype)
        dz_ref[:, cols] = (d_gated * y * (sig * (1.0 + z * (1.0 - sig)))).astype(dz_ref.dtype)
        scaled = (d_y * wide_ref[:, cols]).astype(jnp.bfloat16)
        part = mul(scaled, c_ref[:, g * NS : (g + 1) * NS], by_rows)
        put_state(out_ref, g, part)


def within_kernel(
    dy_ref,
    x_ref,
    b_ref,
    c_ref,
    log_ref,
    entry_ref,
    dx_ref,
    db_ref,
    dc_ref,
    dlog_ref,
    scaled_ref,
    end_ref,
    b_out,
    entry_out,
    last_ref,
    state_ref,
    row_ref,
):
    log = log_ref[...]
    heads, length = log.shape
    width = x_ref.shape[1]
    groups = b_ref.shape[1] // NS
    per_group = heads // groups
    cum, cum_row = running(log)
    row_ref[...] = cum_row
    to_end = to_end_wide(cum, width)
    end_ref[...] = to_end
    scaled_ref[...] = (x_ref[...].astype(jnp.float32) * to_end).astype(scaled_ref.dtype)
    b_out[...] = b_ref[...]
    entry_out[...] = entry_ref[...]
    last_ref[...] = jnp.broadcast_to(jnp.exp(cum[-1:, :]), last_ref.shape)
    masks = half_masks(length)
    zero = jnp.zeros((length, 2 * HEAD_DIM), jnp.bfloat16)
    d_cum = jnp.zeros((length, heads), jnp.float32)
    d_row = jnp.zeros((heads, length), jnp.float32)
    head_col = places((length, heads), 1)
    head_row = places((heads, length), 0)
    for g in range(groups):
        c_group = c_ref[:, g * NS : (g + 1) * NS]
        b_group = b_ref[:, g * NS : (g + 1) * NS]
        c_wide = c_group.astype(jnp.float32)
        scores = mul(c_group, b_group, by_cols)
        state_ref[...] = get_state(entry_ref, g, groups).astype(jnp.bfloat16)

        def pair_step(pair, carry):
            d_scores, d_c, d_cum, d_row = carry
            head = g * per_group + 2 * pair
            cols = pl.ds(pl.multiple_of(head * HEAD_DIM, 2 * HEAD_DIM), 2 * HEAD_DIM)
            state_rows = pl.ds(pl.multiple_of(pair * 2 * HEAD_DIM, 2 * HEAD_DIM), 2 * HEAD_DIM)
            x_pair, dy_pair, entry_pair = x_ref[:, cols], dy_ref[:, cols], state_ref[state_rows, :]
            d_x = jnp.zeros((length, 2 * HEAD_DIM), jnp.float32)
            for k in range(2):
                column = head_column(cum, head + k)
                decay = decays(column, row_ref[pl.ds(head + k, 1), :])
                dy_one = jnp.where(masks[k], dy_pair, zero)
                weights = scores * decay
                d_weights = mul(dy_one, x_pair, by_cols)
                d_x = d_x + mul(weights.astype(jnp.bfloat16), dy_one, by_rows)
                d_scores = d_scores + d_weights * decay
                spread = d_weights * weights
                from_entry = mul(dy_one, entry_pair) * jnp.exp(column)
                d_c = d_c + from_entry
                rows = jnp.sum(spread + c_wide * from_entry, axis=1, keepdims=True)
                d_cum = jnp.where(head_col == head + k, rows, d_cum)
                d_row = jnp.where(
                    head_row == head + k, jnp.sum(spread, axis=0, keepdims=True), d_row
                )
            dx_ref[:, cols] = d_x
            return d_scores, d_c, d_cum, d_row

        square = jnp.zeros((length, length), jnp.float32)
        d_scores, d_c, d_cum, d_row = lax.fori_loop(
            0, per_group // 2, pair_step, (square, jnp.zeros((length, NS), jnp.float32), d_cum, d_row)
        )
        half = d_scores.astype(jnp.bfloat16)
        dc_ref[:, g * NS : (g + 1) * NS] = d_c + mul(half, b_group)
        db_ref[:, g * NS : (g + 1) * NS] = mul(half, c_group, by_rows)
    shape = (length, length)
    upper = (places(shape, 0) <= places(shape, 1)).astype(jnp.float32)
    dlog_ref[...] = mul(upper, d_cum, precision=exact) - mul(upper, d_row, by_cols, precision=exact)


def final_kernel(
    grad_ref,
    scaled_ref,
    end_ref,
    b_ref,
    entry_ref,
    last_ref,
    dx_ref,
    db_ref,
    dlog_ref,
    out_ref,
    gx_ref,
    gb_ref,
    glog_ref,
    gout_ref,
    flush,
    ready,
):
    length, heads = dlog_ref.shape
    width = dx_ref.shape[1]
    groups = b_ref.shape[1] // NS
    each = width // groups
    spread = head_spread(heads, width)
    moved = jnp.zeros((length, heads), jnp.float32)
    ones = jnp.ones((SUB, NS), jnp.float32)
    kept = jnp.zeros((SUB, heads), jnp.float32)
    for g in range(groups):
        cols = slice(g * each, (g + 1) * each)
        grad_wide = get_state(grad_ref, g, groups)
        grad = grad_wide.astype(jnp.bfloat16)
        scaled = scaled_ref[:, cols]
        raw = mul(b_ref[:, g * NS : (g + 1) * NS], grad, by_cols)
        gx_ref[:, cols] = (dx_ref[:, cols] + raw * end_ref[:, cols]).astype(gx_ref.dtype)
        moved = moved + mul(
            scaled.astype(jnp.float32) * raw, spread[:, cols], by_cols, precision=exact
        )
        gb_ref[:, g * NS : (g + 1) * NS] = db_ref[:, g * NS : (g + 1) * NS] + mul(scaled, grad)
        if g == groups - 1:
            ready(9)
            gout_ref[...] = out_ref[...].astype(jnp.float32)
            for k in (0, 1, 3):
                flush(k)
        both = get_state(entry_ref, g, groups) * grad_wide
        kept = kept + mul(
            mul(ones, both, by_cols, precision=exact), spread[:, cols], by_cols, precision=exact
        )
    shape = (length, length)
    earlier = (places(shape, 0) > places(shape, 1)).astype(jnp.float32)
    total = dlog_ref[...] + mul(earlier, moved, precision=exact) + (kept * last_ref[...])[:1, :]
    same = (places(shape, 0) == places(shape, 1)).astype(jnp.float32)
    glog_ref[...] = mul(total, same, by_rows, precision=exact)


def out_grad_kernel(rank_ref, near_ref, core_ref, *refs):
    mid_refs, half_ref, out_ref, all_ref = refs[:-3], refs[-3], refs[-2], refs[-1]
    near_count, length = len(mid_refs) // 2, mid_refs[0].shape[0]
    for j, mid_ref in enumerate(mid_refs):
        near = lax.rem(near_ref[0] + near_count - j // 2, near_count)
        core = lax.rem(core_ref[0] + j % 2, 2)
        all_ref[pl.ds(pl.multiple_of((near * 2 + core) * length, length), length), :] = mid_ref[...]
    total = mul(all_ref[...], half_ref[...], by_rows)
    parts = 4
    rows = total.shape[0] // parts
    for step in range(parts):
        block = pl.ds(block_of(rank_ref[0], step, parts, rows), rows)
        out_ref[block, :] = total[step * rows : (step + 1) * rows].astype(out_ref.dtype)


def in_hbm(array):
    return pltpu.with_memory_space_constraint(array, pltpu.HBM)


def call(kernel, shapes, *args, scratch=(), scalars=0, far=(), kept=(), raw=(), sems=0, late=(), early=False):
    near_spec = pl.BlockSpec(memory_space=pltpu.VMEM)
    far_spec = pl.BlockSpec(memory_space=pltpu.HBM)
    scalar = pl.BlockSpec(memory_space=pltpu.SMEM)
    n_in, n_out = len(args), len(shapes)
    staged = [(args[i].shape, args[i].dtype) for i in far] + [shapes[i] for i in kept]

    def body(*refs):
        ins, outs = list(refs[:n_in]), list(refs[n_in : n_in + n_out])
        own = refs[n_in + n_out :]
        stage, flags = own[len(scratch) : len(scratch) + len(staged)], own[-1]
        fetches, writes, started = {}, {}, set()
        for k, i in enumerate(far):
            fetches[i] = pltpu.make_async_copy(ins[i], stage[k], flags.at[k])
            fetches[i].start()
            ins[i] = stage[k]
        for i in far:
            if i not in late:
                fetches[i].wait()
        for k, i in enumerate(kept, len(far)):
            writes[i] = pltpu.make_async_copy(stage[k], outs[i], flags.at[k])
            outs[i] = stage[k]

        def flush(i):
            started.add(i)
            writes[i].start()

        extra = [own[-2]] if sems else []
        if early:
            extra += [flush, lambda i: fetches[i].wait()]
        kernel(*ins, *outs, *own[: len(scratch)], *extra)
        for i in writes:
            if i not in started:
                flush(i)
        for write in writes.values():
            write.wait()

    spaces = [far_spec if i in (*far, *raw) else near_spec for i in range(n_in)]
    return pl.pallas_call(
        body,
        out_shape=tuple(
            pltpu.HBM(s, d) if i in kept else jax.ShapeDtypeStruct(s, d)
            for i, (s, d) in enumerate(shapes)
        ),
        in_specs=[scalar if i < scalars else spaces[i] for i in range(n_in)],
        out_specs=tuple(far_spec if i in kept else near_spec for i in range(n_out)),
        scratch_shapes=[pltpu.VMEM(s, d) for s, d in (*scratch, *staged)]
        + ([pltpu.SemaphoreType.DMA((sems,))] if sems else [])
        + [pltpu.SemaphoreType.DMA((max(len(staged), 1),))],
        compiler_params=pltpu.CompilerParams(vmem_limit_bytes=GRANT),
    )(*(in_hbm(arg) if i in (*far, *raw) else arg for i, arg in enumerate(args)))


def swap(array, axis):
    return lax.all_to_all(array, axis, split_axis=0, concat_axis=0, tiled=True)


def moved(array, axis, step):
    count = lax.axis_size(axis)
    return lax.ppermute(array, axis, [((i + step) % count, i) for i in range(count)])


def from_others(array, axis):
    return [array] + [moved(array, axis, step) for step in (1, 2, 3)]


def local(
    hidden_rows,
    out_cot,
    routes,
    route_weight,
    gate_w,
    up_w,
    down_w,
    out_weight,
    step_inputs,
    input_map,
    output_map,
    log_decay,
    gate_z,
):
    f32, bf16 = jnp.float32, jnp.bfloat16
    inner = step_inputs.shape[1]
    maps = input_map.shape[1]
    sp_count, tp_count = lax.axis_size(SP), lax.axis_size("tp")
    width = hidden_rows.shape[1]
    slots = sp_count * CAP
    back_tiles = -(-CAP * width // (LANES * SUB))
    pieces = width // LANES
    hidden_units = gate_w.shape[2]
    full = width * tp_count

    length, heads = log_decay.shape
    log_decay = log_decay.T
    rank = lax.axis_index("tp").astype(jnp.int32)[None]
    near = lax.axis_index(NEAR).astype(jnp.int32)[None]
    core = lax.axis_index(CORE).astype(jnp.int32)[None]
    sent, placing = call(
        place_kernel,
        [((sp_count * 2 * pieces, CAP * LANES), bf16), ((slots, length), bf16)],
        routes.T,
        route_weight.T,
        hidden_rows,
        out_cot,
        scratch=[((CAP * 2 * pieces * sp_count, LANES), f32)],
        far=(0, 1, 2, 3), kept=(1,),
    )
    state_rows = inner // 2
    (own,) = call(
        state_kernel,
        [((state_rows, 3 * NS), bf16)],
        step_inputs,
        input_map,
        log_decay,
        far=(0, 1, 2),
    )
    near_pieces = from_others(out_weight, NEAR)
    got = swap(sent.reshape(sp_count, 2 * pieces, CAP * LANES), SP)
    got, near_pieces = lax.optimization_barrier((got, near_pieces))
    rows, cot = call(
        arrange_kernel,
        [((slots, width), bf16)] * 2,
        got.reshape(sent.shape),
        scratch=[((CAP, sent.shape[0], LANES), f32)],
    )
    rows_next, rows_last = moved(rows, "tp", 1), moved(rows, "tp", -1)
    cot_next, cot_last = moved(cot, "tp", 1), moved(cot, "tp", -1)
    rows_far, cot_far = moved(rows_last, "tp", -1), moved(cot_next, "tp", 1)
    filled = (
        rows,
        rows_next,
        rows_far,
        rows_last,
        cot,
        cot_next,
        cot_far,
        cot_last,
    )
    got_own = swap(own.reshape(sp_count, SUB, 3 * NS), SP).reshape(own.shape)
    near_pieces, _ = lax.optimization_barrier((near_pieces, (rows_far, cot_far)))
    near_weight = jnp.concatenate(near_pieces, axis=0)
    half_weight = lax.all_gather(near_weight, FAR, axis=0, tiled=True)
    matrices = (gate_w[0], up_w[0], down_w[0])
    mixed, back, *matrices = call(
        mix_kernel,
        [((state_rows, 2 * NS), bf16), ((state_rows, state_rows), bf16)]
        + [(m.shape, bf16) for m in matrices],
        got_own,
        *matrices,
        kept=(1,),
        raw=(1, 2, 3),
        sems=3,
    )
    filled, mixed = lax.optimization_barrier((filled, mixed))
    hidden, d_gate, d_up, *partials = call(
        expert_kernel,
        [((slots, hidden_units), bf16)] * 3 + [((slots, width), bf16)] * tp_count,
        rank,
        *filled,
        *matrices,
        scalars=1,
        kept=(0, 1, 2), early=True,
    )
    received = [partials[0]] + [moved(partials[step], "tp", -step) for step in (1, 2, 3)]
    entry = swap(mixed.reshape(sp_count, SUB, 2 * NS), SP).reshape(mixed.shape)
    (summed,) = call(
        add_kernel,
        [((sp_count * SUB, back_tiles * LANES), bf16)],
        *received,
        scratch=[((back_tiles * SUB * sp_count, LANES), f32)],
    )
    half_weight, _ = lax.optimization_barrier((half_weight, summed))
    other_weight = moved(half_weight, CORE, 1)
    grad_gate, grad_up, grad_down = call(
        weight_grad_kernel,
        [((full, hidden_units), f32)] * 2 + [((hidden_units, full), f32)],
        rank,
        *filled,
        hidden,
        d_gate,
        d_up,
        scalars=1,
        far=(9, 10, 11), kept=(0, 1, 2),
    )
    returned = swap(summed.reshape(sp_count, SUB, back_tiles * LANES), SP).reshape(summed.shape)
    (mid_part,) = call(
        mid_kernel,
        [((length, width), bf16)],
        near,
        core,
        returned,
        placing,
        out_cot,
        scratch=[((back_tiles, summed.shape[0], LANES), f32), ((slots, width), bf16)],
        scalars=2,
        far=(3, 4),
    )
    mids = from_others(mid_part, "tp")
    y, half = call(
        forward_kernel,
        [((length, inner), f32), ((length, inner), bf16)],
        step_inputs,
        input_map,
        output_map,
        log_decay,
        gate_z,
        entry,
        scratch=[(log_decay.shape, f32)], far=(0, 1, 2, 3, 4, 5), kept=(0, 1),
    )
    full_weight, *gate_values, back, wide = ordered_weight(
        half_weight, other_weight, y, gate_z, output_map, back, log_decay
    )
    halves = lax.all_gather(half, (NEAR, CORE), axis=0, tiled=True)
    d_y, grad_z, entry_grad = call(
        gate_kernel,
        [((length, inner), bf16)] * 2 + [((state_rows, 2 * NS), bf16)],
        rank,
        *mids,
        full_weight,
        *gate_values,
        wide,
        scalars=1,
        kept=(0, 1),
    )
    got_grad = swap(entry_grad.reshape(sp_count, SUB, 2 * NS), SP).reshape(entry_grad.shape)
    (mixed_grad,) = call(
        mix_back_kernel, [((state_rows, 2 * NS), bf16)], got_grad, back
    )
    carried = swap(mixed_grad.reshape(sp_count, SUB, 2 * NS), SP).reshape(mixed_grad.shape)
    near_count = lax.axis_size(NEAR)
    blocks = call(
        spread_kernel,
        [((length, full // (2 * near_count)), bf16)] * (2 * near_count),
        *mids,
    )
    mids_here = []
    for step in range(near_count):
        for side in range(2):
            pairs = [
                (
                    n * 2 + c,
                    (n + step) % near_count * 2 + (c + side) % 2,
                )
                for n in range(near_count)
                for c in range(2)
            ]
            block = blocks[step * 2 + side]
            if step or side:
                block = lax.ppermute(block, (NEAR, CORE), pairs)
            mids_here.append(block)
    mids_here, _ = lax.optimization_barrier((mids_here, entry_grad))
    (out_grad,) = call(
        out_grad_kernel,
        [((full // (2 * near_count), inner), bf16)],
        rank,
        near,
        core,
        *mids_here,
        halves,
        scratch=[((halves.shape[0], full // (2 * near_count)), bf16)],
        scalars=3,
        far=(11,), kept=(0,),
    )
    out_part = lax.psum_scatter(out_grad, FAR, scatter_dimension=0, tiled=True)
    d_x, d_b, grad_out_map, d_log, *tail = call(
        within_kernel,
        [
            ((length, inner), f32),
            ((length, maps), f32),
            ((length, maps), f32),
            ((length, heads), f32),
            ((length, inner), bf16),
            ((length, inner), f32),
            (input_map.shape, bf16),
            (entry.shape, bf16),
            ((SUB, heads), f32),
        ],
        d_y,
        step_inputs,
        input_map,
        output_map,
        log_decay,
        entry,
        scratch=[((inner * NS // maps, NS), bf16), (log_decay.shape, f32)],
        far=(0, 1, 2, 3, 4, 5),
        kept=(2,),
    )
    grad_step, grad_in_map, grad_log, grad_out_weight = call(
        final_kernel,
        [((length, inner), bf16), ((length, maps), f32), ((heads, length), f32), (out_part.shape, f32)],
        carried,
        *tail,
        d_x,
        d_b,
        d_log,
        out_part,
        far=(9,),
        kept=(0, 1, 2, 3),
        late=(9,),
        early=True,
    )
    return (
        grad_gate[None],
        grad_up[None],
        grad_down[None],
        grad_out_weight,
        grad_step,
        grad_z,
        grad_in_map,
        grad_out_map,
        grad_log.T,
    )


def solution(mesh):
    torus = Mesh(mesh.devices.reshape(8, 4, 2, mesh.shape["tp"]), ("sp_0", "sp_1", "sp_2", "tp"))
    placed = (
        P(SP, "tp"),
        P(SP, "tp"),
        P(SP, None),
        P(SP, None),
        P(SP, None, "tp"),
        P(SP, None, "tp"),
        P(SP, "tp", None),
        P(SP, "tp"),
        P(SP, "tp"),
        P(SP, "tp"),
        P(SP, "tp"),
        P(SP, "tp"),
        P(SP, "tp"),
    )
    return jax.shard_map(
        local,
        mesh=torus,
        in_specs=placed,
        out_specs=(
            P(SP, None, "tp"),
            P(SP, None, "tp"),
            P(SP, "tp", None),
            P(SP, "tp"),
            P(SP, "tp"),
            P(SP, "tp"),
            P(SP, "tp"),
            P(SP, "tp"),
            P(SP, "tp"),
        ),
        check_vma=False,
    )
```

```python
import jax
import jax.numpy as jnp
from jax import lax
from jax.experimental import pallas as pl
from jax.experimental.pallas import tpu as pltpu
from jax.sharding import Mesh
from jax.sharding import PartitionSpec as P


SP = ("sp_0", "sp_1", "sp_2")
FAR, NEAR, CORE = SP
CAP = 5
SUB = 8
GRANT = 16 * 1024 * 1024
PIECE = 32
LANES = 128
HEAD_DIM = 64
NS = 128
epsilon = 1e-06
exact = lax.Precision.HIGHEST
by_rows = (((0,), (0,)), ((), ()))
by_cols = (((1,), (1,)), ((), ()))


def mul(a, b, dims=None, precision=None):
    dims = (((1,), (0,)), ((), ())) if dims is None else dims
    return lax.dot_general(a, b, dims, precision=precision, preferred_element_type=jnp.float32)


def places(shape, dim):
    return lax.broadcasted_iota(jnp.int32, shape, dim)


def head_spread(heads, width):
    shape = (heads, width)
    return (places(shape, 1) // HEAD_DIM == places(shape, 0)).astype(jnp.float32)


def running(log):
    length = log.shape[1]
    shape = (length, length)
    lower = (places(shape, 0) >= places(shape, 1)).astype(jnp.float32)
    return mul(lower, log, by_cols, precision=exact), mul(log, lower, by_cols, precision=exact)


def to_end_wide(cum, width):
    last = cum[-1:, :]
    return mul(jnp.exp(last - cum), head_spread(cum.shape[1], width), precision=exact)


def gather_cells(wide_ref, out_ref, count):
    for tile in range(out_ref.shape[1] // LANES):
        for first in range(0, count, 2):
            rows = jnp.concatenate(
                [
                    wide_ref[pl.ds(tile * SUB * count + first + k, SUB, stride=count), :]
                    for k in range(2)
                ],
                axis=0,
            )
            out_ref[first * SUB : (first + 2) * SUB, tile * LANES : (tile + 1) * LANES] = rows.astype(
                out_ref.dtype
            )


def place_kernel(routes_ref, weight_ref, rows_ref, cot_ref, out_ref, placing_ref, wide_ref):
    top, length = routes_ref.shape
    experts = placing_ref.shape[0] // CAP
    shape = (experts, length)
    expert = places(shape, 0)
    hits = [routes_ref[k : k + 1, :] == expert for k in range(top)]
    named = hits[0]
    for k in range(1, top):
        named = jnp.logical_or(named, hits[k])
    square = (length, length)
    sooner = (places(square, 0) < places(square, 1)).astype(jnp.bfloat16)
    taken = mul(named.astype(jnp.bfloat16), sooner)
    ranks = [jnp.sum(jnp.where(h, taken, 0.0), axis=0, keepdims=True) for h in hits]
    rows, cot = rows_ref[...], cot_ref[...]
    width = rows.shape[1]
    pieces = 2 * width // LANES
    for slot in range(CAP):
        here = [jnp.logical_and(hits[k], ranks[k] == float(slot)) for k in range(top)]
        weight = jnp.zeros((experts, 1), jnp.float32)
        for k in range(top):
            weight = weight + jnp.sum(
                jnp.where(here[k], weight_ref[k : k + 1, :], 0.0), axis=1, keepdims=True
            )
        chosen = here[0]
        for k in range(1, top):
            chosen = jnp.logical_or(chosen, here[k])
        chosen = chosen.astype(jnp.float32).astype(jnp.bfloat16)
        placing_ref[slot * experts : (slot + 1) * experts, :] = chosen
        both = (mul(chosen, rows), mul(chosen, cot) * weight)
        for j in range(pieces):
            source = both[j * LANES // width]
            start = j * LANES % width
            cell = (slot * pieces + j) * experts
            wide_ref[cell : cell + experts, :] = source[:, start : start + LANES]
    gather_cells(wide_ref, out_ref, experts)


def arrange_kernel(got_ref, out_ref, wide_ref):
    for slot in range(CAP):
        wide_ref[slot] = got_ref[:, slot * LANES : (slot + 1) * LANES].astype(jnp.float32)
    slots, width = out_ref.shape[0] // 2, out_ref.shape[1]
    count = slots // CAP
    pieces = 2 * width // LANES
    for slot in range(CAP):
        for j in range(pieces):
            block = wide_ref[slot, pl.ds(j, count, stride=pieces), :]
            base = j * LANES // width * slots + slot * count
            start = j * LANES % width
            out_ref[base : base + count, start : start + LANES] = block.astype(out_ref.dtype)


def block_of(rank, step, parts, width):
    return pl.multiple_of(lax.rem(rank + step, parts) * width, width)


def expert_kernel(rank_ref, *refs):
    refs, flush = refs[:-2], refs[-2]
    parts = (len(refs) - 6) // 2
    both_refs, part_refs = refs[:parts], refs[-parts:]
    gate_ref, up_ref, down_ref, hidden_ref, dgate_ref, dup_ref = refs[parts:-parts]
    slots, width = part_refs[0].shape
    gate_pre = up_pre = d_act = None
    for step in range(parts):
        block = pl.ds(block_of(rank_ref[0], step, parts, width), width)
        rows, cot = both_refs[step][:slots, :], both_refs[step][slots:, :]
        one, two = mul(rows, gate_ref[block, :]), mul(rows, up_ref[block, :])
        three = mul(cot, down_ref[:, block], by_cols)
        gate_pre = one if step == 0 else gate_pre + one
        up_pre = two if step == 0 else up_pre + two
        d_act = three if step == 0 else d_act + three
    sig = jax.nn.sigmoid(gate_pre)
    hidden_ref[...] = (gate_pre * sig * up_pre).astype(jnp.bfloat16)
    d_gate = (d_act * up_pre * sig * (1.0 + gate_pre * (1.0 - sig))).astype(jnp.bfloat16)
    d_up = (d_act * gate_pre * sig).astype(jnp.bfloat16)
    dgate_ref[...] = d_gate
    dup_ref[...] = d_up
    for k in range(3):
        flush(k)
    for step in (1, 2, 3, 0):
        block = pl.ds(block_of(rank_ref[0], step, parts, width), width)
        part = mul(d_gate, gate_ref[block, :], by_cols) + mul(d_up, up_ref[block, :], by_cols)
        part_refs[step][...] = part.astype(part_refs[step].dtype)
        if step:
            flush(3 + step)


def weight_grad_kernel(rank_ref, *refs):
    parts = len(refs) - 6
    both_refs = refs[:parts]
    hidden_ref, dgate_ref, dup_ref, gate_ref, up_ref, down_ref = refs[parts:]
    slots, width = hidden_ref.shape[0], both_refs[0].shape[1]
    for step in range(parts):
        block = pl.ds(block_of(rank_ref[0], step, parts, width), width)
        rows, cot = both_refs[step][:slots, :], both_refs[step][slots:, :]
        gate_ref[block, :] = mul(rows, dgate_ref[...], by_rows)
        up_ref[block, :] = mul(rows, dup_ref[...], by_rows)
        down_ref[:, block] = mul(hidden_ref[...], cot, by_rows)


def add_kernel(one_ref, two_ref, three_ref, four_ref, out_ref, wide_ref):
    slots, width = one_ref.shape
    total = one_ref[...].astype(jnp.float32)
    for got_ref in (two_ref, three_ref, four_ref):
        total = total + got_ref[...].astype(jnp.float32)
    count = slots // CAP
    pieces = width // LANES
    used = CAP * pieces * count
    wide_ref[used:, :] = jnp.zeros((wide_ref.shape[0] - used, LANES), jnp.float32)
    for slot in range(CAP):
        for j in range(pieces):
            cell = (slot * pieces + j) * count
            wide_ref[cell : cell + count, :] = total[
                slot * count : (slot + 1) * count, j * LANES : (j + 1) * LANES
            ]
    gather_cells(wide_ref, out_ref, count)


def mid_kernel(back_ref, placing_ref, cot_ref, out_ref, wide_ref, slots_ref):
    for tile in range(wide_ref.shape[0]):
        wide_ref[tile] = back_ref[:, tile * LANES : (tile + 1) * LANES].astype(jnp.float32)
    slots, width = slots_ref.shape
    count = slots // CAP
    pieces = width // LANES
    for slot in range(CAP):
        for j in range(pieces):
            tile, row = divmod(slot * pieces + j, SUB)
            block = wide_ref[tile, pl.ds(row, count, stride=SUB), :]
            slots_ref[slot * count : (slot + 1) * count, j * LANES : (j + 1) * LANES] = block.astype(
                slots_ref.dtype
            )
    routed = mul(placing_ref[...], slots_ref[...], by_rows)
    mid = (cot_ref[...].astype(jnp.float32) + routed).astype(jnp.bfloat16)
    lane = places((1, width), 1)
    per_block = 2 * PIECE
    block, inside = lane // per_block, lane % per_block
    step_near, step_core = block // 2, block % 2
    far, row = inside // PIECE, inside % PIECE
    source = (
        far * (width // 2) + step_near * per_block + step_core * PIECE + row
    )
    moved = (places((width, width), 0) == source).astype(jnp.float32).astype(jnp.bfloat16)
    out_ref[...] = mul(mid, moved).astype(out_ref.dtype)


def weight_kernel(
    near_ref,
    core_ref,
    mine_ref,
    other_ref,
    y_ref,
    z_ref,
    c_ref,
    back_ref,
    log_ref,
    out_ref,
    y_out,
    z_out,
    c_out,
    back_out,
    wide_ref,
    log,
    sems,
):
    steps, tp_count = 4, 4
    per_tp = mine_ref.shape[0] // (tp_count * steps * PIECE)
    count = 2 * mine_ref.shape[0] // PIECE

    def piece(k):
        far, rest = k % per_tp, k // per_tp
        step, q = rest % steps, rest // steps
        source = pl.ds(pl.multiple_of(((q * per_tp + far) * steps + step) * PIECE, PIECE), PIECE)
        near = lax.rem(near_ref[0] + step, steps)
        made = []
        for side, ref in enumerate((mine_ref, other_ref)):
            core = lax.rem(core_ref[0] + side, 2)
            target = (((q * steps + near) * 2 + core) * per_tp + far) * PIECE
            made.append(
                pltpu.make_async_copy(
                    ref.at[source, :],
                    out_ref.at[pl.ds(pl.multiple_of(target, PIECE), PIECE), :],
                    sems.at[2 * k + side],
                )
            )
        return made

    def begin(k, carry):
        for copy in piece(k):
            copy.start()
        return carry

    def finish(k, carry):
        for copy in piece(k):
            copy.wait()
        return carry

    extra = ((log_ref, log), (y_ref, y_out), (z_ref, z_out), (c_ref, c_out), (back_ref, back_out))
    moves = [
        pltpu.make_async_copy(source, target, sems.at[count + k])
        for k, (source, target) in enumerate(extra)
    ]
    for move in moves:
        move.start()
    lax.fori_loop(0, count // 2, begin, 0)
    moves[0].wait()
    cum, _ = running(log[...])
    heads, width = log.shape[0], wide_ref.shape[1]
    wide_ref[...] = mul(jnp.exp(cum), head_spread(heads, width), precision=exact)
    for move in moves[1:]:
        move.wait()
    lax.fori_loop(0, count // 2, finish, 0)


def ordered_weight(near, core, mine, other, y, z, c, back, log):
    far_spec = pl.BlockSpec(memory_space=pltpu.HBM)
    rows, width = mine.shape
    near_spec = pl.BlockSpec(memory_space=pltpu.VMEM)
    shapes = [((2 * rows, width), mine.dtype)]
    shapes += [(a.shape, a.dtype) for a in (y, z, c, back)] + [(y.shape, jnp.float32)]
    return pl.pallas_call(
        weight_kernel,
        out_shape=tuple(jax.ShapeDtypeStruct(s, d) for s, d in shapes),
        in_specs=[pl.BlockSpec(memory_space=pltpu.SMEM)] * 2 + [far_spec] * 7,
        out_specs=(near_spec,) * len(shapes),
        scratch_shapes=[
            pltpu.VMEM(log.shape, log.dtype),
            pltpu.SemaphoreType.DMA((2 * rows // PIECE + 5,)),
        ],
        compiler_params=pltpu.CompilerParams(vmem_limit_bytes=GRANT),
        name="weight_kernel",
    )(near, core, *(in_hbm(a) for a in (mine, other, y, z, c, back, log)))


def spread_kernel(*refs):
    mid_refs, out_ref = refs[:-1], refs[-1]
    count, width = out_ref.shape[0], out_ref.shape[2] // len(mid_refs)
    for j in range(count):
        for k, mid_ref in enumerate(mid_refs):
            out_ref[j, :, k * width : (k + 1) * width] = mid_ref[:, j * width : (j + 1) * width]


def span_of(index, size):
    return pl.ds(pl.multiple_of(index * size, size), size)


def put_state(out_ref, group, part):
    rows = part.shape[0] // 2
    tiles = part.reshape(rows // SUB, 2, SUB, NS)
    for k in range(2):
        out_ref[span_of(group, rows), k * NS : (k + 1) * NS] = (
            tiles[:, k].reshape(rows, NS).astype(out_ref.dtype)
        )


def get_state(ref, group, groups):
    rows = ref.shape[0] // groups
    halves = [
        ref[span_of(group, rows), k * NS : (k + 1) * NS]
        .astype(jnp.float32)
        .reshape(rows // SUB, SUB, NS)
        for k in range(2)
    ]
    return jnp.stack(halves, axis=1).reshape(2 * rows, NS)


def mix_kernel(
    got_ref, gate_ref, up_ref, down_ref, out_ref, back_ref, gate_out, up_out, down_out, sems
):
    fetches = [
        pltpu.make_async_copy(source, target, sems.at[k])
        for k, (source, target) in enumerate(
            ((gate_ref, gate_out), (up_ref, up_out), (down_ref, down_out))
        )
    ]
    for fetch in fetches:
        fetch.start()
    count = got_ref.shape[0]
    devices = count // SUB
    state = got_ref[:, : 2 * NS]
    shape = (devices, count)
    chosen = (places(shape, 1) == SUB * places(shape, 0)).astype(jnp.float32).astype(jnp.bfloat16)
    parts = mul(chosen, got_ref[:, 2 * NS :])
    logs = jnp.sum(jnp.where(places(parts.shape, 1) < 3, parts, 0.0), axis=1, keepdims=True)
    log = jnp.broadcast_to(logs, parts.shape)
    small = (devices, devices)
    one, two = places(small, 0), places(small, 1)
    through = mul((one >= two).astype(jnp.float32), log, precision=exact)
    before = through - log
    through_row = mul(log, (one <= two).astype(jnp.float32), by_rows, precision=exact)[:1]
    before_row = mul(log, (one < two).astype(jnp.float32), by_rows, precision=exact)[:1]
    tall = (count, devices)
    copies = (places(tall, 0) // SUB == places(tall, 1)).astype(jnp.float32).astype(jnp.bfloat16)
    square = (count, count)
    same = places(square, 0) % SUB == places(square, 1) % SUB

    def spread(weights):
        wide = mul(mul(copies, weights).astype(jnp.bfloat16), copies, by_cols)
        return jnp.where(same, wide, 0.0).astype(jnp.bfloat16)

    def wide_weights(spans, mask):
        return spread(jnp.exp(jnp.where(mask, spans, -jnp.inf)).astype(jnp.bfloat16))

    weights = wide_weights(before[:, :1] - through_row, two < one)
    out_ref[...] = mul(weights, state).astype(out_ref.dtype)
    back_ref[...] = wide_weights(before_row - through[:, :1], one < two)
    for fetch in fetches:
        fetch.wait()


def mix_back_kernel(got_ref, back_ref, out_ref):
    out_ref[...] = mul(back_ref[...], got_ref[...]).astype(out_ref.dtype)


def state_kernel(x_ref, b_ref, log_ref, out_ref):
    log = log_ref[...]
    width = x_ref.shape[1]
    cum, _ = running(log)
    scaled = (x_ref[...].astype(jnp.float32) * to_end_wide(cum, width)).astype(jnp.bfloat16)
    groups = b_ref.shape[1] // NS
    each = width // groups
    for g in range(groups):
        part = mul(scaled[:, g * each : (g + 1) * each], b_ref[:, g * NS : (g + 1) * NS], by_rows)
        put_state(out_ref, g, part)
    rows, heads = out_ref.shape[0], log.shape[0]
    shape = (rows, heads)
    owner = places(shape, 0) // (rows // heads) == places(shape, 1)
    total = jnp.sum(jnp.where(owner, cum[-1:, :], 0.0), axis=1, keepdims=True)
    high = total.astype(jnp.bfloat16).astype(jnp.float32)
    middle = (total - high).astype(jnp.bfloat16).astype(jnp.float32)
    low = total - high - middle
    lane = places((rows, NS), 1)
    out_ref[:, 2 * NS :] = jnp.where(
        lane == 0, high, jnp.where(lane == 1, middle, jnp.where(lane == 2, low, 0.0))
    ).astype(out_ref.dtype)


def head_column(values, head):
    return jnp.sum(jnp.where(places(values.shape, 1) == head, values, 0.0), axis=1, keepdims=True)


def decays(column, row):
    shape = (column.shape[0], row.shape[1])
    return jnp.exp(jnp.where(places(shape, 0) >= places(shape, 1), column - row, -jnp.inf))


def half_masks(length):
    lane = places((length, 2 * HEAD_DIM), 1)
    return (lane < HEAD_DIM, lane >= HEAD_DIM)


def forward_kernel(x_ref, b_ref, c_ref, log_ref, z_ref, entry_ref, y_ref, half_ref, row_ref, wide_ref):
    log = log_ref[...]
    heads, length = log.shape
    width = x_ref.shape[1]
    groups = b_ref.shape[1] // NS
    each = width // groups
    per_group = heads // groups
    cum, cum_row = running(log)
    row_ref[...] = cum_row
    from_start = mul(jnp.exp(cum), head_spread(heads, width), precision=exact)
    masks = half_masks(length)
    zero = jnp.zeros((length, 2 * HEAD_DIM), jnp.bfloat16)
    wide_ref[...] = from_start

    def group_step(g, carry):
        c_group = c_ref[:, span_of(g, NS)]
        scores = mul(c_group, b_ref[:, span_of(g, NS)], by_cols)
        carried = mul(c_group, get_state(entry_ref, g, groups).astype(jnp.bfloat16), by_cols)

        def pair_step(pair, carry):
            head = g * per_group + 2 * pair
            lanes = pl.ds(pl.multiple_of(head * HEAD_DIM, 2 * HEAD_DIM), 2 * HEAD_DIM)
            x_pair = x_ref[:, lanes]
            total = jnp.zeros((length, 2 * HEAD_DIM), jnp.float32)
            for k in range(2):
                decay = decays(head_column(cum, head + k), row_ref[pl.ds(head + k, 1), :])
                weights = (scores * decay).astype(jnp.bfloat16)
                total = total + mul(weights, jnp.where(masks[k], x_pair, zero))
            y_ref[:, lanes] = total
            return carry

        lax.fori_loop(0, per_group // 2, pair_step, 0)
        cols = span_of(g, each)
        y = y_ref[:, cols] + carried * wide_ref[:, cols]
        z = z_ref[:, cols].astype(jnp.float32)
        gated = y * (z * jax.nn.sigmoid(z))
        mean = jnp.mean(gated * gated, axis=1, keepdims=True)
        y_ref[:, cols] = y
        half_ref[:, cols] = (gated * lax.rsqrt(mean + epsilon)).astype(half_ref.dtype)
        return carry

    lax.fori_loop(0, groups, group_step, 0)


def gate_kernel(rank_ref, m0, m1, m2, m3, w_ref, y_ref, z_ref, c_ref, wide_ref, dy_ref, dz_ref, out_ref):
    width = y_ref.shape[1]
    groups = c_ref.shape[1] // NS
    each = width // groups
    mid_refs = (m0, m1, m2, m3)
    parts, rows = len(mid_refs), m0.shape[1]

    def group_step(g, carry):
        cols = span_of(g, each)
        d_normed = None
        for step in range(parts):
            block = pl.ds(block_of(rank_ref[0], step, parts, rows), rows)
            part = mul(mid_refs[step][...], w_ref[block, cols])
            d_normed = part if d_normed is None else d_normed + part
        y = y_ref[:, cols]
        z = z_ref[:, cols].astype(jnp.float32)
        sig = jax.nn.sigmoid(z)
        silu = z * sig
        gated = y * silu
        inverse = lax.rsqrt(jnp.mean(gated * gated, axis=1, keepdims=True) + epsilon)
        normed = gated * inverse
        along = jnp.mean(d_normed * normed, axis=1, keepdims=True)
        d_gated = inverse * (d_normed - normed * along)
        d_y = d_gated * silu
        dy_ref[:, cols] = d_y.astype(dy_ref.dtype)
        dz_ref[:, cols] = (d_gated * y * (sig * (1.0 + z * (1.0 - sig)))).astype(dz_ref.dtype)
        scaled = (d_y * wide_ref[:, cols]).astype(jnp.bfloat16)
        part = mul(scaled, c_ref[:, span_of(g, NS)], by_rows)
        put_state(out_ref, g, part)
        return carry

    lax.fori_loop(0, groups, group_step, 0)


def within_kernel(
    dy_ref,
    x_ref,
    b_ref,
    c_ref,
    log_ref,
    entry_ref,
    dx_ref,
    db_ref,
    dc_ref,
    dlog_ref,
    scaled_ref,
    end_ref,
    b_out,
    entry_out,
    last_ref,
    state_ref,
    row_ref,
):
    log = log_ref[...]
    heads, length = log.shape
    width = x_ref.shape[1]
    groups = b_ref.shape[1] // NS
    per_group = heads // groups
    cum, cum_row = running(log)
    row_ref[...] = cum_row
    to_end = to_end_wide(cum, width)
    end_ref[...] = to_end
    scaled_ref[...] = (x_ref[...].astype(jnp.float32) * to_end).astype(scaled_ref.dtype)
    b_out[...] = b_ref[...]
    entry_out[...] = entry_ref[...]
    last_ref[...] = jnp.broadcast_to(jnp.exp(cum[-1:, :]), last_ref.shape)
    masks = half_masks(length)
    zero = jnp.zeros((length, 2 * HEAD_DIM), jnp.bfloat16)
    d_cum = jnp.zeros((length, heads), jnp.float32)
    d_row = jnp.zeros((heads, length), jnp.float32)
    head_col = places((length, heads), 1)
    head_row = places((heads, length), 0)

    def group_step(g, totals):
        d_cum, d_row = totals
        c_group = c_ref[:, span_of(g, NS)]
        b_group = b_ref[:, span_of(g, NS)]
        c_wide = c_group.astype(jnp.float32)
        scores = mul(c_group, b_group, by_cols)
        state_ref[...] = get_state(entry_ref, g, groups).astype(jnp.bfloat16)

        def pair_step(pair, carry):
            d_scores, d_c, d_cum, d_row = carry
            head = g * per_group + 2 * pair
            cols = pl.ds(pl.multiple_of(head * HEAD_DIM, 2 * HEAD_DIM), 2 * HEAD_DIM)
            state_rows = pl.ds(pl.multiple_of(pair * 2 * HEAD_DIM, 2 * HEAD_DIM), 2 * HEAD_DIM)
            x_pair, dy_pair, entry_pair = x_ref[:, cols], dy_ref[:, cols], state_ref[state_rows, :]
            d_x = jnp.zeros((length, 2 * HEAD_DIM), jnp.float32)
            for k in range(2):
                column = head_column(cum, head + k)
                decay = decays(column, row_ref[pl.ds(head + k, 1), :])
                dy_one = jnp.where(masks[k], dy_pair, zero)
                weights = scores * decay
                d_weights = mul(dy_one, x_pair, by_cols)
                d_x = d_x + mul(weights.astype(jnp.bfloat16), dy_one, by_rows)
                d_scores = d_scores + d_weights * decay
                spread = d_weights * weights
                from_entry = mul(dy_one, entry_pair) * jnp.exp(column)
                d_c = d_c + from_entry
                rows = jnp.sum(spread + c_wide * from_entry, axis=1, keepdims=True)
                d_cum = jnp.where(head_col == head + k, rows, d_cum)
                d_row = jnp.where(
                    head_row == head + k, jnp.sum(spread, axis=0, keepdims=True), d_row
                )
            dx_ref[:, cols] = d_x
            return d_scores, d_c, d_cum, d_row

        square = jnp.zeros((length, length), jnp.float32)
        d_scores, d_c, d_cum, d_row = lax.fori_loop(
            0, per_group // 2, pair_step, (square, jnp.zeros((length, NS), jnp.float32), d_cum, d_row)
        )
        half = d_scores.astype(jnp.bfloat16)
        dc_ref[:, span_of(g, NS)] = d_c + mul(half, b_group)
        db_ref[:, span_of(g, NS)] = mul(half, c_group, by_rows)
        return d_cum, d_row

    d_cum, d_row = lax.fori_loop(0, groups, group_step, (d_cum, d_row))
    shape = (length, length)
    upper = (places(shape, 0) <= places(shape, 1)).astype(jnp.float32)
    dlog_ref[...] = mul(upper, d_cum, precision=exact) - mul(upper, d_row, by_cols, precision=exact)


def final_kernel(
    grad_ref,
    scaled_ref,
    end_ref,
    b_ref,
    entry_ref,
    last_ref,
    dx_ref,
    db_ref,
    dlog_ref,
    out_ref,
    gx_ref,
    gb_ref,
    glog_ref,
    gout_ref,
    flush,
    ready,
):
    length, heads = dlog_ref.shape
    width = dx_ref.shape[1]
    groups = b_ref.shape[1] // NS
    each = width // groups
    ones = jnp.ones((SUB, NS), jnp.float32)

    def group_step(g, carry):
        moved, kept = carry
        cols, maps = span_of(g, each), span_of(g, NS)
        shape = (heads, each)
        owner = places(shape, 1) // HEAD_DIM + g * (each // HEAD_DIM)
        spread = (owner == places(shape, 0)).astype(jnp.float32)
        grad_wide = get_state(grad_ref, g, groups)
        grad = grad_wide.astype(jnp.bfloat16)
        scaled = scaled_ref[:, cols]
        raw = mul(b_ref[:, maps], grad, by_cols)
        gx_ref[:, cols] = (dx_ref[:, cols] + raw * end_ref[:, cols]).astype(gx_ref.dtype)
        moved = moved + mul(scaled.astype(jnp.float32) * raw, spread, by_cols, precision=exact)
        gb_ref[:, maps] = db_ref[:, maps] + mul(scaled, grad)
        both = get_state(entry_ref, g, groups) * grad_wide
        kept = kept + mul(
            mul(ones, both, by_cols, precision=exact), spread, by_cols, precision=exact
        )
        return moved, kept

    moved, kept = lax.fori_loop(
        0,
        groups,
        group_step,
        (jnp.zeros((length, heads), jnp.float32), jnp.zeros((SUB, heads), jnp.float32)),
    )
    ready(9)
    gout_ref[...] = out_ref[...].astype(jnp.float32)
    for k in (0, 1, 3):
        flush(k)
    shape = (length, length)
    earlier = (places(shape, 0) > places(shape, 1)).astype(jnp.float32)
    total = dlog_ref[...] + mul(earlier, moved, precision=exact) + (kept * last_ref[...])[:1, :]
    same = (places(shape, 0) == places(shape, 1)).astype(jnp.float32)
    glog_ref[...] = mul(total, same, by_rows, precision=exact)


def out_grad_kernel(rank_ref, mid_ref, half_ref, out_ref):
    total = mul(mid_ref[...], half_ref[...], by_rows)
    parts = 4
    rows = total.shape[0] // parts
    for step in range(parts):
        block = pl.ds(block_of(rank_ref[0], step, parts, rows), rows)
        out_ref[block, :] = total[step * rows : (step + 1) * rows].astype(out_ref.dtype)


def in_hbm(array):
    return pltpu.with_memory_space_constraint(array, pltpu.HBM)


def call(kernel, shapes, *args, scratch=(), scalars=0, far=(), kept=(), raw=(), sems=0, late=(), early=False):
    near_spec = pl.BlockSpec(memory_space=pltpu.VMEM)
    far_spec = pl.BlockSpec(memory_space=pltpu.HBM)
    scalar = pl.BlockSpec(memory_space=pltpu.SMEM)
    n_in, n_out = len(args), len(shapes)
    staged = [(args[i].shape, args[i].dtype) for i in far] + [shapes[i] for i in kept]

    def body(*refs):
        ins, outs = list(refs[:n_in]), list(refs[n_in : n_in + n_out])
        own = refs[n_in + n_out :]
        stage, flags = own[len(scratch) : len(scratch) + len(staged)], own[-1]
        fetches, writes, started = {}, {}, set()
        for k, i in enumerate(far):
            fetches[i] = pltpu.make_async_copy(ins[i], stage[k], flags.at[k])
            fetches[i].start()
            ins[i] = stage[k]
        for i in far:
            if i not in late:
                fetches[i].wait()
        for k, i in enumerate(kept, len(far)):
            writes[i] = pltpu.make_async_copy(stage[k], outs[i], flags.at[k])
            outs[i] = stage[k]

        def flush(i):
            started.add(i)
            writes[i].start()

        extra = [own[-2]] if sems else []
        if early:
            extra += [flush, lambda i: fetches[i].wait()]
        kernel(*ins, *outs, *own[: len(scratch)], *extra)
        for i in writes:
            if i not in started:
                flush(i)
        for write in writes.values():
            write.wait()

    spaces = [far_spec if i in (*far, *raw) else near_spec for i in range(n_in)]
    return pl.pallas_call(
        body,
        out_shape=tuple(
            pltpu.HBM(s, d) if i in kept else jax.ShapeDtypeStruct(s, d)
            for i, (s, d) in enumerate(shapes)
        ),
        in_specs=[scalar if i < scalars else spaces[i] for i in range(n_in)],
        out_specs=tuple(far_spec if i in kept else near_spec for i in range(n_out)),
        scratch_shapes=[pltpu.VMEM(s, d) for s, d in (*scratch, *staged)]
        + ([pltpu.SemaphoreType.DMA((sems,))] if sems else [])
        + [pltpu.SemaphoreType.DMA((max(len(staged), 1),))],
        compiler_params=pltpu.CompilerParams(vmem_limit_bytes=GRANT),
    )(*(in_hbm(arg) if i in (*far, *raw) else arg for i, arg in enumerate(args)))


def swap(array, axis):
    return lax.all_to_all(array, axis, split_axis=0, concat_axis=0, tiled=True)


def moved(array, axis, step):
    count = lax.axis_size(axis)
    return lax.ppermute(array, axis, [((i + step) % count, i) for i in range(count)])


def from_others(array, axis):
    return [array] + [moved(array, axis, step) for step in (1, 2, 3)]


def local(
    hidden_rows,
    out_cot,
    routes,
    route_weight,
    gate_w,
    up_w,
    down_w,
    out_weight,
    step_inputs,
    input_map,
    output_map,
    log_decay,
    gate_z,
):
    f32, bf16 = jnp.float32, jnp.bfloat16
    inner = step_inputs.shape[1]
    maps = input_map.shape[1]
    sp_count, tp_count = lax.axis_size(SP), lax.axis_size("tp")
    width = hidden_rows.shape[1]
    slots = sp_count * CAP
    back_tiles = -(-CAP * width // (LANES * SUB))
    pieces = width // LANES
    hidden_units = gate_w.shape[2]
    full = width * tp_count

    length, heads = log_decay.shape
    log_decay = log_decay.T
    rank = lax.axis_index("tp").astype(jnp.int32)[None]
    near = lax.axis_index(NEAR).astype(jnp.int32)[None]
    core = lax.axis_index(CORE).astype(jnp.int32)[None]
    sent, placing = call(
        place_kernel,
        [((sp_count * 2 * pieces, CAP * LANES), bf16), ((slots, length), bf16)],
        routes.T,
        route_weight.T,
        hidden_rows,
        out_cot,
        scratch=[((CAP * 2 * pieces * sp_count, LANES), f32)],
        far=(0, 1, 2, 3), kept=(1,),
    )
    state_rows = inner // 2
    (own,) = call(
        state_kernel,
        [((state_rows, 3 * NS), bf16)],
        step_inputs,
        input_map,
        log_decay,
        far=(0, 1, 2),
    )
    near_pieces = from_others(out_weight, NEAR)
    got = swap(sent.reshape(sp_count, 2 * pieces, CAP * LANES), SP)
    got, near_pieces = lax.optimization_barrier((got, near_pieces))
    (lined,) = call(
        arrange_kernel,
        [((2 * slots, width), bf16)],
        got.reshape(sent.shape),
        scratch=[((CAP, sent.shape[0], LANES), f32)],
    )
    filled = (lined, moved(lined, "tp", 1), moved(lined, "tp", 2), moved(lined, "tp", -1))
    got_own = swap(own.reshape(sp_count, SUB, 3 * NS), SP).reshape(own.shape)
    matrices = (gate_w[0], up_w[0], down_w[0])
    mixed, back, *matrices = call(
        mix_kernel,
        [((state_rows, 2 * NS), bf16), ((state_rows, state_rows), bf16)]
        + [(m.shape, bf16) for m in matrices],
        got_own,
        *matrices,
        kept=(1,),
        raw=(1, 2, 3),
        sems=3,
    )
    filled, mixed = lax.optimization_barrier((filled, mixed))
    hidden, d_gate, d_up, *partials = call(
        expert_kernel,
        [((slots, hidden_units), bf16)] * 3 + [((slots, width), bf16)] * tp_count,
        rank,
        *filled,
        *matrices,
        scalars=1,
        kept=(0, 1, 2, *range(4, 3 + tp_count)), early=True,
    )
    near_pieces, _ = lax.optimization_barrier((near_pieces, d_up))
    near_weight = jnp.concatenate(near_pieces, axis=0)
    half_weight = lax.all_gather(near_weight, FAR, axis=0, tiled=True)
    received = [partials[0]] + [moved(partials[step], "tp", -step) for step in (1, 2, 3)]
    entry = swap(mixed.reshape(sp_count, SUB, 2 * NS), SP).reshape(mixed.shape)
    (summed,) = call(
        add_kernel,
        [((sp_count * SUB, back_tiles * LANES), bf16)],
        *received,
        scratch=[((back_tiles * SUB * sp_count, LANES), f32)],
    )
    grad_gate, grad_up, grad_down = call(
        weight_grad_kernel,
        [((full, hidden_units), f32)] * 2 + [((hidden_units, full), f32)],
        rank,
        *filled,
        hidden,
        d_gate,
        d_up,
        scalars=1,
        far=(5, 6, 7), kept=(0, 1, 2),
    )
    half_weight, _ = lax.optimization_barrier((half_weight, grad_gate))
    other_weight = moved(half_weight, CORE, 1)
    returned = swap(summed.reshape(sp_count, SUB, back_tiles * LANES), SP).reshape(summed.shape)
    (mid_part,) = call(
        mid_kernel,
        [((length, width), bf16)],
        returned,
        placing,
        out_cot,
        scratch=[((back_tiles, summed.shape[0], LANES), f32), ((slots, width), bf16)],
        far=(1, 2),
    )
    mids = from_others(mid_part, "tp")
    y, half = call(
        forward_kernel,
        [((length, inner), f32), ((length, inner), bf16)],
        step_inputs,
        input_map,
        output_map,
        log_decay,
        gate_z,
        entry,
        scratch=[(log_decay.shape, f32), ((length, inner), f32)], far=(0, 1, 2, 3, 4, 5), kept=(0, 1),
    )
    full_weight, *gate_values, back, wide = ordered_weight(
        near, core, half_weight, other_weight, y, gate_z, output_map, back, log_decay
    )
    halves = lax.all_gather(half, (NEAR, CORE), axis=0, tiled=True)
    d_y, grad_z, entry_grad = call(
        gate_kernel,
        [((length, inner), bf16)] * 2 + [((state_rows, 2 * NS), bf16)],
        rank,
        *mids,
        full_weight,
        *gate_values,
        wide,
        scalars=1,
        kept=(0, 1),
    )
    got_grad = swap(entry_grad.reshape(sp_count, SUB, 2 * NS), SP).reshape(entry_grad.shape)
    (mixed_grad,) = call(
        mix_back_kernel, [((state_rows, 2 * NS), bf16)], got_grad, back
    )
    carried = swap(mixed_grad.reshape(sp_count, SUB, 2 * NS), SP).reshape(mixed_grad.shape)
    near_count = lax.axis_size(NEAR)
    (blocks,) = call(
        spread_kernel, [((2 * near_count, length, full // (2 * near_count)), bf16)], *mids
    )
    blocks = swap(blocks, (NEAR, CORE)).reshape(halves.shape[0], -1)
    blocks, _ = lax.optimization_barrier((blocks, entry_grad))
    (out_grad,) = call(
        out_grad_kernel,
        [((full // (2 * near_count), inner), bf16)],
        rank,
        blocks,
        halves,
        scalars=1,
        far=(2,),
        kept=(0,),
    )
    out_part = lax.psum_scatter(out_grad, FAR, scatter_dimension=0, tiled=True)
    d_x, d_b, grad_out_map, d_log, *tail = call(
        within_kernel,
        [
            ((length, inner), f32),
            ((length, maps), f32),
            ((length, maps), f32),
            ((length, heads), f32),
            ((length, inner), bf16),
            ((length, inner), f32),
            (input_map.shape, bf16),
            (entry.shape, bf16),
            ((SUB, heads), f32),
        ],
        d_y,
        step_inputs,
        input_map,
        output_map,
        log_decay,
        entry,
        scratch=[((inner * NS // maps, NS), bf16), (log_decay.shape, f32)],
        far=(0, 1, 2, 3, 4, 5),
        kept=(2,),
    )
    grad_step, grad_in_map, grad_log, grad_out_weight = call(
        final_kernel,
        [((length, inner), bf16), ((length, maps), f32), ((heads, length), f32), (out_part.shape, f32)],
        carried,
        *tail,
        d_x,
        d_b,
        d_log,
        out_part,
        far=(9,),
        kept=(0, 1, 2, 3),
        late=(9,),
        early=True,
    )
    return (
        grad_gate[None],
        grad_up[None],
        grad_down[None],
        grad_out_weight,
        grad_step,
        grad_z,
        grad_in_map,
        grad_out_map,
        grad_log.T,
    )


def solution(mesh):
    torus = Mesh(mesh.devices.reshape(8, 4, 2, mesh.shape["tp"]), ("sp_0", "sp_1", "sp_2", "tp"))
    placed = (
        P(SP, "tp"),
        P(SP, "tp"),
        P(SP, None),
        P(SP, None),
        P(SP, None, "tp"),
        P(SP, None, "tp"),
        P(SP, "tp", None),
        P(SP, "tp"),
        P(SP, "tp"),
        P(SP, "tp"),
        P(SP, "tp"),
        P(SP, "tp"),
        P(SP, "tp"),
    )
    return jax.shard_map(
        local,
        mesh=torus,
        in_specs=placed,
        out_specs=(
            P(SP, None, "tp"),
            P(SP, None, "tp"),
            P(SP, "tp", None),
            P(SP, "tp"),
            P(SP, "tp"),
            P(SP, "tp"),
            P(SP, "tp"),
            P(SP, "tp"),
            P(SP, "tp"),
        ),
        check_vma=False,
    )
```
